32 devices in a mesh: sp: 8 (over z, y), dp: 4 (over x, core).
Axes of the slice: x: 2, y: 2, z: 4, core: 2. Of those that a mesh axis runs over, the one named last changes fastest.
Arguments:
- residual_input: bfloat16 [4, 1024, 2048], P('dp', 'sp'), may hold values from -6 to 6
- queries: bfloat16 [4, 1024, 512], P('dp', 'sp'), may hold values from -6 to 6
- keys: bfloat16 [4, 1024, 512], P('dp', 'sp'), may hold values from -6 to 6
- values: bfloat16 [4, 1024, 1024], P('dp', 'sp'), may hold values from -6 to 6
- gate_logits: bfloat16 [4, 1024, 32], P('dp', 'sp'), may hold values from -6 to 6
- retention_offset: float32 [8, 2], P('sp'), may hold values from 3 to 12
- log_forget_extra: float32 [4, 8, 1024], P('dp', 'sp'), may hold values from -2.76 to 0
- lane_amplifier: float32 [1024], P('sp'), may hold values from 0.1 to 1.9
- output_gate_logits: bfloat16 [4, 1024, 1024], P('dp', 'sp'), may hold values from -6 to 6
- output_projection: bfloat16 [1024, 2048], P(None, 'dp'), may hold values from -0.1875 to 0.1875
- cell_norm_gain: float32 [2048], replicated, may hold values from 0.1 to 1.9
- expert_norm_gain: float32 [2048], replicated, may hold values from 0.1 to 1.9
- expert_index: int32 [4, 1024, 2], P('dp', 'sp'), may hold values from 0 to 31, all different within a row; in each aligned block of 128 rows (0 to 127, 128 to 255, ..., all dimensions but the last counted through in order) at most 16 rows name the same one
- group_mixing_weight: float32 [4, 1024, 4], P('dp', 'sp'), may hold values from 0.05 to 1
- within_group_weight: float32 [4, 1024, 2], P('dp', 'sp'), may hold values from 0.1 to 1
- gate_weight: bfloat16 [32, 2048, 1024], P(('sp', 'dp')), may hold values from -0.125 to 0.125
- up_weight: bfloat16 [32, 2048, 1024], P(('sp', 'dp')), may hold values from -0.125 to 0.125
- down_weight: bfloat16 [32, 1024, 2048], P(('sp', 'dp')), may hold values from -0.75 to 0.75
Outputs:
- stream_out: bfloat16 [4, 1024, 2048], P('dp', 'sp')
The draws below stay inside these ranges and needn't reach their ends.
Inputs may be any that keep to these rules, and one draw needn't show every extreme that they name: `expert_index`: A token's two experts differ; among the 128 tokens of one device no expert is named more than 16 times, a bound that some block reaches.
All inputs are finite; a program needn't handle non-finite values.
Results may differ from the reference program's by a relative error of at most 0.0095.
Values may be sent and summed in bfloat16 or wider, within the bound.
A program may use at most 128 MiB of HBM per device.

```python
import math
from functools import partial
import jax
import jax.numpy as jnp
import numpy as np
from jax import lax

D = 2048
DK = 64
CONTENT_WIDTH = 128
ATTENTION_LANES = 8
W_A = 1024
FF = 1024
GROUPS = 4
EXPERTS = 32
SPAN_STEPS = 512
T_DEV = 128
SEQS = 4
LEN = 1024
TOKENS = 4096
CAP = 16


def draw_log_forget_extra(key, part):
    first_key, second_key = jax.random.split(jax.random.fold_in(key, 17))
    places = jax.random.randint(first_key, (SEQS, ATTENTION_LANES, 4), 0, LEN)
    depth = jax.random.uniform(second_key, (SEQS, ATTENTION_LANES, 4), jnp.float32, 0.22, 0.69)
    positions = jnp.arange(LEN, dtype=jnp.int32)
    struck = places[:, :, :, None] == positions[None, None, None, :]
    return -jnp.sum(jnp.where(struck, depth[:, :, :, None], 0.0), axis=2).astype(jnp.float32)


def steps_of(own_key, extent, shards, smallest, largest):
    factor_of, own = 1.0, jax.random.fold_in(own_key, 6)
    for position, parts in shards:
        heights = jnp.exp(jax.random.uniform(jax.random.fold_in(own, position), (parts,), jnp.float32, smallest / len(shards), largest / len(shards)))
        factor_of = factor_of * jnp.repeat(heights, extent[position] // parts).reshape([-1 if axis == position else 1 for axis in range(len(extent))])
    return factor_of


def assign_block(key, own, number, rows, number_of, top, limit, skew):
    order = jax.random.permutation(key, number_of)
    heavy_load, ordinary = shares(number_of, rows * top, limit, skew, True), shares(number_of, rows * top, limit, skew, False)
    places = jnp.arange(number_of)

    def named(sizes, offset_by):
        used = int((sizes > 0).sum())
        fixed = max(1, used // 4)
        passed = fixed + (places - fixed + offset_by * (used - fixed)) % max(1, number_of - fixed)
        return jnp.zeros((number_of,), jnp.int32).at[order[jnp.where(places < fixed, places, passed)]].set(jnp.asarray(sizes, jnp.int32))

    sizes = jnp.where(number % 4 == 0, named(heavy_load, number // 4), named(ordinary, number - number // 4 - 1))
    mixed = jax.random.permutation(jax.random.fold_in(own, 3), number_of)
    donor, sink = mixed[0:number_of // 2 * 2:2], mixed[1:number_of // 2 * 2:2]
    slack = jnp.minimum(sizes[donor] - 1, limit - sizes[sink]) // 2
    slack = jnp.where((donor == order[0]) | (sink == order[0]) | (sizes[sink] == 0), 0, jnp.maximum(slack, 0))
    passed = jax.random.randint(jax.random.fold_in(own, 4), (number_of // 2,), 0, 1 << 20) % (slack + 1)
    sizes = sizes.at[donor].add(-passed).at[sink].add(passed)
    items = jnp.searchsorted(jnp.cumsum(sizes), jnp.arange(rows * top), side="right").astype(jnp.int32)
    listing = items.reshape(top, rows).T
    listing = listing[jax.random.permutation(jax.random.fold_in(own, 1), rows)]
    offset_by = jax.random.randint(jax.random.fold_in(own, 2), (rows, 1), 0, top)
    return jnp.take_along_axis(listing, (jnp.arange(top)[None, :] + offset_by) % top, axis=1)


def shares(count, total, bound, lean, full):
    loads = [(1 << 20) // math.isqrt(standing ** lean) + 1 for standing in range(1, count + 1)]
    largest = bound if full else min(bound, max(-(-total // count), total * loads[0] // sum(loads)))
    least = 1 if total - largest >= count - 1 else 0
    counts, spare = [largest] + [least] * (count - 1), total - largest - least * (count - 1)
    while spare > 0:
        movable = [i for i in range(1, count) if counts[i] < largest] or [i for i in range(1, count) if counts[i] < bound]
        pool, remaining = sum([loads[i] for i in movable]), spare
        for i in movable:
            extra = min(bound - counts[i], max(1, remaining * loads[i] // pool), spare)
            counts[i] = counts[i] + extra
            spare = spare - extra
    return np.array(counts)


def normal_values(own_key, extent, deviation, most, shards=(), held_as=jnp.bfloat16):
    factor_of = steps_of(own_key, extent, shards, -0.22, 0.18) if shards else 1.0
    result = jax.random.normal(own_key, extent, jnp.float32) * deviation * factor_of
    return jnp.minimum(jnp.maximum(result, -most), most).astype(held_as)


def setup_inputs(seed: int = 0) -> dict:
    arg_keys = jax.random.split(jax.random.key(seed), 19)
    residual_input = normal_values(arg_keys[0], (SEQS, LEN, D), 1.0, 6.0, ((0, 4), (1, 8)))
    queries = normal_values(arg_keys[1], (SEQS, LEN, ATTENTION_LANES * DK), 1.0, 6.0, ((0, 4), (1, 8)))
    keys = normal_values(arg_keys[2], (SEQS, LEN, ATTENTION_LANES * DK), 1.0, 6.0, ((0, 4), (1, 8)))
    values = normal_values(arg_keys[3], (SEQS, LEN, W_A), 1.0, 6.0, ((0, 4), (1, 8)))
    gate_logits = normal_values(arg_keys[4], (SEQS, LEN, 4 * ATTENTION_LANES), 1.0, 6.0, ((0, 4), (1, 8)))
    retention_offset = jnp.clip(3.0 + 9.0 * jax.random.uniform(arg_keys[5], (ATTENTION_LANES, 2), jnp.float32) ** steps_of(arg_keys[5], (ATTENTION_LANES, 2), ((0, 8),), -0.2, 0.2), 3.0, 12.0)
    log_forget_extra = draw_log_forget_extra(jax.random.fold_in(arg_keys[18], 71), 0)
    lane_amplifier = jnp.clip(1.0 + 0.18 * jax.random.normal(arg_keys[7], (W_A,), jnp.float32), 0.1, 1.9)
    output_gate_logits = normal_values(arg_keys[8], (SEQS, LEN, W_A), 1.0, 6.0, ((0, 4), (1, 8)))
    output_projection = normal_values(arg_keys[9], (W_A, D), W_A ** -0.5, 0.1875, ((1, 4),))
    cell_norm_gain = jnp.clip(1.0 + 0.18 * jax.random.normal(arg_keys[10], (D,), jnp.float32), 0.1, 1.9)
    expert_norm_gain = jnp.clip(1.0 + 0.18 * jax.random.normal(arg_keys[11], (D,), jnp.float32), 0.1, 1.9)
    expert_index_keys = jax.random.split(jax.random.fold_in(arg_keys[12], 1), SEQS * LEN // T_DEV)
    expert_index_turns = jax.random.permutation(jax.random.fold_in(arg_keys[12], 3), SEQS * LEN // T_DEV)
    expert_index = jax.vmap(lambda own, number: assign_block(jax.random.fold_in(arg_keys[12], 2), own, number, T_DEV, EXPERTS, 2, CAP, 2))(expert_index_keys, expert_index_turns).reshape((SEQS, LEN, 2))
    group_mixing_weight = jnp.clip(0.05 + 0.95 * jax.random.uniform(arg_keys[13], (SEQS, LEN, GROUPS), jnp.float32) ** steps_of(arg_keys[13], (SEQS, LEN, GROUPS), ((0, 4), (1, 8)), -0.2, 0.2), 0.05, 1.0)
    within_group_weight = jnp.clip(0.1 + 0.9 * jax.random.uniform(arg_keys[14], (SEQS, LEN, 2), jnp.float32) ** steps_of(arg_keys[14], (SEQS, LEN, 2), ((0, 4), (1, 8)), -0.2, 0.2), 0.1, 1.0)
    gate_weight = normal_values(arg_keys[15], (EXPERTS, D, FF), D ** -0.5, 0.125, ((0, 32),))
    up_weight = normal_values(arg_keys[16], (EXPERTS, D, FF), D ** -0.5, 0.125, ((0, 32),))
    down_weight = normal_values(arg_keys[17], (EXPERTS, FF, D), (FF // 16) ** -0.5, 0.75, ((0, 32),))
    return dict(residual_input=residual_input, queries=queries, keys=keys, values=values, gate_logits=gate_logits, retention_offset=retention_offset, log_forget_extra=log_forget_extra, lane_amplifier=lane_amplifier, output_gate_logits=output_gate_logits, output_projection=output_projection, cell_norm_gain=cell_norm_gain, expert_norm_gain=expert_norm_gain, expert_index=expert_index, group_mixing_weight=group_mixing_weight, within_group_weight=within_group_weight, gate_weight=gate_weight, up_weight=up_weight, down_weight=down_weight)


EPS = 1e-06
HIGH_PRECISION = lax.Precision.HIGHEST

def block_states(keys_f, values_f, in_gate, log_forget, span_steps):
    length, key_width = keys_f.shape
    blocks = length // span_steps
    blocked_keys = keys_f.reshape(blocks, span_steps, key_width)
    blocked_values = values_f.reshape(blocks, span_steps, values_f.shape[1])
    running = jnp.cumsum(log_forget.reshape(blocks, span_steps), axis=1)
    block_end = running[:, -1]
    weight_log = block_end[:, None] - running + in_gate.reshape(blocks, span_steps)
    local_top = lax.optimization_barrier(jnp.max(weight_log, axis=1))
    weight_table = jnp.exp(weight_log - local_top[:, None])
    local_memory = jnp.einsum('ryd,rya->rda', blocked_values * weight_table[:, :, None], blocked_keys, precision=HIGH_PRECISION)
    local_normalizer = jnp.einsum('nb,nby->ny', weight_table, blocked_keys, precision=HIGH_PRECISION)

    def advance(carried_state, inputs):
        memory, normal, stable = carried_state
        end_log, top_log, memory_new, normal_new = inputs
        raised = jnp.maximum(end_log + stable, top_log)
        keep_old = jnp.exp(end_log + stable - raised)
        keep_new = jnp.exp(top_log - raised)
        updated = (keep_old * memory + keep_new * memory_new, keep_old * normal + keep_new * normal_new, raised)
        return (updated, (memory, normal, stable))
    initial = (jnp.zeros((values_f.shape[1], key_width), jnp.float32), jnp.zeros((key_width,), jnp.float32), jnp.zeros((), jnp.float32))
    _, entries = lax.scan(advance, initial, (block_end, local_top, local_memory, local_normalizer))
    return entries

def direction_out(query_f, keys_f, values_f, in_gate, log_forget, span_steps):
    entry_memory, entry_normal, entry_top = block_states(keys_f, values_f, in_gate, log_forget, span_steps)
    length, key_width = keys_f.shape
    blocks = length // span_steps
    query_blocks = query_f.reshape(blocks, span_steps, key_width) * key_width ** (-0.5)
    blocked_keys = keys_f.reshape(blocks, span_steps, key_width)
    blocked_values = values_f.reshape(blocks, span_steps, values_f.shape[1])
    running = jnp.cumsum(log_forget.reshape(blocks, span_steps), axis=1)
    entry_log = running + entry_top[:, None]
    pair_log = running[:, :, None] - running[:, None, :] + in_gate.reshape(blocks, span_steps)[:, None, :]
    earlier = jnp.tril(jnp.ones((span_steps, span_steps), dtype=bool))
    pair_log = jnp.where(earlier[None], pair_log, -jnp.inf)
    top_log = jnp.maximum(entry_log, lax.optimization_barrier(jnp.max(pair_log, axis=2)))
    scores = jnp.einsum('ctk,csk->cts', query_blocks, blocked_keys, precision=HIGH_PRECISION) * jnp.exp(pair_log - top_log[:, :, None])
    carried = jnp.exp(entry_log - top_log)
    numerator = carried[:, :, None] * jnp.einsum('cvk,ctk->ctv', entry_memory, query_blocks, precision=HIGH_PRECISION)
    numerator = numerator + jnp.einsum('cts,csv->ctv', scores, blocked_values, precision=HIGH_PRECISION)
    denominator = carried * jnp.einsum('ck,ctk->ct', entry_normal, query_blocks, precision=HIGH_PRECISION) + lax.optimization_barrier(jnp.sum(scores, axis=2))
    output = numerator / jnp.maximum(jnp.abs(denominator), jnp.exp(-top_log))[:, :, None]
    return output.reshape(length, blocked_values.shape[2])

def lane_blend(lane_question, lane_addresses, lane_contents, lane_switches, lane_offset, lane_spread, lane_rescaling, span_steps):
    query_f = lane_question.astype(jnp.float32)
    keys_f = lane_addresses.astype(jnp.float32)
    values_f = lane_contents.astype(jnp.float32)
    retention_entries = lane_switches.astype(jnp.float32)
    onward_fading = jax.nn.log_sigmoid(retention_entries[:, 1] + lane_offset[0]) + lane_spread
    reverse_fading = jax.nn.log_sigmoid(retention_entries[:, 3] + lane_offset[1]) + lane_spread
    forward = direction_out(query_f, keys_f, values_f, retention_entries[:, 0], onward_fading, span_steps)
    backward = direction_out(query_f[::-1], keys_f[::-1], values_f[::-1], retention_entries[::-1, 2], reverse_fading[::-1], span_steps)[::-1]
    total = forward + backward
    normed = total * lax.rsqrt(lax.optimization_barrier(jnp.mean(total * total, axis=1, keepdims=True)) + EPS) * lane_rescaling
    return normed.astype(jnp.bfloat16)

def series_blender(series_question, series_addresses, series_contents, series_switches, series_spread, retention_offset, lane_amplifier):
    lane_question = series_question.reshape(LEN, ATTENTION_LANES, DK).transpose(1, 0, 2)
    lane_addresses = series_addresses.reshape(LEN, ATTENTION_LANES, DK).transpose(1, 0, 2)
    lane_contents = series_contents.reshape(LEN, ATTENTION_LANES, CONTENT_WIDTH).transpose(1, 0, 2)
    lane_switches = series_switches.reshape(LEN, ATTENTION_LANES, 4).transpose(1, 0, 2)
    return jax.vmap(partial(lane_blend, span_steps=SPAN_STEPS))(lane_question, lane_addresses, lane_contents, lane_switches, retention_offset, series_spread, lane_amplifier.reshape(ATTENTION_LANES, CONTENT_WIDTH))

def reference(residual_input, queries, keys, values, gate_logits, retention_offset, log_forget_extra, lane_amplifier, output_gate_logits, output_projection, cell_norm_gain, expert_norm_gain, expert_index, group_mixing_weight, within_group_weight, gate_weight, up_weight, down_weight):
    mixed_output = lax.map(lambda packed_rows: series_blender(packed_rows[0], packed_rows[1], packed_rows[2], packed_rows[3], packed_rows[4], retention_offset, lane_amplifier), (queries, keys, values, gate_logits, log_forget_extra))
    mixed_output = mixed_output.transpose(0, 2, 1, 3).reshape(TOKENS, W_A)
    gated = (mixed_output.astype(jnp.float32) * jax.nn.sigmoid(output_gate_logits.reshape(TOKENS, W_A).astype(jnp.float32))).astype(jnp.bfloat16)
    proj = jnp.dot(gated, output_projection, preferred_element_type=jnp.float32)
    stream_f = residual_input.reshape(TOKENS, D).astype(jnp.float32)
    stream = (stream_f + cell_norm_gain * proj * lax.rsqrt(lax.optimization_barrier(jnp.mean(proj * proj, axis=1, keepdims=True)) + EPS)).astype(jnp.bfloat16)
    stream_f = stream.astype(jnp.float32)
    moe_in = (expert_norm_gain * stream_f * lax.rsqrt(lax.optimization_barrier(jnp.mean(stream_f * stream_f, axis=1, keepdims=True)) + EPS)).astype(jnp.bfloat16)
    dev_blocks = TOKENS // T_DEV
    flat_ids = expert_index.reshape(TOKENS * 2)
    block_ids = flat_ids.reshape(dev_blocks, T_DEV * 2)
    onehot = (block_ids[:, :, None] == jnp.arange(EXPERTS, dtype=jnp.int32)[None, None, :]).astype(jnp.int32)
    slot_index = lax.optimization_barrier(jnp.sum((jnp.cumsum(onehot, axis=1) - onehot) * onehot, axis=2))
    column = (jnp.arange(dev_blocks, dtype=jnp.int32)[:, None] * CAP + slot_index).reshape(TOKENS * 2).astype(jnp.int32)
    token_of = (jnp.arange(TOKENS * 2, dtype=jnp.int32) // 2).astype(jnp.int32)
    group_of = expert_index.reshape(TOKENS, 2) // (EXPERTS // GROUPS)
    group_hit = (group_of[:, :, None] == jnp.arange(GROUPS, dtype=jnp.int32)[None, None, :]).astype(jnp.float32)
    chosen_group = lax.optimization_barrier(jnp.sum(group_mixing_weight.reshape(TOKENS, 1, GROUPS) * group_hit, axis=2))
    route = (chosen_group * within_group_weight.reshape(TOKENS, 2)).reshape(TOKENS * 2)
    table = jnp.full((EXPERTS, dev_blocks * CAP), TOKENS, jnp.int32).at[flat_ids, column].set(token_of)
    share = jnp.zeros((EXPERTS, dev_blocks * CAP), jnp.float32).at[flat_ids, column].set(route)
    padded = jnp.concatenate([moe_in, jnp.zeros((1, D), jnp.bfloat16)], axis=0)

    def expert_pass(total, inputs):
        rows_index, rows_share, gate_w, up_w, down_w = inputs
        picked = padded[rows_index]
        hidden = (jax.nn.silu(jnp.dot(picked, gate_w, preferred_element_type=jnp.float32)) * jnp.dot(picked, up_w, preferred_element_type=jnp.float32)).astype(jnp.bfloat16)
        produced = jnp.dot(hidden, down_w, preferred_element_type=jnp.float32).astype(jnp.bfloat16)
        return (total.at[rows_index].add(rows_share[:, None] * produced.astype(jnp.float32)), None)
    total, _ = lax.scan(expert_pass, jnp.zeros((TOKENS + 1, D), jnp.float32), (table, share, gate_weight, up_weight, down_weight))
    stream_out = (stream_f + total[:TOKENS]).astype(jnp.bfloat16)
    return stream_out.reshape(SEQS, LEN, D)
```

```python
from functools import partial

import jax
import jax.numpy as jnp
from jax import lax
from jax.experimental import pallas as pl
from jax.experimental.pallas import tpu as pltpu
from jax.sharding import PartitionSpec as P

EPS = 1e-06
MESH = pl.DeviceIdType.MESH
GATE_ROWS = 16
PARTS = 4
FF_TILE = 256
PIECES = 4


def log_sigmoid(x):
    return jnp.minimum(x, 0.0) - jnp.log1p(jnp.exp(-jnp.abs(x)))


def layer_kernel(*refs, n, dpn, inputs):
    hbm, (out_ref,), rest = refs[:inputs], refs[inputs : inputs + 1], refs[inputs + 1 :]
    local, rest = rest[:inputs], rest[inputs:]
    (
        q_ref, k_ref, v_ref, g_ref, offset_ref, extra_ref, amp_ref, logits_ref, w_ref,
        res_ref, cell_gain_ref, expert_gain_ref, index_ref, group_ref, within_ref,
        gate_ref, up_ref, down_ref,
    ) = local
    (
        send, recv, gates_t, cols, mixed, mrecv, wfull, proj,
        meta, table_t, table_hi, table_lo, line, outgoing, incoming, hs, produced, returned,
        partial_out, partial_in, total,
        in_sem, send_sem, recv_sem, msend_sem, mrecv_sem, wx_send, wx_recv, wc_send, wc_recv,
        wl_sem, meta_send, meta_recv, up_send, down_send, line_recv,
        out_send, out_recv, back_send, back_recv, part_send, part_recv,
    ) = rest
    loads = [pltpu.make_async_copy(hbm[i], local[i], in_sem.at[i]) for i in range(inputs)]
    for load in loads:
        load.start()
    tok = q_ref.shape[1]
    dk = q_ref.shape[2] // n
    dv = v_ref.shape[2] // n
    length = n * tok
    wcol = w_ref.shape[1]
    me = lax.axis_index("sp")
    my_dp = lax.axis_index("dp")
    my_x, my_core = my_dp // 2, my_dp % 2
    chips = dpn // 2

    barrier = pltpu.get_barrier_semaphore()

    devices = n * dpn
    cap = 4 * tok // devices
    ny = chips if n % chips == 0 else 1
    nz = n // ny
    plane = ny * dpn
    my_z, my_y = me // ny, me % ny
    my_q = my_y * dpn + my_dp

    def device(z, q):
        return {"sp": z * ny + q // dpn, "dp": q % dpn}

    def greet_sp(o, _):
        pl.semaphore_signal(
            barrier, inc=1, device_id={"sp": (me + o) % n, "dp": my_dp}, device_id_type=MESH
        )
        return 0

    def greet_plane(o, _):
        pl.semaphore_signal(
            barrier, inc=1, device_id=device(my_z, (my_q + o) % plane), device_id_type=MESH
        )
        return 0

    lax.fori_loop(1, n, greet_sp, 0)
    lax.fori_loop(1, plane, greet_plane, 0)
    for load in loads[:4]:
        load.wait()

    for h in range(n):
        send[h, 0:tok, 0:dk] = k_ref[0, :, h * dk : (h + 1) * dk]
        send[h, 0:tok, dk : 2 * dk] = q_ref[0, :, h * dk : (h + 1) * dk]
        send[h, 0:tok, 2 * dk : 2 * dk + dv] = v_ref[0, :, h * dv : (h + 1) * dv]
    g = g_ref[0].astype(jnp.float32)
    g = jnp.concatenate([g, jnp.zeros((tok, 128 - g.shape[1]), jnp.float32)], axis=1)
    gates_t[...] = g.T
    for h in range(n):
        send[h, tok : tok + GATE_ROWS, 0:tok] = gates_t[4 * h : 4 * h + GATE_ROWS, :].astype(
            jnp.bfloat16
        )
        send[h, tok : tok + GATE_ROWS, tok:] = jnp.zeros(
            (GATE_ROWS, send.shape[2] - tok), jnp.bfloat16
        )

    pl.semaphore_wait(barrier, n - 1 + plane - 1)

    def qkv_copy(o):
        return pltpu.make_async_remote_copy(
            src_ref=send.at[(me + o) % n],
            dst_ref=recv.at[me],
            send_sem=send_sem.at[o],
            recv_sem=recv_sem.at[o],
            device_id={"sp": (me + o) % n, "dp": my_dp},
            device_id_type=MESH,
        )

    def qkv_arrival(o):
        return pltpu.make_async_remote_copy(
            src_ref=send.at[(me + o) % n],
            dst_ref=recv.at[(me + n - o) % n],
            send_sem=send_sem.at[o],
            recv_sem=recv_sem.at[o],
            device_id={"sp": (me + o) % n, "dp": my_dp},
            device_id_type=MESH,
        )

    piece = w_ref.shape[0] // PIECES

    def wx_copy(o, p, slot):
        return pltpu.make_async_remote_copy(
            src_ref=w_ref.at[pl.ds(p * piece, piece)],
            dst_ref=wfull.at[slot, pl.ds(p * piece, piece)],
            send_sem=wx_send.at[o, p],
            recv_sem=wx_recv.at[o, p],
            device_id={"sp": me, "dp": ((my_x + o) % chips) * 2 + my_core},
            device_id_type=MESH,
        )

    def wc_copy(o, p, src, slot):
        return pltpu.make_async_remote_copy(
            src_ref=src.at[pl.ds(p * piece, piece)],
            dst_ref=wfull.at[slot, pl.ds(p * piece, piece)],
            send_sem=wc_send.at[o, p],
            recv_sem=wc_recv.at[o, p],
            device_id={"sp": me, "dp": my_x * 2 + 1 - my_core},
            device_id_type=MESH,
        )

    def from_chip(o):
        return ((my_x + chips - o) % chips) * 2 + my_core

    def pass_on(p):
        for o in range(1, chips):
            slot = from_chip(o)
            wx_copy(o, p, slot).wait_recv()
            wc_copy(o, p, wfull.at[slot], slot).start()

    for o in range(1, n):
        qkv_copy(o).start()
    loads[8].wait()
    for p in range(PIECES):
        for o in range(1, chips):
            wx_copy(o, p, my_dp).start()
        wc_copy(0, p, w_ref, my_dp).start()
    own_w = pltpu.make_async_copy(w_ref, wfull.at[my_dp], wl_sem)
    own_w.start()
    recv[me] = send[me]
    for i in (4, 5, 6, 7, 9, 10, 11, 12, 13, 14):
        loads[i].wait()

    rows_in = plane * cap
    ids = index_ref[0].astype(jnp.float32)
    e_0, e_1 = ids[:, 0:1], ids[:, 1:2]
    wide = -(-devices // 128) * 128
    lane_e = lax.broadcasted_iota(jnp.int32, (tok, wide), 1).astype(jnp.float32)
    hit_0 = jnp.where(lane_e == e_0, 1.0, 0.0)
    hit_1 = jnp.where(lane_e == e_1, 1.0, 0.0)
    tri = jnp.where(
        lax.broadcasted_iota(jnp.int32, (tok, tok), 1)
        < lax.broadcasted_iota(jnp.int32, (tok, tok), 0),
        1.0,
        0.0,
    ).astype(jnp.bfloat16)
    rank_0 = jnp.dot(tri, hit_0.astype(jnp.bfloat16), preferred_element_type=jnp.float32)
    rank_1 = jnp.dot(tri, hit_1.astype(jnp.bfloat16), preferred_element_type=jnp.float32)
    rank_1 = rank_1 + jnp.sum(hit_0, axis=0, keepdims=True)
    place_0 = e_0 * cap + jnp.sum(hit_0 * rank_0, axis=1, keepdims=True)
    place_1 = e_1 * cap + jnp.sum(hit_1 * rank_1, axis=1, keepdims=True)
    groups = group_ref.shape[2]
    span = devices // groups
    route_0 = jnp.zeros((tok, 1), jnp.float32)
    route_1 = jnp.zeros((tok, 1), jnp.float32)
    for c in range(groups):
        weight_c = group_ref[0, :, c : c + 1]
        route_0 += jnp.where((e_0 >= c * span) & (e_0 < (c + 1) * span), weight_c, 0.0)
        route_1 += jnp.where((e_1 >= c * span) & (e_1 < (c + 1) * span), weight_c, 0.0)
    route_0 = route_0 * within_ref[0, :, 0:1]
    route_1 = route_1 * within_ref[0, :, 1:2]
    lane_t = lax.broadcasted_iota(jnp.int32, (tok, 128), 1)
    packed = jnp.where(
        lane_t == 0, place_0, jnp.where(lane_t == 1, place_1, jnp.where(lane_t == 2, route_0, route_1))
    )
    meta[my_z] = packed.T[0:8]

    def meta_copy(z, slot):
        return pltpu.make_async_remote_copy(
            src_ref=meta.at[my_z],
            dst_ref=meta.at[slot],
            send_sem=meta_send.at[z],
            recv_sem=meta_recv.at[slot],
            device_id=device(z, my_q),
            device_id_type=MESH,
        )

    for o in range(1, nz):
        meta_copy((my_z + o) % nz, my_z).start()

    for o in range(1, n):
        qkv_arrival(o).wait_recv()

    gates = jnp.concatenate(
        [recv[d, tok : tok + GATE_ROWS, 0:tok].astype(jnp.float32) for d in range(n)], axis=1
    )
    extra = extra_ref[0]
    f = log_sigmoid(gates[1:2] + offset_ref[0:1, 0:1]) + extra
    b = log_sigmoid(gates[3:4] + offset_ref[0:1, 1:2]) + extra
    f = jnp.broadcast_to(f, (8, length))
    b = jnp.broadcast_to(b, (8, length))
    lane = lax.broadcasted_iota(jnp.int32, (8, length), 1)
    step = 1
    while step < length:
        f = f + jnp.where(lane >= step, pltpu.roll(f, step, 1), 0.0)
        b = b + jnp.where(lane < length - step, pltpu.roll(b, length - step, 1), 0.0)
        step *= 2
    row_i = gates[0:1]
    row_f = row_i - f[0:1]
    row_b = gates[2:3] - b[0:1]
    sub = lax.broadcasted_iota(jnp.int32, (128, length), 0)
    stacked = jnp.where(sub == 0, f[0:1], jnp.where(sub == 1, b[0:1], row_i))
    cols[...] = stacked.T

    scale = dk ** (-0.5)
    amp = amp_ref[...]

    def mixed_copy(o, slot):
        return pltpu.make_async_remote_copy(
            src_ref=mixed.at[(me + o) % n],
            dst_ref=mrecv.at[slot],
            send_sem=msend_sem.at[o],
            recv_sem=mrecv_sem.at[o],
            device_id={"sp": (me + o) % n, "dp": my_dp},
            device_id_type=MESH,
        )

    def segment(j, _):
        d = (me + 1 + j) % n
        start = pl.multiple_of(d * tok, tok)
        kq = recv[d, 0:tok, 0 : 2 * dk]
        qs = kq[:, dk:].astype(jnp.float32) * scale
        ks = kq[:, :dk].astype(jnp.float32)
        diag = jnp.sum(qs * ks, axis=1, keepdims=True)
        qs = jnp.concatenate([qs, jnp.zeros_like(qs)], axis=1).astype(jnp.bfloat16)
        kall = recv[:, 0:tok, 0 : 2 * dk].reshape(length, 2 * dk)
        vall = recv[:, 0:tok, 2 * dk : 2 * dk + dv].reshape(length, dv)
        scores = lax.dot_general(
            qs, kall, (((1,), (1,)), ((), ())), preferred_element_type=jnp.float32
        )
        col = cols[pl.ds(start, tok), :]
        col_f, col_b, col_i = col[:, 0:1], col[:, 1:2], col[:, 2:3]
        t_pos = start + lax.broadcasted_iota(jnp.int32, (tok, length), 0)
        s_pos = lax.broadcasted_iota(jnp.int32, (tok, length), 1)
        before = s_pos < t_pos
        weight = scores * jnp.exp(jnp.where(before, col_f + row_f, col_b + row_b))
        diag = diag * jnp.exp(col_i)
        z_f = jnp.sum(jnp.where(before, weight, 0.0), axis=1, keepdims=True) + diag
        z_b = jnp.sum(jnp.where(before, 0.0, weight), axis=1, keepdims=True)
        inv_f = 1.0 / jnp.maximum(jnp.abs(z_f), 1.0)
        inv_b = 1.0 / jnp.maximum(jnp.abs(z_b), 1.0)
        probs = (weight * jnp.where(before, inv_f, inv_b)).astype(jnp.bfloat16)
        total = jnp.dot(probs, vall, preferred_element_type=jnp.float32)
        total = total + (diag * inv_f) * recv[d, 0:tok, 2 * dk : 2 * dk + dv].astype(jnp.float32)
        total = total * lax.rsqrt(jnp.mean(total * total, axis=1, keepdims=True) + EPS) * amp
        mixed[d] = total.astype(jnp.bfloat16)

        @pl.when(j >= 1)
        def _():
            mixed_copy(j, me).start()

        @pl.when(j == n // 2)
        def _():
            pass_on(PIECES - 2)

        return 0

    for p in range(PIECES - 2):
        pass_on(p)
    lax.fori_loop(0, n, segment, 0)
    pass_on(PIECES - 1)
    mrecv[me] = mixed[me]
    sub_r = lax.broadcasted_iota(jnp.int32, (rows_in, tok), 0).astype(jnp.float32)
    at = sub_r + (my_z * rows_in).astype(jnp.float32)

    def tables(o, _):
        z = (my_z + o) % nz

        @pl.when(o > 0)
        def _():
            meta_copy(z, z).wait_recv()

        rows = meta[z]
        hit_0, hit_1 = at == rows[0:1], at == rows[1:2]
        table_t[z] = (jnp.where(hit_0, 1.0, 0.0) + jnp.where(hit_1, 1.0, 0.0)).astype(jnp.bfloat16)
        weighted = (jnp.where(hit_0, rows[2:3], 0.0) + jnp.where(hit_1, rows[3:4], 0.0)).T
        high = weighted.astype(jnp.bfloat16)
        table_hi[z] = high
        table_lo[z] = (weighted - high.astype(jnp.float32)).astype(jnp.bfloat16)
        return 0

    lax.fori_loop(0, nz, tables, 0)
    sig = jax.nn.sigmoid(logits_ref[0].astype(jnp.float32))
    for o in range(1, n):
        mixed_copy(o, (me + n - o) % n).wait_recv()
    gated = jnp.concatenate([mrecv[h].astype(jnp.float32) for h in range(n)], axis=1) * sig
    gated = gated.astype(jnp.bfloat16)
    own_w.wait()
    partner = 1 - my_core
    for p in range(PIECES):
        wc_copy(0, p, w_ref, my_x * 2 + partner).wait_recv()
        for o in range(1, chips):
            slot = ((my_x + chips - o) % chips) * 2 + partner
            wc_copy(o, p, wfull.at[slot], slot).wait_recv()
    for j in range(dpn):
        proj[:, j * wcol : (j + 1) * wcol] = jnp.dot(
            gated, wfull[j], preferred_element_type=jnp.float32
        )
    p = proj[...]
    stream = (
        res_ref[0].astype(jnp.float32)
        + cell_gain_ref[...] * p * lax.rsqrt(jnp.mean(p * p, axis=1, keepdims=True) + EPS)
    ).astype(jnp.bfloat16)
    s = stream.astype(jnp.float32)
    width = s.shape[1]
    part = width // PARTS
    moe = (
        expert_gain_ref[...] * s * lax.rsqrt(jnp.mean(s * s, axis=1, keepdims=True) + EPS)
    ).astype(jnp.bfloat16)

    def line_copy(z, p, to, sems):
        return pltpu.make_async_remote_copy(
            src_ref=line.at[z, p],
            dst_ref=line.at[z, p],
            send_sem=sems.at[z, p],
            recv_sem=line_recv.at[z, p],
            device_id=device(to, my_q),
            device_id_type=MESH,
        )

    above, below = (my_z + 1) % nz, (my_z + nz - 1) % nz
    has_above, has_below = my_z + 1 < nz, my_z > 0
    edge = (my_z == 0) | (my_z == nz - 1)

    def spread(z, p):
        @pl.when((z <= my_z) & has_above)
        def _():
            line_copy(z, p, above, up_send).start()

        @pl.when((z >= my_z) & has_below)
        def _():
            line_copy(z, p, below, down_send).start()

    for p in range(PARTS):
        line[my_z, p] = moe[:, p * part : (p + 1) * part]
        spread(my_z, p)
    for p in range(PARTS):
        total[p] = s[:, p * part : (p + 1) * part]
    for i in (15, 16, 17):
        loads[i].wait()
    ff = hs.shape[1]

    def by_distance(k):
        found = my_z
        for z in range(nz):
            inner = 1 if 2 * z < nz - 1 else -1
            near = sorted(range(nz), key=lambda s: (abs(s - z), -(s - z) * inner))
            for place in range(nz):
                found = jnp.where((my_z == z) & (k == place), near[place], found)
        return found

    def plane_copy(src, dst, sems, z, p, q_to, q_src, q_dst):
        return pltpu.make_async_remote_copy(
            src_ref=src.at[z, p, q_src],
            dst_ref=dst.at[z, p, q_dst],
            send_sem=sems[0].at[z, p],
            recv_sem=sems[1].at[z, p],
            device_id=device(my_z, q_to),
            device_id_type=MESH,
        )

    def plane_send(src, dst, sems, z, p):
        def one(o, _):
            q = (my_q + o) % plane
            plane_copy(src, dst, sems, z, p, q, q, my_q).start()
            return 0

        lax.fori_loop(1, plane, one, 0)
        dst[z, p, my_q] = src[z, p, my_q]

    def plane_all(src, dst, sems, z, p):
        others = pl.ds(0, plane - 1)
        return pltpu.make_async_remote_copy(
            src_ref=src.at[z, p, others],
            dst_ref=dst.at[z, p, others],
            send_sem=sems[0].at[z, p],
            recv_sem=sems[1].at[z, p],
            device_id=device(my_z, (my_q + 1) % plane),
            device_id_type=MESH,
        )

    out_way = (outgoing, incoming, (out_send, out_recv))
    back_way = (produced, returned, (back_send, back_recv))

    def dispatch(k):
        z = by_distance(k)

        def piece(p, _):
            @pl.when(k > 0)
            def _():
                line_copy(z, p, above, up_send).wait_recv()
                spread(z, p)

            block = jnp.dot(table_t[z], line[z, p], preferred_element_type=jnp.float32)
            outgoing[z, p] = block.astype(jnp.bfloat16).reshape(plane, cap, part)
            plane_send(*out_way, z, p)
            return 0

        lax.fori_loop(0, PARTS, piece, 0)

    def expert(k):
        z = by_distance(k)

        def arrive(p, _):
            plane_all(*out_way, z, p).wait_recv()
            return 0

        lax.fori_loop(0, PARTS, arrive, 0)

        def up_tile(t, _):
            at = pl.ds(pl.multiple_of(t * FF_TILE, FF_TILE), FF_TILE)
            x = jnp.concatenate(
                [incoming[z, p].reshape(rows_in, part) for p in range(PARTS)], axis=1
            )
            a = jnp.dot(x, gate_ref[0, :, at], preferred_element_type=jnp.float32)
            u = jnp.dot(x, up_ref[0, :, at], preferred_element_type=jnp.float32)
            hs[:, at] = (jax.nn.silu(a) * u).astype(jnp.bfloat16)
            return 0

        lax.fori_loop(0, ff // FF_TILE, up_tile, 0)

        def down_tile(p, _):
            at = pl.ds(pl.multiple_of(p * part, part), part)
            y = jnp.dot(hs[...], down_ref[0, :, at], preferred_element_type=jnp.float32)
            produced[z, p] = y.astype(jnp.bfloat16).reshape(plane, cap, part)
            plane_send(*back_way, z, p)
            return 0

        lax.fori_loop(0, PARTS, down_tile, 0)

    def partial_copy(z, p):
        to = jnp.where(z < my_z, below, above)
        slot = jnp.where((z > my_z) & (to == z), nz, z)
        return pltpu.make_async_remote_copy(
            src_ref=partial_out.at[z, p],
            dst_ref=partial_in.at[slot, p],
            send_sem=part_send.at[z, p],
            recv_sem=part_recv.at[slot, p],
            device_id=device(to, my_q),
            device_id_type=MESH,
        )

    def partial_arrive(slot, p):
        pltpu.make_async_remote_copy(
            src_ref=partial_out.at[0, p],
            dst_ref=partial_in.at[slot, p],
            send_sem=part_send.at[0, p],
            recv_sem=part_recv.at[slot, p],
            device_id=device(above, my_q),
            device_id_type=MESH,
        ).wait_recv()

    def combine(z, p):
        plane_all(*back_way, z, p).wait_recv()
        block = returned[z, p].reshape(rows_in, part)
        mine = jnp.dot(table_hi[z], block, preferred_element_type=jnp.float32) + jnp.dot(
            table_lo[z], block, preferred_element_type=jnp.float32
        )
        total[PARTS] = mine

        @pl.when(z == my_z)
        def _():
            total[p] += total[PARTS]

        @pl.when(z != my_z)
        def _():
            @pl.when(~edge)
            def _():
                partial_arrive(z, p)
                total[PARTS] += partial_in[z, p].astype(jnp.float32)

            partial_out[z, p] = total[PARTS].astype(jnp.bfloat16)
            partial_copy(z, p).start()

    def tick(t, _):
        @pl.when(t < nz)
        def _():
            dispatch(t)

        e = jnp.where(edge | (t == 0), t, t - 1)

        @pl.when((e < nz) & (edge | (t != 1)))
        def _():
            expert(e)

        c = jnp.where(edge, t, t - nz)

        @pl.when((c >= 0) & (c < nz))
        def _():
            def one(j, _):
                late = max(nz - 2, 1)
                m = jnp.maximum(c * PARTS + j - 2 * PARTS, 0)
                straight = edge | (c < 2)
                k = jnp.where(straight, c, nz - 1 - m % late)
                p = jnp.where(straight, j, m // late)
                combine(by_distance(k), p)
                return 0

            lax.fori_loop(0, PARTS, one, 0)

        return 0

    lax.fori_loop(0, 2 * nz, tick, 0)
    for p in range(PARTS):
        @pl.when(has_above)
        def _():
            partial_arrive(my_z, p)
            total[p] += partial_in[my_z, p].astype(jnp.float32)

        @pl.when(has_below)
        def _():
            partial_arrive(nz, p)
            total[p] += partial_in[nz, p].astype(jnp.float32)

        out_ref[0, :, p * part : (p + 1) * part] = total[p].astype(jnp.bfloat16)

    def drain(i, _):
        z, p = i // PARTS, i % PARTS
        plane_all(*out_way, z, p).wait_send()
        plane_all(*back_way, z, p).wait_send()

        @pl.when((z <= my_z) & has_above)
        def _():
            line_copy(z, p, above, up_send).wait_send()

        @pl.when((z >= my_z) & has_below)
        def _():
            line_copy(z, p, below, down_send).wait_send()

        @pl.when(z != my_z)
        def _():
            partial_copy(z, p).wait_send()

        return 0

    lax.fori_loop(0, nz * PARTS, drain, 0)
    for o in range(1, nz):
        meta_copy((my_z + o) % nz, my_z).wait_send()
    for o in range(1, n):
        qkv_copy(o).wait_send()
        mixed_copy(o, me).wait_send()
    for p in range(PIECES):
        for o in range(1, chips):
            wx_copy(o, p, my_dp).wait_send()
            slot = from_chip(o)
            wc_copy(o, p, wfull.at[slot], slot).wait_send()
        wc_copy(0, p, w_ref, my_dp).wait_send()


def on_device(
    residual_input,
    queries,
    keys,
    values,
    gate_logits,
    retention_offset,
    log_forget_extra,
    lane_amplifier,
    output_gate_logits,
    output_projection,
    cell_norm_gain,
    expert_norm_gain,
    expert_index,
    group_mixing_weight,
    within_group_weight,
    gate_weight,
    up_weight,
    down_weight,
):
    n, dpn = lax.axis_size("sp"), lax.axis_size("dp")
    tok, width = residual_input.shape[1:]
    dk, dv = queries.shape[2] // n, values.shape[2] // n
    length, devices, ff = n * tok, n * dpn, gate_weight.shape[2]
    cap, chips = 4 * tok // devices, dpn // 2
    ny = chips if n % chips == 0 else 1
    nz, plane = n // ny, ny * dpn
    rows_in, part = plane * cap, width // PARTS
    operands = (
        queries, keys, values, gate_logits, retention_offset, log_forget_extra,
        lane_amplifier.reshape(1, dv), output_gate_logits, output_projection,
        residual_input, cell_norm_gain.reshape(1, width), expert_norm_gain.reshape(1, width),
        expert_index, group_mixing_weight, within_group_weight,
        gate_weight, up_weight, down_weight,
    )
    dma = pltpu.SemaphoreType.DMA
    bf16, f32 = jnp.bfloat16, jnp.float32
    hbm = pl.BlockSpec(memory_space=pltpu.HBM)
    return pl.pallas_call(
        partial(layer_kernel, n=n, dpn=dpn, inputs=len(operands)),
        out_shape=jax.ShapeDtypeStruct((1, tok, width), bf16),
        in_specs=[hbm] * len(operands),
        out_specs=pl.BlockSpec(memory_space=pltpu.VMEM),
        scratch_shapes=[pltpu.VMEM(x.shape, x.dtype) for x in operands]
        + [
            pltpu.VMEM((n, tok + GATE_ROWS, 2 * dk + dv), bf16),
            pltpu.VMEM((n, tok + GATE_ROWS, 2 * dk + dv), bf16),
            pltpu.VMEM((128, tok), f32),
            pltpu.VMEM((length, 128), f32),
            pltpu.VMEM((n, tok, dv), bf16),
            pltpu.VMEM((n, tok, dv), bf16),
            pltpu.VMEM((dpn,) + output_projection.shape, bf16),
            pltpu.VMEM((tok, width), f32),
            pltpu.VMEM((nz, 8, tok), f32),
            pltpu.VMEM((nz, rows_in, tok), bf16),
            pltpu.VMEM((nz, tok, rows_in), bf16),
            pltpu.VMEM((nz, tok, rows_in), bf16),
            pltpu.VMEM((nz, PARTS, tok, part), bf16),
            pltpu.VMEM((nz, PARTS, plane, cap, part), bf16),
            pltpu.VMEM((nz, PARTS, plane, cap, part), bf16),
            pltpu.VMEM((rows_in, ff), bf16),
            pltpu.VMEM((nz, PARTS, plane, cap, part), bf16),
            pltpu.VMEM((nz, PARTS, plane, cap, part), bf16),
            pltpu.VMEM((nz, PARTS, tok, part), bf16),
            pltpu.VMEM((nz + 1, PARTS, tok, part), bf16),
            pltpu.VMEM((PARTS + 1, tok, part), f32),
            dma((len(operands),)),
            dma((n,)), dma((n,)), dma((n,)), dma((n,)),
            dma((dpn // 2, PIECES)), dma((dpn // 2, PIECES)),
            dma((dpn // 2, PIECES)), dma((dpn // 2, PIECES)),
            dma(()),
            dma((nz,)), dma((nz,)),
            dma((nz, PARTS)), dma((nz, PARTS)), dma((nz, PARTS)),
            dma((nz, PARTS)), dma((nz, PARTS)), dma((nz, PARTS)), dma((nz, PARTS)),
            dma((nz, PARTS)), dma((nz + 1, PARTS)),
        ],
        compiler_params=pltpu.CompilerParams(
            collective_id=0, has_side_effects=True, vmem_limit_bytes=60 * 1024 * 1024
        ),
    )(*operands)


def solution(mesh):
    in_specs = (
        P("dp", "sp", None),
        P("dp", "sp", None),
        P("dp", "sp", None),
        P("dp", "sp", None),
        P("dp", "sp", None),
        P("sp", None),
        P("dp", "sp", None),
        P("sp"),
        P("dp", "sp", None),
        P(None, "dp"),
        P(),
        P(),
        P("dp", "sp", None),
        P("dp", "sp", None),
        P("dp", "sp", None),
        P(("sp", "dp"), None, None),
        P(("sp", "dp"), None, None),
        P(("sp", "dp"), None, None),
    )
    out_specs = P("dp", "sp", None)
    return jax.shard_map(
        on_device, mesh=mesh, in_specs=in_specs, out_specs=out_specs, check_vma=False
    )
```

```python
from functools import partial

import jax
import jax.numpy as jnp
from jax import lax
from jax.experimental import pallas as pl
from jax.experimental.pallas import tpu as pltpu
from jax.sharding import PartitionSpec as P

EPS = 1e-06
MESH = pl.DeviceIdType.MESH
GATE_ROWS = 16
PARTS = 4
FF_TILE = 256
PIECES = 8


def log_sigmoid(x):
    return jnp.minimum(x, 0.0) - jnp.log1p(jnp.exp(-jnp.abs(x)))


def layer_kernel(*refs, n, dpn, inputs):
    hbm, (out_ref,), rest = refs[:inputs], refs[inputs : inputs + 1], refs[inputs + 1 :]
    local, rest = rest[:inputs], rest[inputs:]
    (
        q_ref, k_ref, v_ref, g_ref, offset_ref, extra_ref, amp_ref, logits_ref, w_ref,
        res_ref, cell_gain_ref, expert_gain_ref, index_ref, group_ref, within_ref,
        gate_ref, up_ref, down_ref,
    ) = local
    (
        send, recv, gates_t, cols, mixed, mrecv, wfull, proj,
        meta, table_t, table_hi, table_lo, line, outgoing, incoming, hs, produced, returned,
        partial_out, partial_in, total,
        in_sem, send_sem, recv_sem, msend_sem, mrecv_sem, wx_send, wx_recv, wy_send, wc_send,
        wc_recv, wl_sem, meta_send, meta_recv, up_send, down_send, line_recv,
        out_send, out_recv, back_send, back_recv, part_send, part_recv,
    ) = rest
    loads = [pltpu.make_async_copy(hbm[i], local[i], in_sem.at[i]) for i in range(inputs)]
    early = (0, 1, 2, 3, 8)
    for i in early:
        loads[i].start()
    tok = q_ref.shape[1]
    dk = q_ref.shape[2] // n
    dv = v_ref.shape[2] // n
    length = n * tok
    wcol = w_ref.shape[1]
    me = lax.axis_index("sp")
    my_dp = lax.axis_index("dp")
    my_x, my_core = my_dp // 2, my_dp % 2
    chips = dpn // 2

    barrier = pltpu.get_barrier_semaphore()

    devices = n * dpn
    cap = 4 * tok // devices
    ny = chips if n % chips == 0 else 1
    nz = n // ny
    plane = ny * dpn
    my_z, my_y = me // ny, me % ny
    my_q = my_y * dpn + my_dp

    def device(z, q):
        return {"sp": z * ny + q // dpn, "dp": q % dpn}

    def greet_sp(o, _):
        pl.semaphore_signal(
            barrier, inc=1, device_id={"sp": (me + o) % n, "dp": my_dp}, device_id_type=MESH
        )
        return 0

    def greet_plane(o, _):
        pl.semaphore_signal(
            barrier, inc=1, device_id=device(my_z, (my_q + o) % plane), device_id_type=MESH
        )
        return 0

    lax.fori_loop(1, n, greet_sp, 0)
    lax.fori_loop(1, plane, greet_plane, 0)
    for load in loads[:4]:
        load.wait()

    for h in range(n):
        send[h, 0:tok, 0:dk] = k_ref[0, :, h * dk : (h + 1) * dk]
        send[h, 0:tok, dk : 2 * dk] = q_ref[0, :, h * dk : (h + 1) * dk]
        send[h, 0:tok, 2 * dk : 2 * dk + dv] = v_ref[0, :, h * dv : (h + 1) * dv]
    gate_rows = g_ref.shape[1]
    gates_t[0:gate_rows] = g_ref[0].astype(jnp.float32)
    gates_t[gate_rows:] = jnp.zeros((128 - gate_rows, tok), jnp.float32)
    for h in range(n):
        send[h, tok : tok + GATE_ROWS, 0:tok] = gates_t[4 * h : 4 * h + GATE_ROWS, :].astype(
            jnp.bfloat16
        )
        send[h, tok : tok + GATE_ROWS, tok:] = jnp.zeros(
            (GATE_ROWS, send.shape[2] - tok), jnp.bfloat16
        )

    pl.semaphore_wait(barrier, n - 1 + plane - 1)
    for i in range(inputs):
        if i not in early:
            loads[i].start()

    def qkv_copy(o):
        return pltpu.make_async_remote_copy(
            src_ref=send.at[(me + o) % n],
            dst_ref=recv.at[me],
            send_sem=send_sem.at[o],
            recv_sem=recv_sem.at[o],
            device_id={"sp": (me + o) % n, "dp": my_dp},
            device_id_type=MESH,
        )

    def qkv_arrival(o):
        return pltpu.make_async_remote_copy(
            src_ref=send.at[(me + o) % n],
            dst_ref=recv.at[(me + n - o) % n],
            send_sem=send_sem.at[o],
            recv_sem=recv_sem.at[o],
            device_id={"sp": (me + o) % n, "dp": my_dp},
            device_id_type=MESH,
        )

    piece = w_ref.shape[0] // PIECES

    share = PIECES // ny
    first_piece = my_y * share

    def rows_of(p):
        return pl.ds(pl.multiple_of(p * piece, piece), piece)

    def wx_copy(o, p):
        return pltpu.make_async_remote_copy(
            src_ref=w_ref.at[rows_of(p)],
            dst_ref=wfull.at[my_dp, rows_of(p)],
            send_sem=wx_send.at[o, p],
            recv_sem=wx_recv.at[o, p],
            device_id={"sp": me, "dp": ((my_x + o) % chips) * 2 + my_core},
            device_id_type=MESH,
        )

    def from_chip(o):
        return ((my_x + chips - o) % chips) * 2 + my_core

    def wy_copy(o, p, yo):
        return pltpu.make_async_remote_copy(
            src_ref=wfull.at[from_chip(o), rows_of(p)],
            dst_ref=wfull.at[from_chip(o), rows_of(p)],
            send_sem=wy_send.at[o, p, yo],
            recv_sem=wx_recv.at[o, p],
            device_id={"sp": my_z * ny + (my_y + yo) % ny, "dp": my_dp},
            device_id_type=MESH,
        )

    def wc_copy(o, p):
        return pltpu.make_async_remote_copy(
            src_ref=wfull.at[from_chip(o), rows_of(p)],
            dst_ref=wfull.at[from_chip(o), rows_of(p)],
            send_sem=wc_send.at[o, p],
            recv_sem=wc_recv.at[o, p],
            device_id={"sp": me, "dp": my_x * 2 + 1 - my_core},
            device_id_type=MESH,
        )

    def own_copy():
        return pltpu.make_async_remote_copy(
            src_ref=w_ref,
            dst_ref=wfull.at[my_dp],
            send_sem=wc_send.at[0, 0],
            recv_sem=wc_recv.at[0, 0],
            device_id={"sp": me, "dp": my_x * 2 + 1 - my_core},
            device_id_type=MESH,
        )

    def pass_on(j):
        p = (first_piece + j) % PIECES
        for o in range(1, chips):
            wx_copy(o, p).wait_recv()
            wc_copy(o, p).start()
            if j < share:
                for yo in range(1, ny):
                    wy_copy(o, p, yo).start()

    for o in range(1, n):
        qkv_copy(o).start()
    loads[8].wait()
    for j in range(share):
        for o in range(1, chips):
            wx_copy(o, first_piece + j).start()
    own_copy().start()
    own_w = pltpu.make_async_copy(w_ref, wfull.at[my_dp], wl_sem)
    own_w.start()
    recv[me] = send[me]
    for i in (4, 5, 6, 7, 9, 10, 11, 12, 13, 14):
        loads[i].wait()

    rows_in = plane * cap
    ids = index_ref[0].astype(jnp.float32)
    e_0, e_1 = ids[0:1], ids[1:2]
    wide = -(-devices // 128) * 128
    sub_e = lax.broadcasted_iota(jnp.int32, (wide, tok), 0).astype(jnp.float32)
    hit_0 = jnp.where(sub_e == e_0, 1.0, 0.0)
    hit_1 = jnp.where(sub_e == e_1, 1.0, 0.0)
    tri = jnp.where(
        lax.broadcasted_iota(jnp.int32, (tok, tok), 0)
        < lax.broadcasted_iota(jnp.int32, (tok, tok), 1),
        1.0,
        0.0,
    ).astype(jnp.bfloat16)
    rank_0 = jnp.dot(hit_0.astype(jnp.bfloat16), tri, preferred_element_type=jnp.float32)
    rank_1 = jnp.dot(hit_1.astype(jnp.bfloat16), tri, preferred_element_type=jnp.float32)
    rank_1 = rank_1 + jnp.sum(hit_0, axis=1, keepdims=True)
    place_0 = e_0 * cap + jnp.sum(hit_0 * rank_0, axis=0, keepdims=True)
    place_1 = e_1 * cap + jnp.sum(hit_1 * rank_1, axis=0, keepdims=True)
    groups = group_ref.shape[1]
    span = devices // groups
    route_0 = jnp.zeros((1, tok), jnp.float32)
    route_1 = jnp.zeros((1, tok), jnp.float32)
    for c in range(groups):
        weight_c = group_ref[0, c : c + 1, :]
        route_0 += jnp.where((e_0 >= c * span) & (e_0 < (c + 1) * span), weight_c, 0.0)
        route_1 += jnp.where((e_1 >= c * span) & (e_1 < (c + 1) * span), weight_c, 0.0)
    route_0 = route_0 * within_ref[0, 0:1, :]
    route_1 = route_1 * within_ref[0, 1:2, :]
    sub_m = lax.broadcasted_iota(jnp.int32, (8, tok), 0)
    meta[my_z] = jnp.where(
        sub_m == 0,
        place_0,
        jnp.where(sub_m == 1, place_1, jnp.where(sub_m == 2, route_0, route_1)),
    )

    def meta_copy(z, slot):
        return pltpu.make_async_remote_copy(
            src_ref=meta.at[my_z],
            dst_ref=meta.at[slot],
            send_sem=meta_send.at[z],
            recv_sem=meta_recv.at[slot],
            device_id=device(z, my_q),
            device_id_type=MESH,
        )

    for o in range(1, nz):
        meta_copy((my_z + o) % nz, my_z).start()

    for j in range(max(share - 1, 1)):
        pass_on(j)
    for o in range(1, n):
        qkv_arrival(o).wait_recv()

    gates = jnp.concatenate(
        [recv[d, tok : tok + GATE_ROWS, 0:tok].astype(jnp.float32) for d in range(n)], axis=1
    )
    extra = extra_ref[0]
    f = log_sigmoid(gates[1:2] + offset_ref[0:1, 0:1]) + extra
    b = log_sigmoid(gates[3:4] + offset_ref[0:1, 1:2]) + extra
    f = jnp.broadcast_to(f, (8, length))
    b = jnp.broadcast_to(b, (8, length))
    lane = lax.broadcasted_iota(jnp.int32, (8, length), 1)
    step = 1
    while step < length:
        f = f + jnp.where(lane >= step, pltpu.roll(f, step, 1), 0.0)
        b = b + jnp.where(lane < length - step, pltpu.roll(b, length - step, 1), 0.0)
        step *= 2
    row_i = gates[0:1]
    row_f = row_i - f[0:1]
    row_b = gates[2:3] - b[0:1]
    sub = lax.broadcasted_iota(jnp.int32, (128, length), 0)
    stacked = jnp.where(sub == 0, f[0:1], jnp.where(sub == 1, b[0:1], row_i))
    cols[...] = stacked.T

    scale = dk ** (-0.5)
    amp = amp_ref[...]

    def mixed_copy(o, slot):
        return pltpu.make_async_remote_copy(
            src_ref=mixed.at[(me + o) % n],
            dst_ref=mrecv.at[slot],
            send_sem=msend_sem.at[o],
            recv_sem=mrecv_sem.at[o],
            device_id={"sp": (me + o) % n, "dp": my_dp},
            device_id_type=MESH,
        )

    def segment(j, _):
        d = (me + 1 + j) % n
        start = pl.multiple_of(d * tok, tok)
        kq = recv[d, 0:tok, 0 : 2 * dk]
        qs = kq[:, dk:].astype(jnp.float32) * scale
        ks = kq[:, :dk].astype(jnp.float32)
        diag = jnp.sum(qs * ks, axis=1, keepdims=True)
        qs = jnp.concatenate([qs, jnp.zeros_like(qs)], axis=1).astype(jnp.bfloat16)
        kall = recv[:, 0:tok, 0 : 2 * dk].reshape(length, 2 * dk)
        vall = recv[:, 0:tok, 2 * dk : 2 * dk + dv].reshape(length, dv)
        scores = lax.dot_general(
            qs, kall, (((1,), (1,)), ((), ())), preferred_element_type=jnp.float32
        )
        col = cols[pl.ds(start, tok), :]
        col_f, col_b, col_i = col[:, 0:1], col[:, 1:2], col[:, 2:3]
        t_pos = start + lax.broadcasted_iota(jnp.int32, (tok, length), 0)
        s_pos = lax.broadcasted_iota(jnp.int32, (tok, length), 1)
        before = s_pos < t_pos
        weight = scores * jnp.exp(jnp.where(before, col_f + row_f, col_b + row_b))
        diag = diag * jnp.exp(col_i)
        z_f = jnp.sum(jnp.where(before, weight, 0.0), axis=1, keepdims=True) + diag
        z_b = jnp.sum(jnp.where(before, 0.0, weight), axis=1, keepdims=True)
        inv_f = 1.0 / jnp.maximum(jnp.abs(z_f), 1.0)
        inv_b = 1.0 / jnp.maximum(jnp.abs(z_b), 1.0)
        probs = (weight * jnp.where(before, inv_f, inv_b)).astype(jnp.bfloat16)
        total = jnp.dot(probs, vall, preferred_element_type=jnp.float32)
        total = total + (diag * inv_f) * recv[d, 0:tok, 2 * dk : 2 * dk + dv].astype(jnp.float32)
        total = total * lax.rsqrt(jnp.mean(total * total, axis=1, keepdims=True) + EPS) * amp
        mixed[d] = total.astype(jnp.bfloat16)

        @pl.when(j >= 1)
        def _():
            mixed_copy(j, me).start()

        @pl.when(j == 0)
        def _():
            for late in range(max(share - 1, 1), share):
                pass_on(late)

        @pl.when(j == n // 2)
        def _():
            for late in range(share, share + (PIECES - share) // 2):
                pass_on(late)

        return 0

    lax.fori_loop(0, n, segment, 0)
    for j in range(share + (PIECES - share) // 2, PIECES):
        pass_on(j)
    mrecv[me] = mixed[me]
    sub_r = lax.broadcasted_iota(jnp.int32, (rows_in, tok), 0).astype(jnp.float32)
    at = sub_r + (my_z * rows_in).astype(jnp.float32)

    def tables(o, _):
        z = (my_z + o) % nz

        @pl.when(o > 0)
        def _():
            meta_copy(z, z).wait_recv()

        rows = meta[z]
        hit_0, hit_1 = at == rows[0:1], at == rows[1:2]
        table_t[z] = (jnp.where(hit_0, 1.0, 0.0) + jnp.where(hit_1, 1.0, 0.0)).astype(jnp.bfloat16)
        weighted = (jnp.where(hit_0, rows[2:3], 0.0) + jnp.where(hit_1, rows[3:4], 0.0)).T
        high = weighted.astype(jnp.bfloat16)
        table_hi[z] = high
        table_lo[z] = (weighted - high.astype(jnp.float32)).astype(jnp.bfloat16)
        return 0

    lax.fori_loop(0, nz, tables, 0)
    sig = jax.nn.sigmoid(logits_ref[0].astype(jnp.float32))
    for o in range(1, n):
        mixed_copy(o, (me + n - o) % n).wait_recv()
    gated = jnp.concatenate([mrecv[h].astype(jnp.float32) for h in range(n)], axis=1) * sig
    gated = gated.astype(jnp.bfloat16)
    own_w.wait()
    own_copy().wait_recv()
    for p in range(PIECES):
        for o in range(1, chips):
            wc_copy(o, p).wait_recv()
    for j in range(dpn):
        proj[:, j * wcol : (j + 1) * wcol] = jnp.dot(
            gated, wfull[j], preferred_element_type=jnp.float32
        )
    p = proj[...]
    stream = (
        res_ref[0].astype(jnp.float32)
        + cell_gain_ref[...] * p * lax.rsqrt(jnp.mean(p * p, axis=1, keepdims=True) + EPS)
    ).astype(jnp.bfloat16)
    s = stream.astype(jnp.float32)
    width = s.shape[1]
    part = width // PARTS
    moe = (
        expert_gain_ref[...] * s * lax.rsqrt(jnp.mean(s * s, axis=1, keepdims=True) + EPS)
    ).astype(jnp.bfloat16)

    def line_copy(z, p, to, sems):
        return pltpu.make_async_remote_copy(
            src_ref=line.at[z, p],
            dst_ref=line.at[z, p],
            send_sem=sems.at[z, p],
            recv_sem=line_recv.at[z, p],
            device_id=device(to, my_q),
            device_id_type=MESH,
        )

    above, below = (my_z + 1) % nz, (my_z + nz - 1) % nz
    has_above, has_below = my_z + 1 < nz, my_z > 0
    edge = (my_z == 0) | (my_z == nz - 1)

    def spread(z, p):
        @pl.when((z <= my_z) & has_above)
        def _():
            line_copy(z, p, above, up_send).start()

        @pl.when((z >= my_z) & has_below)
        def _():
            line_copy(z, p, below, down_send).start()

    for p in range(PARTS):
        line[my_z, p] = moe[:, p * part : (p + 1) * part]
        spread(my_z, p)
    for p in range(PARTS):
        total[p] = s[:, p * part : (p + 1) * part]
    for i in (15, 16, 17):
        loads[i].wait()
    ff = hs.shape[1]

    def by_distance(k):
        found = my_z
        for z in range(nz):
            inner = 1 if 2 * z < nz - 1 else -1
            near = sorted(range(nz), key=lambda s: (abs(s - z), -(s - z) * inner))
            for place in range(nz):
                found = jnp.where((my_z == z) & (k == place), near[place], found)
        return found

    def plane_copy(src, dst, sems, z, p, q_to, q_src, q_dst):
        return pltpu.make_async_remote_copy(
            src_ref=src.at[z, p, q_src],
            dst_ref=dst.at[z, p, q_dst],
            send_sem=sems[0].at[z, p],
            recv_sem=sems[1].at[z, p],
            device_id=device(my_z, q_to),
            device_id_type=MESH,
        )

    def plane_send(src, dst, sems, z, p):
        def one(o, _):
            q = (my_q + o) % plane
            plane_copy(src, dst, sems, z, p, q, q, my_q).start()
            return 0

        lax.fori_loop(1, plane, one, 0)
        dst[z, p, my_q] = src[z, p, my_q]

    def plane_all(src, dst, sems, z, p):
        others = pl.ds(0, plane - 1)
        return pltpu.make_async_remote_copy(
            src_ref=src.at[z, p, others],
            dst_ref=dst.at[z, p, others],
            send_sem=sems[0].at[z, p],
            recv_sem=sems[1].at[z, p],
            device_id=device(my_z, (my_q + 1) % plane),
            device_id_type=MESH,
        )

    out_way = (outgoing, incoming, (out_send, out_recv))
    back_way = (produced, returned, (back_send, back_recv))

    def dispatch(k, first, last):
        z = by_distance(k)

        def piece(p, _):
            @pl.when(k > 0)
            def _():
                line_copy(z, p, above, up_send).wait_recv()
                spread(z, p)

            block = jnp.dot(table_t[z], line[z, p], preferred_element_type=jnp.float32)
            outgoing[z, p] = block.astype(jnp.bfloat16).reshape(plane, cap, part)
            plane_send(*out_way, z, p)
            return 0

        lax.fori_loop(first, last, piece, 0)

    def expert(k, inline):
        z = by_distance(k)

        def arrive(p, _):
            plane_all(*out_way, z, p).wait_recv()
            return 0

        lax.fori_loop(0, PARTS, arrive, 0)

        def up_tile(t, _):
            at = pl.ds(pl.multiple_of(t * FF_TILE, FF_TILE), FF_TILE)
            x = jnp.concatenate(
                [incoming[z, p].reshape(rows_in, part) for p in range(PARTS)], axis=1
            )
            a = jnp.dot(x, gate_ref[0, :, at], preferred_element_type=jnp.float32)
            u = jnp.dot(x, up_ref[0, :, at], preferred_element_type=jnp.float32)
            hs[:, at] = (jax.nn.silu(a) * u).astype(jnp.bfloat16)
            return 0

        lax.fori_loop(0, ff // FF_TILE, up_tile, 0)

        def down_tile(p, _):
            at = pl.ds(pl.multiple_of(p * part, part), part)
            y = jnp.dot(hs[...], down_ref[0, :, at], preferred_element_type=jnp.float32)
            produced[z, p] = y.astype(jnp.bfloat16).reshape(plane, cap, part)

            @pl.when(inline)
            def _():
                plane_send(*back_way, z, p)

            return 0

        lax.fori_loop(0, PARTS, down_tile, 0)

    def send_back(k):
        def piece(p, _):
            plane_send(*back_way, by_distance(k), p)
            return 0

        lax.fori_loop(0, PARTS, piece, 0)

    def partial_copy(z, p):
        to = jnp.where(z < my_z, below, above)
        slot = jnp.where((z > my_z) & (to == z), nz, z)
        return pltpu.make_async_remote_copy(
            src_ref=partial_out.at[z, p],
            dst_ref=partial_in.at[slot, p],
            send_sem=part_send.at[z, p],
            recv_sem=part_recv.at[slot, p],
            device_id=device(to, my_q),
            device_id_type=MESH,
        )

    def partial_arrive(slot, p):
        pltpu.make_async_remote_copy(
            src_ref=partial_out.at[0, p],
            dst_ref=partial_in.at[slot, p],
            send_sem=part_send.at[0, p],
            recv_sem=part_recv.at[slot, p],
            device_id=device(above, my_q),
            device_id_type=MESH,
        ).wait_recv()

    def combine(z, p):
        plane_all(*back_way, z, p).wait_recv()
        block = returned[z, p].reshape(rows_in, part)
        mine = jnp.dot(table_hi[z], block, preferred_element_type=jnp.float32) + jnp.dot(
            table_lo[z], block, preferred_element_type=jnp.float32
        )
        total[PARTS] = mine

        @pl.when(z == my_z)
        def _():
            total[p] += total[PARTS]

        @pl.when(z != my_z)
        def _():
            @pl.when(~edge)
            def _():
                partial_arrive(z, p)
                total[PARTS] += partial_in[z, p].astype(jnp.float32)

            partial_out[z, p] = total[PARTS].astype(jnp.bfloat16)
            partial_copy(z, p).start()

    def combine_all(k):
        def one(p, _):
            combine(by_distance(k), p)
            return 0

        lax.fori_loop(0, PARTS, one, 0)

    dispatch(0, 0, PARTS)
    half = PARTS // 2

    def tick(k, _):
        last = k == nz - 1
        stop = jnp.where(last, 0, PARTS)
        early = jnp.minimum(jnp.where(k == 0, half, jnp.where(edge, jnp.where(k == 1, half // 2, half), PARTS)), stop)
        dispatch(k + 1, 0, early)

        @pl.when(~edge & (k == nz - 2))
        def _():
            send_back(1)

        expert(k, edge & (k > 0))
        dispatch(k + 1, early, stop)

        @pl.when(edge & (k > 0))
        def _():
            combine_all(k)

        return 0

    lax.fori_loop(0, nz, tick, 0)

    @pl.when(edge)
    def _():
        send_back(0)

    @pl.when(~edge)
    def _():
        for k in range(nz - 1, 1, -1):
            send_back(k)
        send_back(0)
        if nz > 2:
            combine_all(1)
        late = max(nz - 2, 1)

        def one(m, _):
            combine(by_distance(nz - 1 - m % late), m // late)
            return 0

        lax.fori_loop(0, (nz - 2) * PARTS, one, 0)

    combine_all(0)
    for p in range(PARTS):
        @pl.when(has_above)
        def _():
            partial_arrive(my_z, p)
            total[p] += partial_in[my_z, p].astype(jnp.float32)

        @pl.when(has_below)
        def _():
            partial_arrive(nz, p)
            total[p] += partial_in[nz, p].astype(jnp.float32)

        out_ref[0, :, p * part : (p + 1) * part] = total[p].astype(jnp.bfloat16)

    def drain(i, _):
        z, p = i // PARTS, i % PARTS
        plane_all(*out_way, z, p).wait_send()
        plane_all(*back_way, z, p).wait_send()

        @pl.when((z <= my_z) & has_above)
        def _():
            line_copy(z, p, above, up_send).wait_send()

        @pl.when((z >= my_z) & has_below)
        def _():
            line_copy(z, p, below, down_send).wait_send()

        @pl.when(z != my_z)
        def _():
            partial_copy(z, p).wait_send()

        return 0

    lax.fori_loop(0, nz * PARTS, drain, 0)
    for o in range(1, nz):
        meta_copy((my_z + o) % nz, my_z).wait_send()
    for o in range(1, n):
        qkv_copy(o).wait_send()
        mixed_copy(o, me).wait_send()
    own_copy().wait_send()
    for o in range(1, chips):
        for p in range(PIECES):
            wc_copy(o, p).wait_send()
        for j in range(share):
            wx_copy(o, first_piece + j).wait_send()
            for yo in range(1, ny):
                wy_copy(o, first_piece + j, yo).wait_send()


def on_device(
    residual_input,
    queries,
    keys,
    values,
    gate_logits,
    retention_offset,
    log_forget_extra,
    lane_amplifier,
    output_gate_logits,
    output_projection,
    cell_norm_gain,
    expert_norm_gain,
    expert_index,
    group_mixing_weight,
    within_group_weight,
    gate_weight,
    up_weight,
    down_weight,
):
    n, dpn = lax.axis_size("sp"), lax.axis_size("dp")
    tok, width = residual_input.shape[1:]
    dk, dv = queries.shape[2] // n, values.shape[2] // n
    length, devices, ff = n * tok, n * dpn, gate_weight.shape[2]
    cap, chips = 4 * tok // devices, dpn // 2
    ny = chips if n % chips == 0 else 1
    nz, plane = n // ny, ny * dpn
    rows_in, part = plane * cap, width // PARTS
    operands = (
        queries, keys, values, jnp.swapaxes(gate_logits, 1, 2), retention_offset, log_forget_extra,
        lane_amplifier.reshape(1, dv), output_gate_logits, output_projection,
        residual_input, cell_norm_gain.reshape(1, width), expert_norm_gain.reshape(1, width),
        jnp.swapaxes(expert_index, 1, 2), jnp.swapaxes(group_mixing_weight, 1, 2),
        jnp.swapaxes(within_group_weight, 1, 2),
        gate_weight, up_weight, down_weight,
    )
    dma = pltpu.SemaphoreType.DMA
    bf16, f32 = jnp.bfloat16, jnp.float32
    hbm = pl.BlockSpec(memory_space=pltpu.HBM)
    return pl.pallas_call(
        partial(layer_kernel, n=n, dpn=dpn, inputs=len(operands)),
        out_shape=pltpu.VMEM((1, tok, width), bf16),
        in_specs=[hbm] * len(operands),
        out_specs=pl.BlockSpec(memory_space=pltpu.VMEM),
        scratch_shapes=[pltpu.VMEM(x.shape, x.dtype) for x in operands]
        + [
            pltpu.VMEM((n, tok + GATE_ROWS, 2 * dk + dv), bf16),
            pltpu.VMEM((n, tok + GATE_ROWS, 2 * dk + dv), bf16),
            pltpu.VMEM((128, tok), f32),
            pltpu.VMEM((length, 128), f32),
            pltpu.VMEM((n, tok, dv), bf16),
            pltpu.VMEM((n, tok, dv), bf16),
            pltpu.VMEM((dpn,) + output_projection.shape, bf16),
            pltpu.VMEM((tok, width), f32),
            pltpu.VMEM((nz, 8, tok), f32),
            pltpu.VMEM((nz, rows_in, tok), bf16),
            pltpu.VMEM((nz, tok, rows_in), bf16),
            pltpu.VMEM((nz, tok, rows_in), bf16),
            pltpu.VMEM((nz, PARTS, tok, part), bf16),
            pltpu.VMEM((nz, PARTS, plane, cap, part), bf16),
            pltpu.VMEM((nz, PARTS, plane, cap, part), bf16),
            pltpu.VMEM((rows_in, ff), bf16),
            pltpu.VMEM((nz, PARTS, plane, cap, part), bf16),
            pltpu.VMEM((nz, PARTS, plane, cap, part), bf16),
            pltpu.VMEM((nz, PARTS, tok, part), bf16),
            pltpu.VMEM((nz + 1, PARTS, tok, part), bf16),
            pltpu.VMEM((PARTS + 1, tok, part), f32),
            dma((len(operands),)),
            dma((n,)), dma((n,)), dma((n,)), dma((n,)),
            dma((chips, PIECES)), dma((chips, PIECES)), dma((chips, PIECES, ny)),
            dma((chips, PIECES)), dma((chips, PIECES)),
            dma(()),
            dma((nz,)), dma((nz,)),
            dma((nz, PARTS)), dma((nz, PARTS)), dma((nz, PARTS)),
            dma((nz, PARTS)), dma((nz, PARTS)), dma((nz, PARTS)), dma((nz, PARTS)),
            dma((nz, PARTS)), dma((nz + 1, PARTS)),
        ],
        compiler_params=pltpu.CompilerParams(
            collective_id=0, has_side_effects=True, vmem_limit_bytes=60 * 1024 * 1024
        ),
    )(*operands)


def solution(mesh):
    in_specs = (
        P("dp", "sp", None),
        P("dp", "sp", None),
        P("dp", "sp", None),
        P("dp", "sp", None),
        P("dp", "sp", None),
        P("sp", None),
        P("dp", "sp", None),
        P("sp"),
        P("dp", "sp", None),
        P(None, "dp"),
        P(),
        P(),
        P("dp", "sp", None),
        P("dp", "sp", None),
        P("dp", "sp", None),
        P(("sp", "dp"), None, None),
        P(("sp", "dp"), None, None),
        P(("sp", "dp"), None, None),
    )
    out_specs = P("dp", "sp", None)
    return jax.shard_map(
        on_device, mesh=mesh, in_specs=in_specs, out_specs=out_specs, check_vma=False
    )
```

```python
from functools import partial

import jax
import jax.numpy as jnp
from jax import lax
from jax.experimental import pallas as pl
from jax.experimental.pallas import tpu as pltpu
from jax.sharding import PartitionSpec as P

EPS = 1e-06
MESH = pl.DeviceIdType.MESH
GATE_ROWS = 16
PARTS = 4
SUBS = 2
FF_TILE = 256
PIECES = 8
EXTRA = 1


def log_sigmoid(x):
    return jnp.minimum(x, 0.0) - jnp.log1p(jnp.exp(-jnp.abs(x)))


def layer_kernel(*refs, n, dpn, inputs):
    hbm, (out_ref,), rest = refs[:inputs], refs[inputs : inputs + 1], refs[inputs + 1 :]
    local, rest = rest[:inputs], rest[inputs:]
    (
        q_ref, k_ref, v_ref, g_ref, offset_ref, extra_ref, amp_ref, logits_ref, w_ref,
        res_ref, cell_gain_ref, expert_gain_ref, index_ref, group_ref, within_ref,
        gate_ref, up_ref, down_ref,
    ) = local
    (
        send, recv, gates_t, params, rows_of_gate, cols, weights, sums, state_out, state_in,
        mixed, mrecv, wfull, proj,
        meta, table_t, table_hi, table_lo, line, outgoing, incoming, hs, produced, returned,
        partial_out, partial_in, total,
        in_sem, send_sem, recv_sem, param_send, param_recv, state_send, state_recv, msend_sem, mrecv_sem, wx_send, wx_recv, wy_send, wc_send,
        wc_recv, wl_sem, meta_send, meta_recv, up_send, down_send, line_recv,
        out_send, out_recv, back_send, back_recv, part_send, part_recv,
    ) = rest
    loads = [pltpu.make_async_copy(hbm[i], local[i], in_sem.at[i]) for i in range(inputs)]
    early = (0, 1, 2, 3, 8)
    for i in early:
        loads[i].start()
    tok = q_ref.shape[1]
    dk = q_ref.shape[2] // n
    dv = v_ref.shape[2] // n
    half = n // 2
    length = half * tok
    wcol = w_ref.shape[1]
    me = lax.axis_index("sp")
    my_half, my_rank = me // half, me % half
    first = my_half * half
    opposite = (me + half) % n
    my_dp = lax.axis_index("dp")
    my_x, my_core = my_dp // 2, my_dp % 2
    chips = dpn // 2

    barrier = pltpu.get_barrier_semaphore()

    devices = n * dpn
    cap = 4 * tok // devices
    ny = chips if n % chips == 0 else 1
    nz = n // ny
    plane = ny * dpn
    my_z, my_y = me // ny, me % ny
    my_q = my_y * dpn + my_dp

    def device(z, q):
        return {"sp": z * ny + q // dpn, "dp": q % dpn}

    def greet_sp(o, _):
        pl.semaphore_signal(
            barrier, inc=1, device_id={"sp": (me + o) % n, "dp": my_dp}, device_id_type=MESH
        )
        return 0

    def greet_plane(o, _):
        pl.semaphore_signal(
            barrier, inc=1, device_id=device(my_z, (my_q + o) % plane), device_id_type=MESH
        )
        return 0

    lax.fori_loop(1, n, greet_sp, 0)
    lax.fori_loop(1, plane, greet_plane, 0)
    for load in loads[:4]:
        load.wait()

    for h in range(n):
        send[h, 0:tok, 0:dk] = k_ref[0, :, h * dk : (h + 1) * dk]
        send[h, 0:tok, dk : 2 * dk] = q_ref[0, :, h * dk : (h + 1) * dk]
        send[h, 0:tok, 2 * dk : 2 * dk + dv] = v_ref[0, :, h * dv : (h + 1) * dv]
    gate_rows = g_ref.shape[1]
    gates_t[0:gate_rows] = g_ref[0].astype(jnp.float32)
    gates_t[gate_rows:] = jnp.zeros((128 - gate_rows, tok), jnp.float32)
    for h in range(n):
        send[h, tok : tok + GATE_ROWS, 0:tok] = gates_t[4 * h : 4 * h + GATE_ROWS, :].astype(
            jnp.bfloat16
        )
        send[h, tok : tok + GATE_ROWS, tok:] = jnp.zeros(
            (GATE_ROWS, send.shape[2] - tok), jnp.bfloat16
        )

    pl.semaphore_wait(barrier, n - 1 + plane - 1)
    for i in range(inputs):
        if i not in early:
            loads[i].start()

    def qkv_copy(o, j):
        return pltpu.make_async_remote_copy(
            src_ref=send.at[(my_rank + o) % half + j * half],
            dst_ref=recv.at[j, my_rank],
            send_sem=send_sem.at[o, j],
            recv_sem=recv_sem.at[o, j],
            device_id={"sp": first + (my_rank + o) % half, "dp": my_dp},
            device_id_type=MESH,
        )

    def qkv_arrival(o, j):
        return pltpu.make_async_remote_copy(
            src_ref=send.at[(my_rank + o) % half + j * half],
            dst_ref=recv.at[j, (my_rank + half - o) % half],
            send_sem=send_sem.at[o, j],
            recv_sem=recv_sem.at[o, j],
            device_id={"sp": first + (my_rank + o) % half, "dp": my_dp},
            device_id_type=MESH,
        )

    def param_copy(slot):
        return pltpu.make_async_remote_copy(
            src_ref=params.at[my_half],
            dst_ref=params.at[slot],
            send_sem=param_send,
            recv_sem=param_recv,
            device_id={"sp": opposite, "dp": my_dp},
            device_id_type=MESH,
        )

    def state_copy():
        return pltpu.make_async_remote_copy(
            src_ref=state_out,
            dst_ref=state_in,
            send_sem=state_send,
            recv_sem=state_recv,
            device_id={"sp": opposite, "dp": my_dp},
            device_id_type=MESH,
        )

    piece = w_ref.shape[0] // PIECES

    share = PIECES // ny
    direct = share + (EXTRA if ny > 1 else 0)
    first_piece = my_y * share

    def rows_of(p):
        return pl.ds(pl.multiple_of(p * piece, piece), piece)

    def wx_copy(o, p):
        return pltpu.make_async_remote_copy(
            src_ref=w_ref.at[rows_of(p)],
            dst_ref=wfull.at[my_dp, rows_of(p)],
            send_sem=wx_send.at[o, p],
            recv_sem=wx_recv.at[o, p],
            device_id={"sp": me, "dp": ((my_x + o) % chips) * 2 + my_core},
            device_id_type=MESH,
        )

    def from_chip(o):
        return ((my_x + chips - o) % chips) * 2 + my_core

    def wy_copy(o, p, yo):
        return pltpu.make_async_remote_copy(
            src_ref=wfull.at[from_chip(o), rows_of(p)],
            dst_ref=wfull.at[from_chip(o), rows_of(p)],
            send_sem=wy_send.at[o, p, yo],
            recv_sem=wx_recv.at[o, p],
            device_id={"sp": my_z * ny + (my_y + yo) % ny, "dp": my_dp},
            device_id_type=MESH,
        )

    def wc_copy(o, p):
        return pltpu.make_async_remote_copy(
            src_ref=wfull.at[from_chip(o), rows_of(p)],
            dst_ref=wfull.at[from_chip(o), rows_of(p)],
            send_sem=wc_send.at[o, p],
            recv_sem=wc_recv.at[o, p],
            device_id={"sp": me, "dp": my_x * 2 + 1 - my_core},
            device_id_type=MESH,
        )

    def own_copy():
        return pltpu.make_async_remote_copy(
            src_ref=w_ref,
            dst_ref=wfull.at[my_dp],
            send_sem=wc_send.at[0, 0],
            recv_sem=wc_recv.at[0, 0],
            device_id={"sp": me, "dp": my_x * 2 + 1 - my_core},
            device_id_type=MESH,
        )

    def onward(j, yo):
        return j < share and (j >= EXTRA or yo < ny - 1)

    def pass_on(j):
        p = (first_piece + j) % PIECES
        for o in range(1, chips):
            wx_copy(o, p).wait_recv()
            wc_copy(o, p).start()
            for yo in range(1, ny):
                if onward(j, yo):
                    wy_copy(o, p, yo).start()

    for o in range(1, half):
        for j in range(2):
            qkv_copy(o, j).start()
    loads[8].wait()
    for j in range(direct):
        for o in range(1, chips):
            wx_copy(o, (first_piece + j) % PIECES).start()
    own_copy().start()
    own_w = pltpu.make_async_copy(w_ref, wfull.at[my_dp], wl_sem)
    own_w.start()
    for j in range(2):
        recv[j, my_rank] = send[my_rank + j * half]
    for i in (4, 5, 6, 7, 9, 10, 11, 12, 13, 14):
        loads[i].wait()
    for d in range(n):
        params[my_half, d : d + 1, 0:tok] = extra_ref[0, :, d * tok : (d + 1) * tok]
    params[my_half, n : n + 1, 0:dv] = amp_ref[...]
    lane_p = lax.broadcasted_iota(jnp.int32, (1, params.shape[2]), 1)
    params[my_half, n + 1 : n + 2] = jnp.where(
        lane_p == 0, offset_ref[0:1, 0:1], offset_ref[0:1, 1:2]
    )
    param_copy(my_half).start()

    rows_in = plane * cap
    ids = index_ref[0].astype(jnp.float32)
    e_0, e_1 = ids[0:1], ids[1:2]
    wide = -(-devices // 128) * 128
    sub_e = lax.broadcasted_iota(jnp.int32, (wide, tok), 0).astype(jnp.float32)
    hit_0 = jnp.where(sub_e == e_0, 1.0, 0.0)
    hit_1 = jnp.where(sub_e == e_1, 1.0, 0.0)
    tri = jnp.where(
        lax.broadcasted_iota(jnp.int32, (tok, tok), 0)
        < lax.broadcasted_iota(jnp.int32, (tok, tok), 1),
        1.0,
        0.0,
    ).astype(jnp.bfloat16)
    rank_0 = jnp.dot(hit_0.astype(jnp.bfloat16), tri, preferred_element_type=jnp.float32)
    rank_1 = jnp.dot(hit_1.astype(jnp.bfloat16), tri, preferred_element_type=jnp.float32)
    rank_1 = rank_1 + jnp.sum(hit_0, axis=1, keepdims=True)
    place_0 = e_0 * cap + jnp.sum(hit_0 * rank_0, axis=0, keepdims=True)
    place_1 = e_1 * cap + jnp.sum(hit_1 * rank_1, axis=0, keepdims=True)
    groups = group_ref.shape[1]
    span = devices // groups
    route_0 = jnp.zeros((1, tok), jnp.float32)
    route_1 = jnp.zeros((1, tok), jnp.float32)
    for c in range(groups):
        weight_c = group_ref[0, c : c + 1, :]
        route_0 += jnp.where((e_0 >= c * span) & (e_0 < (c + 1) * span), weight_c, 0.0)
        route_1 += jnp.where((e_1 >= c * span) & (e_1 < (c + 1) * span), weight_c, 0.0)
    route_0 = route_0 * within_ref[0, 0:1, :]
    route_1 = route_1 * within_ref[0, 1:2, :]
    sub_m = lax.broadcasted_iota(jnp.int32, (8, tok), 0)
    meta[my_z] = jnp.where(
        sub_m == 0,
        place_0,
        jnp.where(sub_m == 1, place_1, jnp.where(sub_m == 2, route_0, route_1)),
    )

    def meta_copy(z, slot):
        return pltpu.make_async_remote_copy(
            src_ref=meta.at[my_z],
            dst_ref=meta.at[slot],
            send_sem=meta_send.at[z],
            recv_sem=meta_recv.at[slot],
            device_id=device(z, my_q),
            device_id_type=MESH,
        )

    for o in range(1, nz):
        meta_copy((my_z + o) % nz, my_z).start()

    stops = [PIECES * i // 8 for i in (2, 3, 5, 6, 8)]

    def pass_until(i):
        for j in range(stops[i - 1] if i else 0, stops[i]):
            pass_on(j)

    pass_until(0)
    for o in range(1, half):
        for j in range(2):
            qkv_arrival(o, j).wait_recv()
    param_copy(1 - my_half).wait_recv()

    upper = my_half == 1
    lane = lax.broadcasted_iota(jnp.int32, (8, length), 1)
    sub = lax.broadcasted_iota(jnp.int32, (8, length), 0)
    gates, f, b = [], [], []
    for j in range(2):
        gates.append(
            jnp.concatenate(
                [recv[j, d, tok : tok + GATE_ROWS, 0:tok].astype(jnp.float32) for d in range(half)],
                axis=1,
            )
        )
        extra = jnp.concatenate(
            [params[j, pl.ds(first + d, 1), 0:tok] for d in range(half)], axis=1
        )
        offset = params[j, n + 1 : n + 2]
        f.append(log_sigmoid(gates[j][1:2] + offset[:, 0:1]) + extra)
        b.append(log_sigmoid(gates[j][3:4] + offset[:, 1:2]) + extra)
    f = jnp.where(sub == 0, f[0], f[1])
    b = jnp.where(sub == 0, b[0], b[1])
    step = 1
    while step < length:
        f = f + jnp.where(lane >= step, pltpu.roll(f, step, 1), 0.0)
        b = b + jnp.where(lane < length - step, pltpu.roll(b, length - step, 1), 0.0)
        step *= 2
    wide_sub = lax.broadcasted_iota(jnp.int32, (128, length), 0)
    for j in range(2):
        row_i = gates[j][0:1]
        row_f = row_i - f[j : j + 1]
        row_b = gates[j][2:3] - b[j : j + 1]
        rows_of_gate[j] = jnp.where(sub == 0, row_f, row_b)
        leaving = jnp.exp(
            jnp.where(upper, row_b + b[j : j + 1, 0:1], row_f + f[j : j + 1, length - 1 : length])
        )
        stacked = jnp.where(wide_sub == 0, f[j : j + 1], jnp.where(wide_sub == 1, b[j : j + 1], row_i))
        cols[j] = jnp.where(wide_sub == 3, leaving, stacked).T

    scale = dk ** (-0.5)

    def state(j, _):
        kq = recv[j, :, 0:tok, 0 : 2 * dk].reshape(length, 2 * dk).astype(jnp.float32)
        kq = kq * cols[j][:, 3:4]
        memory = lax.dot_general(
            kq.astype(jnp.bfloat16),
            recv[j, :, 0:tok, 2 * dk : 2 * dk + dv].reshape(length, dv),
            (((0,), (0,)), ((), ())),
            preferred_element_type=jnp.float32,
        )
        normal = jnp.sum(kq, axis=0, keepdims=True)
        high = normal.astype(jnp.bfloat16).astype(jnp.float32)
        at = lax.broadcasted_iota(jnp.int32, (GATE_ROWS, 2 * dk), 0)
        state_out[j, 0:dk] = memory[0:dk].astype(jnp.bfloat16)
        state_out[j, dk:, 0 : 2 * dk] = jnp.where(
            at == 0, high, jnp.where(at == 1, normal - high, 0.0)
        ).astype(jnp.bfloat16)
        return 0

    lax.fori_loop(0, 2, state, 0)
    state_copy().start()
    pass_until(1)

    def mixed_copy(o, j, rank):
        return pltpu.make_async_remote_copy(
            src_ref=mixed.at[j, (my_rank + o) % half],
            dst_ref=mrecv.at[rank + j * half],
            send_sem=msend_sem.at[o, j],
            recv_sem=mrecv_sem.at[o, j],
            device_id={"sp": first + (my_rank + o) % half, "dp": my_dp},
            device_id_type=MESH,
        )

    def scaled(j, d):
        return recv[j, d, 0:tok, dk : 2 * dk].astype(jnp.float32) * scale

    def before_of(d):
        t_pos = d * tok + lax.broadcasted_iota(jnp.int32, (tok, length), 0)
        return lax.broadcasted_iota(jnp.int32, (tok, length), 1) < t_pos

    lane_z = lax.broadcasted_iota(jnp.int32, (tok, 128), 1)

    def weigh_head(d, k, j):
        m = 2 * k + j
        start = pl.multiple_of(d * tok, tok)
        qs = scaled(j, d)
        ks = recv[j, d, 0:tok, 0:dk].astype(jnp.float32)
        diag = jnp.sum(qs * ks, axis=1, keepdims=True)
        qs = jnp.concatenate([qs, jnp.zeros_like(qs)], axis=1).astype(jnp.bfloat16)
        kall = recv[j, :, 0:tok, 0 : 2 * dk].reshape(length, 2 * dk)
        scores = lax.dot_general(
            qs, kall, (((1,), (1,)), ((), ())), preferred_element_type=jnp.float32
        )
        col = cols[j, pl.ds(start, tok), :]
        col_f, col_b, col_i = col[:, 0:1], col[:, 1:2], col[:, 2:3]
        before = before_of(d)
        rows = rows_of_gate[j]
        weight = scores * jnp.exp(jnp.where(before, col_f + rows[0:1], col_b + rows[1:2]))
        weights[m] = weight
        diag = diag * jnp.exp(col_i)
        z_f = jnp.sum(jnp.where(before, weight, 0.0), axis=1, keepdims=True) + diag
        z_b = jnp.sum(jnp.where(before, 0.0, weight), axis=1, keepdims=True)
        sums[m] = jnp.where(lane_z == 0, z_f, jnp.where(lane_z == 1, z_b, diag))
    def weigh(k, _):
        for j in range(2):
            weigh_head((my_rank + 1 + k) % half, k, j)
        return 0

    lax.fori_loop(0, half, weigh, 0)
    pass_until(2)
    state_copy().wait_recv()

    def segment_head(d, k, j):
        m = 2 * k + j
        start = pl.multiple_of(d * tok, tok)
        col = cols[j, pl.ds(start, tok), :]
        carried = jnp.exp(jnp.where(upper, col[:, 0:1], col[:, 1:2]))
        qs = scaled(j, d) * carried
        normal = state_in[j, dk:, 0:dk].astype(jnp.float32)
        z_state = jnp.sum(qs * (normal[0:1] + normal[1:2]), axis=1, keepdims=True)
        z = sums[m]
        z_f, z_b, diag = z[:, 0:1], z[:, 1:2], z[:, 2:3]
        z_f = z_f + jnp.where(upper, z_state, 0.0)
        z_b = z_b + jnp.where(upper, 0.0, z_state)
        inv_f = 1.0 / jnp.maximum(jnp.abs(z_f), 1.0)
        inv_b = 1.0 / jnp.maximum(jnp.abs(z_b), 1.0)
        probs = (weights[m] * jnp.where(before_of(d), inv_f, inv_b)).astype(jnp.bfloat16)
        vall = recv[j, :, 0:tok, 2 * dk : 2 * dk + dv].reshape(length, dv)
        total = jnp.dot(probs, vall, preferred_element_type=jnp.float32)
        total = total + jnp.dot(
            (qs * jnp.where(upper, inv_f, inv_b)).astype(jnp.bfloat16),
            state_in[j, 0:dk],
            preferred_element_type=jnp.float32,
        )
        total = total + (diag * inv_f) * recv[j, d, 0:tok, 2 * dk : 2 * dk + dv].astype(jnp.float32)
        amp = params[j, n : n + 1, 0:dv]
        total = total * lax.rsqrt(jnp.mean(total * total, axis=1, keepdims=True) + EPS) * amp
        mixed[j, d] = total.astype(jnp.bfloat16)

    def segment(k, _):
        d = (my_rank + 1 + k) % half
        for j in range(2):
            segment_head(d, k, j)

        @pl.when(k < half - 1)
        def _():
            for j in range(2):
                mixed_copy(k + 1, j, my_rank).start()

        return 0

    lax.fori_loop(0, half, segment, 0)
    pass_until(3)
    for j in range(2):
        mrecv[my_rank + j * half] = mixed[j, my_rank]
    sub_r = lax.broadcasted_iota(jnp.int32, (rows_in, tok), 0).astype(jnp.float32)
    at = sub_r + (my_z * rows_in).astype(jnp.float32)

    def tables(o, _):
        z = (my_z + o) % nz

        @pl.when(o > 0)
        def _():
            meta_copy(z, z).wait_recv()

        rows = meta[z]
        hit_0, hit_1 = at == rows[0:1], at == rows[1:2]
        table_t[z] = (jnp.where(hit_0, 1.0, 0.0) + jnp.where(hit_1, 1.0, 0.0)).astype(jnp.bfloat16)
        weighted = (jnp.where(hit_0, rows[2:3], 0.0) + jnp.where(hit_1, rows[3:4], 0.0)).T
        high = weighted.astype(jnp.bfloat16)
        table_hi[z] = high
        table_lo[z] = (weighted - high.astype(jnp.float32)).astype(jnp.bfloat16)
        return 0

    lax.fori_loop(0, nz, tables, 0)
    sig = jax.nn.sigmoid(logits_ref[0].astype(jnp.float32))
    pass_until(4)
    for o in range(1, half):
        for j in range(2):
            mixed_copy(o, j, (my_rank + half - o) % half).wait_recv()
    gated = jnp.concatenate([mrecv[h].astype(jnp.float32) for h in range(n)], axis=1) * sig
    gated = gated.astype(jnp.bfloat16)
    own_w.wait()
    own_copy().wait_recv()
    for p in range(PIECES):
        for o in range(1, chips):
            wc_copy(o, p).wait_recv()
    for j in range(dpn):
        proj[:, j * wcol : (j + 1) * wcol] = jnp.dot(
            gated, wfull[j], preferred_element_type=jnp.float32
        )
    p = proj[...]
    stream = (
        res_ref[0].astype(jnp.float32)
        + cell_gain_ref[...] * p * lax.rsqrt(jnp.mean(p * p, axis=1, keepdims=True) + EPS)
    ).astype(jnp.bfloat16)
    s = stream.astype(jnp.float32)
    width = s.shape[1]
    part = width // PARTS
    moe = (
        expert_gain_ref[...] * s * lax.rsqrt(jnp.mean(s * s, axis=1, keepdims=True) + EPS)
    ).astype(jnp.bfloat16)

    def line_copy(z, p, to, sems):
        return pltpu.make_async_remote_copy(
            src_ref=line.at[z, p],
            dst_ref=line.at[z, p],
            send_sem=sems.at[z, p],
            recv_sem=line_recv.at[z, p],
            device_id=device(to, my_q),
            device_id_type=MESH,
        )

    above, below = (my_z + 1) % nz, (my_z + nz - 1) % nz
    has_above, has_below = my_z + 1 < nz, my_z > 0
    edge = (my_z == 0) | (my_z == nz - 1)

    def spread(z, p):
        @pl.when((z <= my_z) & has_above)
        def _():
            line_copy(z, p, above, up_send).start()

        @pl.when((z >= my_z) & has_below)
        def _():
            line_copy(z, p, below, down_send).start()

    for p in range(PARTS):
        line[my_z, p] = moe[:, p * part : (p + 1) * part]
        spread(my_z, p)
    for p in range(PARTS):
        total[p] = s[:, p * part : (p + 1) * part]
    for i in (15, 16, 17):
        loads[i].wait()
    ff = hs.shape[1]

    def by_distance(k):
        found = my_z
        for z in range(nz):
            inner = 1 if 2 * z < nz - 1 else -1
            near = sorted(range(nz), key=lambda s: (abs(s - z), -(s - z) * inner))
            for place in range(nz):
                found = jnp.where((my_z == z) & (k == place), near[place], found)
        return found

    def plane_copy(src, dst, sems, z, p, q_to, q_src, q_dst):
        return pltpu.make_async_remote_copy(
            src_ref=src.at[z, p, q_src],
            dst_ref=dst.at[z, p, q_dst],
            send_sem=sems[0].at[z, p],
            recv_sem=sems[1].at[z, p],
            device_id=device(my_z, q_to),
            device_id_type=MESH,
        )

    def plane_send(src, dst, sems, z, p):
        def one(o, _):
            q = (my_q + o) % plane
            plane_copy(src, dst, sems, z, p, q, q, my_q).start()
            return 0

        lax.fori_loop(1, plane, one, 0)
        dst[z, p, my_q] = src[z, p, my_q]

    def plane_all(src, dst, sems, z, p):
        others = pl.ds(0, plane - 1)
        return pltpu.make_async_remote_copy(
            src_ref=src.at[z, p, others],
            dst_ref=dst.at[z, p, others],
            send_sem=sems[0].at[z, p],
            recv_sem=sems[1].at[z, p],
            device_id=device(my_z, (my_q + 1) % plane),
            device_id_type=MESH,
        )

    out_way = (outgoing, incoming, (out_send, out_recv))
    back_way = (produced, returned, (back_send, back_recv))

    def dispatch(k, first, last):
        z = by_distance(k)

        def piece(p, _):
            @pl.when(k > 0)
            def _():
                line_copy(z, p, above, up_send).wait_recv()
                spread(z, p)

            block = jnp.dot(table_t[z], line[z, p], preferred_element_type=jnp.float32)
            outgoing[z, p] = block.astype(jnp.bfloat16).reshape(plane, cap, part)
            plane_send(*out_way, z, p)
            return 0

        lax.fori_loop(first, last, piece, 0)

    def expert(k, inline):
        z = by_distance(k)

        def arrive(p, _):
            plane_all(*out_way, z, p).wait_recv()
            return 0

        lax.fori_loop(0, PARTS, arrive, 0)

        def up_tile(t, _):
            at = pl.ds(pl.multiple_of(t * FF_TILE, FF_TILE), FF_TILE)
            x = jnp.concatenate(
                [incoming[z, p].reshape(rows_in, part) for p in range(PARTS)], axis=1
            )
            a = jnp.dot(x, gate_ref[0, :, at], preferred_element_type=jnp.float32)
            u = jnp.dot(x, up_ref[0, :, at], preferred_element_type=jnp.float32)
            hs[:, at] = (jax.nn.silu(a) * u).astype(jnp.bfloat16)
            return 0

        lax.fori_loop(0, ff // FF_TILE, up_tile, 0)

        def down_tile(p, _):
            at = pl.ds(pl.multiple_of(p * part, part), part)
            y = jnp.dot(hs[...], down_ref[0, :, at], preferred_element_type=jnp.float32)
            produced[z, p] = y.astype(jnp.bfloat16).reshape(plane, cap, part)

            @pl.when(inline)
            def _():
                plane_send(*back_way, z, p)

            return 0

        lax.fori_loop(0, PARTS, down_tile, 0)

    def send_back(k):
        def piece(p, _):
            plane_send(*back_way, by_distance(k), p)
            return 0

        lax.fori_loop(0, PARTS, piece, 0)

    def partial_copy(z, f):
        to = jnp.where(z < my_z, below, above)
        slot = jnp.where((z > my_z) & (to == z), nz, z)
        return pltpu.make_async_remote_copy(
            src_ref=partial_out.at[z, f],
            dst_ref=partial_in.at[slot, f],
            send_sem=part_send.at[z, f],
            recv_sem=part_recv.at[slot, f],
            device_id=device(to, my_q),
            device_id_type=MESH,
        )

    def partial_arrive(slot, f):
        pltpu.make_async_remote_copy(
            src_ref=partial_out.at[0, f],
            dst_ref=partial_in.at[slot, f],
            send_sem=part_send.at[0, f],
            recv_sem=part_recv.at[slot, f],
            device_id=device(above, my_q),
            device_id_type=MESH,
        ).wait_recv()

    fine = part // SUBS

    def combine(z, p):
        plane_all(*back_way, z, p).wait_recv()
        block = returned[z, p].reshape(rows_in, part)
        mine = jnp.dot(table_hi[z], block, preferred_element_type=jnp.float32) + jnp.dot(
            table_lo[z], block, preferred_element_type=jnp.float32
        )

        @pl.when(z == my_z)
        def _():
            total[p] += mine

        @pl.when((z != my_z) & edge)
        def _():
            for i in range(SUBS):
                f = p * SUBS + i
                partial_out[z, f] = mine[:, i * fine : (i + 1) * fine].astype(jnp.bfloat16)
                partial_copy(z, f).start()

        @pl.when((z != my_z) & ~edge)
        def _():
            total[PARTS] = mine
            for i in range(SUBS):
                f = p * SUBS + i
                partial_arrive(z, f)
                partial_out[z, f] = (
                    total[PARTS, :, i * fine : (i + 1) * fine]
                    + partial_in[z, f].astype(jnp.float32)
                ).astype(jnp.bfloat16)
                partial_copy(z, f).start()

    def combine_all(k):
        def one(p, _):
            combine(by_distance(k), p)
            return 0

        lax.fori_loop(0, PARTS, one, 0)

    dispatch(0, 0, PARTS)
    midway = PARTS // 2

    def tick(k, _):
        last = k == nz - 1
        stop = jnp.where(last, 0, PARTS)
        early = jnp.minimum(jnp.where(k == 0, midway, jnp.where(edge, jnp.where(k == 1, midway // 2, midway), PARTS)), stop)
        dispatch(k + 1, 0, early)

        @pl.when(~edge & (k == nz - 2))
        def _():
            send_back(1)

        expert(k, edge & (k > 0))
        dispatch(k + 1, early, stop)

        @pl.when(edge & (k > 0))
        def _():
            combine_all(k)

        return 0

    lax.fori_loop(0, nz, tick, 0)

    @pl.when(edge)
    def _():
        send_back(0)

    @pl.when(~edge)
    def _():
        for k in range(nz - 1, 1, -1):
            send_back(k)
        send_back(0)
        if nz > 2:
            combine_all(1)

        def one(s, _):
            for behind in range(nz - 2):
                p = s - behind

                @pl.when((p >= 0) & (p < PARTS))
                def _():
                    combine(by_distance(nz - 1 - behind), p)

            return 0

        lax.fori_loop(0, PARTS + max(nz - 3, 0), one, 0)

    combine_all(0)
    for f in range(PARTS * SUBS):
        p, at = f // SUBS, pl.ds(f % SUBS * fine, fine)

        @pl.when(has_above)
        def _():
            partial_arrive(my_z, f)
            total[p, :, at] += partial_in[my_z, f].astype(jnp.float32)

        @pl.when(has_below)
        def _():
            partial_arrive(nz, f)
            total[p, :, at] += partial_in[nz, f].astype(jnp.float32)

        out_ref[0, :, f * fine : (f + 1) * fine] = total[p, :, at].astype(jnp.bfloat16)

    def drain(i, _):
        z, p = i // PARTS, i % PARTS
        plane_all(*out_way, z, p).wait_send()
        plane_all(*back_way, z, p).wait_send()

        @pl.when((z <= my_z) & has_above)
        def _():
            line_copy(z, p, above, up_send).wait_send()

        @pl.when((z >= my_z) & has_below)
        def _():
            line_copy(z, p, below, down_send).wait_send()

        @pl.when(z != my_z)
        def _():
            for i in range(SUBS):
                partial_copy(z, p * SUBS + i).wait_send()

        return 0

    lax.fori_loop(0, nz * PARTS, drain, 0)
    for o in range(1, nz):
        meta_copy((my_z + o) % nz, my_z).wait_send()
    for o in range(1, half):
        for j in range(2):
            qkv_copy(o, j).wait_send()
            mixed_copy(o, j, my_rank).wait_send()
    param_copy(my_half).wait_send()
    state_copy().wait_send()
    own_copy().wait_send()
    for o in range(1, chips):
        for p in range(PIECES):
            wc_copy(o, p).wait_send()
        for j in range(direct):
            p = (first_piece + j) % PIECES
            wx_copy(o, p).wait_send()
            for yo in range(1, ny):
                if onward(j, yo):
                    wy_copy(o, p, yo).wait_send()


def on_device(
    residual_input,
    queries,
    keys,
    values,
    gate_logits,
    retention_offset,
    log_forget_extra,
    lane_amplifier,
    output_gate_logits,
    output_projection,
    cell_norm_gain,
    expert_norm_gain,
    expert_index,
    group_mixing_weight,
    within_group_weight,
    gate_weight,
    up_weight,
    down_weight,
):
    n, dpn = lax.axis_size("sp"), lax.axis_size("dp")
    tok, width = residual_input.shape[1:]
    dk, dv = queries.shape[2] // n, values.shape[2] // n
    half = n // 2
    length, devices, ff = half * tok, n * dpn, gate_weight.shape[2]
    cap, chips = 4 * tok // devices, dpn // 2
    ny = chips if n % chips == 0 else 1
    nz, plane = n // ny, ny * dpn
    rows_in, part = plane * cap, width // PARTS
    operands = (
        queries, keys, values, jnp.swapaxes(gate_logits, 1, 2), retention_offset, log_forget_extra,
        lane_amplifier.reshape(1, dv), output_gate_logits, output_projection,
        residual_input, cell_norm_gain.reshape(1, width), expert_norm_gain.reshape(1, width),
        jnp.swapaxes(expert_index, 1, 2), jnp.swapaxes(group_mixing_weight, 1, 2),
        jnp.swapaxes(within_group_weight, 1, 2),
        gate_weight, up_weight, down_weight,
    )
    dma = pltpu.SemaphoreType.DMA
    bf16, f32 = jnp.bfloat16, jnp.float32
    hbm = pl.BlockSpec(memory_space=pltpu.HBM)
    return pl.pallas_call(
        partial(layer_kernel, n=n, dpn=dpn, inputs=len(operands)),
        out_shape=pltpu.VMEM((1, tok, width), bf16),
        in_specs=[hbm] * len(operands),
        out_specs=pl.BlockSpec(memory_space=pltpu.VMEM),
        scratch_shapes=[pltpu.VMEM(x.shape, x.dtype) for x in operands]
        + [
            pltpu.VMEM((n, tok + GATE_ROWS, 2 * dk + dv), bf16),
            pltpu.VMEM((2, half, tok + GATE_ROWS, 2 * dk + dv), bf16),
            pltpu.VMEM((128, tok), f32),
            pltpu.VMEM((2, -(-(n + 2) // 8) * 8, max(tok, dv)), f32),
            pltpu.VMEM((2, 8, length), f32),
            pltpu.VMEM((2, length, 128), f32),
            pltpu.VMEM((n, tok, length), f32),
            pltpu.VMEM((n, tok, 128), f32),
            pltpu.VMEM((2, dk + GATE_ROWS, dv), bf16),
            pltpu.VMEM((2, dk + GATE_ROWS, dv), bf16),
            pltpu.VMEM((2, half, tok, dv), bf16),
            pltpu.VMEM((n, tok, dv), bf16),
            pltpu.VMEM((dpn,) + output_projection.shape, bf16),
            pltpu.VMEM((tok, width), f32),
            pltpu.VMEM((nz, 8, tok), f32),
            pltpu.VMEM((nz, rows_in, tok), bf16),
            pltpu.VMEM((nz, tok, rows_in), bf16),
            pltpu.VMEM((nz, tok, rows_in), bf16),
            pltpu.VMEM((nz, PARTS, tok, part), bf16),
            pltpu.VMEM((nz, PARTS, plane, cap, part), bf16),
            pltpu.VMEM((nz, PARTS, plane, cap, part), bf16),
            pltpu.VMEM((rows_in, ff), bf16),
            pltpu.VMEM((nz, PARTS, plane, cap, part), bf16),
            pltpu.VMEM((nz, PARTS, plane, cap, part), bf16),
            pltpu.VMEM((nz, PARTS * SUBS, tok, part // SUBS), bf16),
            pltpu.VMEM((nz + 1, PARTS * SUBS, tok, part // SUBS), bf16),
            pltpu.VMEM((PARTS + 1, tok, part), f32),
            dma((len(operands),)),
            dma((half, 2)), dma((half, 2)), dma(()), dma(()), dma(()), dma(()),
            dma((half, 2)), dma((half, 2)),
            dma((chips, PIECES)), dma((chips, PIECES)), dma((chips, PIECES, ny)),
            dma((chips, PIECES)), dma((chips, PIECES)),
            dma(()),
            dma((nz,)), dma((nz,)),
            dma((nz, PARTS)), dma((nz, PARTS)), dma((nz, PARTS)),
            dma((nz, PARTS)), dma((nz, PARTS)), dma((nz, PARTS)), dma((nz, PARTS)),
            dma((nz, PARTS * SUBS)), dma((nz + 1, PARTS * SUBS)),
        ],
        compiler_params=pltpu.CompilerParams(
            collective_id=0, has_side_effects=True, vmem_limit_bytes=60 * 1024 * 1024
        ),
    )(*operands)


def solution(mesh):
    in_specs = (
        P("dp", "sp", None),
        P("dp", "sp", None),
        P("dp", "sp", None),
        P("dp", "sp", None),
        P("dp", "sp", None),
        P("sp", None),
        P("dp", "sp", None),
        P("sp"),
        P("dp", "sp", None),
        P(None, "dp"),
        P(),
        P(),
        P("dp", "sp", None),
        P("dp", "sp", None),
        P("dp", "sp", None),
        P(("sp", "dp"), None, None),
        P(("sp", "dp"), None, None),
        P(("sp", "dp"), None, None),
    )
    out_specs = P("dp", "sp", None)
    return jax.shard_map(
        on_device, mesh=mesh, in_specs=in_specs, out_specs=out_specs, check_vma=False
    )
```

```python
from functools import partial

import jax
import jax.numpy as jnp
from jax import lax
from jax.experimental import pallas as pl
from jax.experimental.pallas import tpu as pltpu
from jax.sharding import PartitionSpec as P

EPS = 1e-06
MESH = pl.DeviceIdType.MESH
GATE_ROWS = 16
PARTS = 4
SUBS = 2
FF_TILE = 256
PIECES = 8
EXTRA = 1


def log_sigmoid(x):
    return jnp.minimum(x, 0.0) - jnp.log1p(jnp.exp(-jnp.abs(x)))


def layer_kernel(*refs, n, dpn, inputs):
    hbm, (out_ref,), rest = refs[:inputs], refs[inputs : inputs + 1], refs[inputs + 1 :]
    local, rest = rest[:inputs], rest[inputs:]
    (
        q_ref, k_ref, v_ref, g_ref, offset_ref, extra_ref, amp_ref, logits_ref, w_ref,
        res_ref, cell_gain_ref, expert_gain_ref, index_ref, group_ref, within_ref,
        gate_ref, up_ref, down_ref,
    ) = local
    (
        send, recv, gates_t, params, rows_of_gate, cols, weights, sums, state_out, state_in,
        mixed, mrecv, wfull, proj,
        meta, table_t, table_hi, table_lo, line, outgoing, incoming, hs, produced, returned,
        partial_out, partial_in, total, partial,
        in_sem, send_sem, recv_sem, param_send, param_recv, state_send, state_recv, msend_sem, mrecv_sem, wx_send, wx_recv, wy_send, wc_send,
        wc_recv, wl_sem, meta_send, meta_recv, up_send, down_send, line_recv,
        out_send, out_recv, back_send, back_recv, part_send, part_recv,
    ) = rest
    loads = [pltpu.make_async_copy(hbm[i], local[i], in_sem.at[i]) for i in range(inputs)]
    early = (0, 1, 2, 3, 8)
    for i in early:
        loads[i].start()
    tok = q_ref.shape[1]
    dk = q_ref.shape[2] // n
    dv = v_ref.shape[2] // n
    half = n // 2
    length = half * tok
    wcol = w_ref.shape[1]
    me = lax.axis_index("sp")
    my_half, my_rank = me // half, me % half
    first = my_half * half
    opposite = (me + half) % n
    my_dp = lax.axis_index("dp")
    my_x, my_core = my_dp // 2, my_dp % 2
    chips = dpn // 2

    barrier = pltpu.get_barrier_semaphore()

    devices = n * dpn
    cap = 4 * tok // devices
    ny = chips if n % chips == 0 else 1
    nz = n // ny
    plane = ny * dpn
    my_z, my_y = me // ny, me % ny
    my_q = my_y * dpn + my_dp

    def device(z, q):
        return {"sp": z * ny + q // dpn, "dp": q % dpn}

    def greet_sp(o, _):
        pl.semaphore_signal(
            barrier, inc=1, device_id={"sp": (me + o) % n, "dp": my_dp}, device_id_type=MESH
        )
        return 0

    def greet_plane(o, _):
        pl.semaphore_signal(
            barrier, inc=1, device_id=device(my_z, (my_q + o) % plane), device_id_type=MESH
        )
        return 0

    lax.fori_loop(1, n, greet_sp, 0)
    lax.fori_loop(1, plane, greet_plane, 0)
    for load in loads[:4]:
        load.wait()

    for h in range(n):
        send[h, 0:tok, 0:dk] = k_ref[0, :, h * dk : (h + 1) * dk]
        send[h, 0:tok, dk : 2 * dk] = q_ref[0, :, h * dk : (h + 1) * dk]
        send[h, 0:tok, 2 * dk : 2 * dk + dv] = v_ref[0, :, h * dv : (h + 1) * dv]
    gate_rows = g_ref.shape[1]
    gates_t[0:gate_rows] = g_ref[0].astype(jnp.float32)
    gates_t[gate_rows:] = jnp.zeros((128 - gate_rows, tok), jnp.float32)
    for h in range(n):
        send[h, tok : tok + GATE_ROWS, 0:tok] = gates_t[4 * h : 4 * h + GATE_ROWS, :].astype(
            jnp.bfloat16
        )
        send[h, tok : tok + GATE_ROWS, tok:] = jnp.zeros(
            (GATE_ROWS, send.shape[2] - tok), jnp.bfloat16
        )

    pl.semaphore_wait(barrier, n - 1 + plane - 1)
    for i in range(inputs):
        if i not in early:
            loads[i].start()

    def all_of(ref, send_sem, recv_sem):
        return pltpu.make_async_remote_copy(
            src_ref=ref,
            dst_ref=ref,
            send_sem=send_sem,
            recv_sem=recv_sem,
            device_id={"sp": opposite, "dp": my_dp},
            device_id_type=MESH,
        )

    def qkv_copy(o, j):
        return pltpu.make_async_remote_copy(
            src_ref=send.at[(my_rank + o) % half + j * half],
            dst_ref=recv.at[j, my_rank],
            send_sem=send_sem,
            recv_sem=recv_sem,
            device_id={"sp": first + (my_rank + o) % half, "dp": my_dp},
            device_id_type=MESH,
        )

    def qkv_all():
        return all_of(send.at[pl.ds(0, 2 * (half - 1))], send_sem, recv_sem)

    def param_copy(slot):
        return pltpu.make_async_remote_copy(
            src_ref=params.at[my_half],
            dst_ref=params.at[slot],
            send_sem=param_send,
            recv_sem=param_recv,
            device_id={"sp": opposite, "dp": my_dp},
            device_id_type=MESH,
        )

    def state_copy():
        return pltpu.make_async_remote_copy(
            src_ref=state_out,
            dst_ref=state_in,
            send_sem=state_send,
            recv_sem=state_recv,
            device_id={"sp": opposite, "dp": my_dp},
            device_id_type=MESH,
        )

    piece = w_ref.shape[0] // PIECES

    share = PIECES // ny
    direct = share + (EXTRA if ny > 1 else 0)
    first_piece = my_y * share

    def rows_of(p):
        return pl.ds(pl.multiple_of(p * piece, piece), piece)

    def wx_copy(o, p):
        return pltpu.make_async_remote_copy(
            src_ref=w_ref.at[rows_of(p)],
            dst_ref=wfull.at[my_dp, rows_of(p)],
            send_sem=wx_send.at[o - 1],
            recv_sem=wx_recv.at[o - 1, p],
            device_id={"sp": me, "dp": ((my_x + o) % chips) * 2 + my_core},
            device_id_type=MESH,
        )

    def from_chip(o):
        return ((my_x + chips - o) % chips) * 2 + my_core

    def wy_copy(o, p, yo):
        return pltpu.make_async_remote_copy(
            src_ref=wfull.at[from_chip(o), rows_of(p)],
            dst_ref=wfull.at[from_chip(o), rows_of(p)],
            send_sem=wy_send.at[o - 1, yo - 1],
            recv_sem=wx_recv.at[o - 1, p],
            device_id={"sp": my_z * ny + (my_y + yo) % ny, "dp": my_dp},
            device_id_type=MESH,
        )

    def wc_copy(o, p):
        return pltpu.make_async_remote_copy(
            src_ref=wfull.at[from_chip(o), rows_of(p)],
            dst_ref=wfull.at[from_chip(o), rows_of(p)],
            send_sem=wc_send.at[o],
            recv_sem=wc_recv.at[o],
            device_id={"sp": me, "dp": my_x * 2 + 1 - my_core},
            device_id_type=MESH,
        )

    def own_copy():
        return pltpu.make_async_remote_copy(
            src_ref=w_ref,
            dst_ref=wfull.at[my_dp],
            send_sem=wc_send.at[0],
            recv_sem=wc_recv.at[0],
            device_id={"sp": me, "dp": my_x * 2 + 1 - my_core},
            device_id_type=MESH,
        )

    def onward(j, yo):
        return j < share and (j >= EXTRA or yo < ny - 1)

    def pass_on(j):
        p = (first_piece + j) % PIECES
        for o in range(1, chips):
            wx_copy(o, p).wait_recv()
            wc_copy(o, p).start()
            for yo in range(1, ny):
                if onward(j, yo):
                    wy_copy(o, p, yo).start()

    for o in range(1, half):
        for j in range(2):
            qkv_copy(o, j).start()
    loads[8].wait()
    for j in range(direct):
        for o in range(1, chips):
            wx_copy(o, (first_piece + j) % PIECES).start()
    own_copy().start()
    own_w = pltpu.make_async_copy(w_ref, wfull.at[my_dp], wl_sem)
    own_w.start()
    for j in range(2):
        recv[j, my_rank] = send[my_rank + j * half]
    for i in (4, 5, 6, 7, 9, 10, 11, 12, 13, 14):
        loads[i].wait()
    for d in range(n):
        params[my_half, d : d + 1, 0:tok] = extra_ref[0, :, d * tok : (d + 1) * tok]
    params[my_half, n : n + 1, 0:dv] = amp_ref[...]
    lane_p = lax.broadcasted_iota(jnp.int32, (1, params.shape[2]), 1)
    params[my_half, n + 1 : n + 2] = jnp.where(
        lane_p == 0, offset_ref[0:1, 0:1], offset_ref[0:1, 1:2]
    )
    param_copy(my_half).start()

    rows_in = plane * cap
    ids = index_ref[0].astype(jnp.float32)
    e_0, e_1 = ids[0:1], ids[1:2]
    wide = -(-devices // 128) * 128
    sub_e = lax.broadcasted_iota(jnp.int32, (wide, tok), 0).astype(jnp.float32)
    hit_0 = jnp.where(sub_e == e_0, 1.0, 0.0)
    hit_1 = jnp.where(sub_e == e_1, 1.0, 0.0)
    tri = jnp.where(
        lax.broadcasted_iota(jnp.int32, (tok, tok), 0)
        < lax.broadcasted_iota(jnp.int32, (tok, tok), 1),
        1.0,
        0.0,
    ).astype(jnp.bfloat16)
    rank_0 = jnp.dot(hit_0.astype(jnp.bfloat16), tri, preferred_element_type=jnp.float32)
    rank_1 = jnp.dot(hit_1.astype(jnp.bfloat16), tri, preferred_element_type=jnp.float32)
    rank_1 = rank_1 + jnp.sum(hit_0, axis=1, keepdims=True)
    place_0 = e_0 * cap + jnp.sum(hit_0 * rank_0, axis=0, keepdims=True)
    place_1 = e_1 * cap + jnp.sum(hit_1 * rank_1, axis=0, keepdims=True)
    groups = group_ref.shape[1]
    span = devices // groups
    route_0 = jnp.zeros((1, tok), jnp.float32)
    route_1 = jnp.zeros((1, tok), jnp.float32)
    for c in range(groups):
        weight_c = group_ref[0, c : c + 1, :]
        route_0 += jnp.where((e_0 >= c * span) & (e_0 < (c + 1) * span), weight_c, 0.0)
        route_1 += jnp.where((e_1 >= c * span) & (e_1 < (c + 1) * span), weight_c, 0.0)
    route_0 = route_0 * within_ref[0, 0:1, :]
    route_1 = route_1 * within_ref[0, 1:2, :]
    sub_m = lax.broadcasted_iota(jnp.int32, (8, tok), 0)
    meta[my_z] = jnp.where(
        sub_m == 0,
        place_0,
        jnp.where(sub_m == 1, place_1, jnp.where(sub_m == 2, route_0, route_1)),
    )

    def meta_copy(z, slot):
        return pltpu.make_async_remote_copy(
            src_ref=meta.at[my_z],
            dst_ref=meta.at[slot],
            send_sem=meta_send,
            recv_sem=meta_recv,
            device_id=device(z, my_q),
            device_id_type=MESH,
        )

    for o in range(1, nz):
        meta_copy((my_z + o) % nz, my_z).start()

    stops = [PIECES * i // 8 for i in (2, 3, 4, 8, 8)]

    def pass_until(i):
        for j in range(stops[i - 1] if i else 0, stops[i]):
            pass_on(j)

    pass_until(0)
    if half > 1:
        qkv_all().wait_recv()
    param_copy(1 - my_half).wait_recv()

    upper = my_half == 1
    lane = lax.broadcasted_iota(jnp.int32, (8, length), 1)
    sub = lax.broadcasted_iota(jnp.int32, (8, length), 0)
    gates, f, b = [], [], []
    for j in range(2):
        gates.append(
            jnp.concatenate(
                [recv[j, d, tok : tok + GATE_ROWS, 0:tok].astype(jnp.float32) for d in range(half)],
                axis=1,
            )
        )
        extra = jnp.concatenate(
            [params[j, pl.ds(first + d, 1), 0:tok] for d in range(half)], axis=1
        )
        offset = params[j, n + 1 : n + 2]
        f.append(log_sigmoid(gates[j][1:2] + offset[:, 0:1]) + extra)
        b.append(log_sigmoid(gates[j][3:4] + offset[:, 1:2]) + extra)
    f = jnp.where(sub == 0, f[0], f[1])
    b = jnp.where(sub == 0, b[0], b[1])
    step = 1
    while step < length:
        f = f + jnp.where(lane >= step, pltpu.roll(f, step, 1), 0.0)
        b = b + jnp.where(lane < length - step, pltpu.roll(b, length - step, 1), 0.0)
        step *= 2
    wide_sub = lax.broadcasted_iota(jnp.int32, (128, length), 0)
    for j in range(2):
        row_i = gates[j][0:1]
        row_f = row_i - f[j : j + 1]
        row_b = gates[j][2:3] - b[j : j + 1]
        rows_of_gate[j] = jnp.where(sub == 0, row_f, row_b)
        leaving = jnp.exp(
            jnp.where(upper, row_b + b[j : j + 1, 0:1], row_f + f[j : j + 1, length - 1 : length])
        )
        stacked = jnp.where(wide_sub == 0, f[j : j + 1], jnp.where(wide_sub == 1, b[j : j + 1], row_i))
        cols[j] = jnp.where(wide_sub == 3, leaving, stacked).T

    scale = dk ** (-0.5)

    def state(j, _):
        kq = recv[j, :, 0:tok, 0 : 2 * dk].reshape(length, 2 * dk).astype(jnp.float32)
        kq = kq * cols[j][:, 3:4]
        memory = lax.dot_general(
            kq.astype(jnp.bfloat16),
            recv[j, :, 0:tok, 2 * dk : 2 * dk + dv].reshape(length, dv),
            (((0,), (0,)), ((), ())),
            preferred_element_type=jnp.float32,
        )
        normal = jnp.sum(kq, axis=0, keepdims=True)
        high = normal.astype(jnp.bfloat16).astype(jnp.float32)
        at = lax.broadcasted_iota(jnp.int32, (GATE_ROWS, 2 * dk), 0)
        state_out[j, 0:dk] = memory[0:dk].astype(jnp.bfloat16)
        state_out[j, dk:, 0 : 2 * dk] = jnp.where(
            at == 0, high, jnp.where(at == 1, normal - high, 0.0)
        ).astype(jnp.bfloat16)
        return 0

    lax.fori_loop(0, 2, state, 0)
    state_copy().start()
    pass_until(1)

    def mixed_copy(o, j, rank):
        return pltpu.make_async_remote_copy(
            src_ref=mixed.at[j, (my_rank + o) % half],
            dst_ref=mrecv.at[rank + j * half],
            send_sem=msend_sem,
            recv_sem=mrecv_sem,
            device_id={"sp": first + (my_rank + o) % half, "dp": my_dp},
            device_id_type=MESH,
        )

    def mixed_all():
        return all_of(mrecv.at[pl.ds(0, 2 * (half - 1))], msend_sem, mrecv_sem)

    def scaled(j, d):
        return recv[j, d, 0:tok, dk : 2 * dk].astype(jnp.float32) * scale

    def before_of(d):
        t_pos = d * tok + lax.broadcasted_iota(jnp.int32, (tok, length), 0)
        return lax.broadcasted_iota(jnp.int32, (tok, length), 1) < t_pos

    lane_z = lax.broadcasted_iota(jnp.int32, (tok, 128), 1)

    def weigh_head(d, k, j):
        m = 2 * k + j
        start = pl.multiple_of(d * tok, tok)
        qs = scaled(j, d)
        ks = recv[j, d, 0:tok, 0:dk].astype(jnp.float32)
        diag = jnp.sum(qs * ks, axis=1, keepdims=True)
        qs = jnp.concatenate([qs, jnp.zeros_like(qs)], axis=1).astype(jnp.bfloat16)
        kall = recv[j, :, 0:tok, 0 : 2 * dk].reshape(length, 2 * dk)
        scores = lax.dot_general(
            qs, kall, (((1,), (1,)), ((), ())), preferred_element_type=jnp.float32
        )
        col = cols[j, pl.ds(start, tok), :]
        col_f, col_b, col_i = col[:, 0:1], col[:, 1:2], col[:, 2:3]
        before = before_of(d)
        rows = rows_of_gate[j]
        weight = scores * jnp.exp(jnp.where(before, col_f + rows[0:1], col_b + rows[1:2]))
        weights[m] = weight
        diag = diag * jnp.exp(col_i)
        z_f = jnp.sum(jnp.where(before, weight, 0.0), axis=1, keepdims=True) + diag
        z_b = jnp.sum(jnp.where(before, 0.0, weight), axis=1, keepdims=True)
        sums[m] = jnp.where(lane_z == 0, z_f, jnp.where(lane_z == 1, z_b, diag))
    def weigh(k, _):
        for j in range(2):
            weigh_head((my_rank + 1 + k) % half, k, j)
        return 0

    lax.fori_loop(0, half, weigh, 0)
    pass_until(2)
    state_copy().wait_recv()

    def segment_head(d, k, j):
        m = 2 * k + j
        start = pl.multiple_of(d * tok, tok)
        col = cols[j, pl.ds(start, tok), :]
        carried = jnp.exp(jnp.where(upper, col[:, 0:1], col[:, 1:2]))
        qs = scaled(j, d) * carried
        normal = state_in[j, dk:, 0:dk].astype(jnp.float32)
        z_state = jnp.sum(qs * (normal[0:1] + normal[1:2]), axis=1, keepdims=True)
        z = sums[m]
        z_f, z_b, diag = z[:, 0:1], z[:, 1:2], z[:, 2:3]
        z_f = z_f + jnp.where(upper, z_state, 0.0)
        z_b = z_b + jnp.where(upper, 0.0, z_state)
        inv_f = 1.0 / jnp.maximum(jnp.abs(z_f), 1.0)
        inv_b = 1.0 / jnp.maximum(jnp.abs(z_b), 1.0)
        probs = (weights[m] * jnp.where(before_of(d), inv_f, inv_b)).astype(jnp.bfloat16)
        vall = recv[j, :, 0:tok, 2 * dk : 2 * dk + dv].reshape(length, dv)
        total = jnp.dot(probs, vall, preferred_element_type=jnp.float32)
        total = total + jnp.dot(
            (qs * jnp.where(upper, inv_f, inv_b)).astype(jnp.bfloat16),
            state_in[j, 0:dk],
            preferred_element_type=jnp.float32,
        )
        total = total + (diag * inv_f) * recv[j, d, 0:tok, 2 * dk : 2 * dk + dv].astype(jnp.float32)
        amp = params[j, n : n + 1, 0:dv]
        total = total * lax.rsqrt(jnp.mean(total * total, axis=1, keepdims=True) + EPS) * amp
        mixed[j, d] = total.astype(jnp.bfloat16)

    def segment(k, _):
        d = (my_rank + 1 + k) % half
        for j in range(2):
            segment_head(d, k, j)

        @pl.when(k < half - 1)
        def _():
            for j in range(2):
                mixed_copy(k + 1, j, my_rank).start()

        return 0

    lax.fori_loop(0, half, segment, 0)
    pass_until(3)
    for j in range(2):
        mrecv[my_rank + j * half] = mixed[j, my_rank]
    sub_r = lax.broadcasted_iota(jnp.int32, (rows_in, tok), 0).astype(jnp.float32)
    at = sub_r + (my_z * rows_in).astype(jnp.float32)

    def tables(o, _):
        z = (my_z + o) % nz

        rows = meta[z]
        hit_0, hit_1 = at == rows[0:1], at == rows[1:2]
        table_t[z] = (jnp.where(hit_0, 1.0, 0.0) + jnp.where(hit_1, 1.0, 0.0)).astype(jnp.bfloat16)
        weighted = (jnp.where(hit_0, rows[2:3], 0.0) + jnp.where(hit_1, rows[3:4], 0.0)).T
        high = weighted.astype(jnp.bfloat16)
        table_hi[z] = high
        table_lo[z] = (weighted - high.astype(jnp.float32)).astype(jnp.bfloat16)
        return 0

    if nz > 1:
        all_of(meta.at[pl.ds(0, nz - 1)], meta_send, meta_recv).wait_recv()
    lax.fori_loop(0, nz, tables, 0)
    sig = jax.nn.sigmoid(logits_ref[0].astype(jnp.float32))
    pass_until(4)
    if half > 1:
        mixed_all().wait_recv()
    gated = jnp.concatenate([mrecv[h].astype(jnp.float32) for h in range(n)], axis=1) * sig
    gated = gated.astype(jnp.bfloat16)
    own_w.wait()
    for o in range(chips):
        all_of(w_ref, wc_send.at[o], wc_recv.at[o]).wait_recv()
    for j in range(dpn):
        proj[:, j * wcol : (j + 1) * wcol] = jnp.dot(
            gated, wfull[j], preferred_element_type=jnp.float32
        )
    p = proj[...]
    stream = (
        res_ref[0].astype(jnp.float32)
        + cell_gain_ref[...] * p * lax.rsqrt(jnp.mean(p * p, axis=1, keepdims=True) + EPS)
    ).astype(jnp.bfloat16)
    s = stream.astype(jnp.float32)
    width = s.shape[1]
    part = width // PARTS
    moe = (
        expert_gain_ref[...] * s * lax.rsqrt(jnp.mean(s * s, axis=1, keepdims=True) + EPS)
    ).astype(jnp.bfloat16)

    def line_copy(z, p, to, sems):
        return pltpu.make_async_remote_copy(
            src_ref=line.at[z, p],
            dst_ref=line.at[z, p],
            send_sem=sems.at[z],
            recv_sem=line_recv.at[z, p],
            device_id=device(to, my_q),
            device_id_type=MESH,
        )

    above, below = (my_z + 1) % nz, (my_z + nz - 1) % nz
    has_above, has_below = my_z + 1 < nz, my_z > 0
    edge = (my_z == 0) | (my_z == nz - 1)

    def spread(z, p):
        @pl.when((z <= my_z) & has_above)
        def _():
            line_copy(z, p, above, up_send).start()

        @pl.when((z >= my_z) & has_below)
        def _():
            line_copy(z, p, below, down_send).start()

    for p in range(PARTS):
        line[my_z, p] = moe[:, p * part : (p + 1) * part]
        spread(my_z, p)
    for p in range(PARTS):
        total[p] = s[:, p * part : (p + 1) * part]
    for i in (15, 16, 17):
        loads[i].wait()
    ff = hs.shape[1]

    def by_distance(k):
        found = my_z
        for z in range(nz):
            inner = 1 if 2 * z < nz - 1 else -1
            near = sorted(range(nz), key=lambda s: (abs(s - z), -(s - z) * inner))
            for place in range(nz):
                found = jnp.where((my_z == z) & (k == place), near[place], found)
        return found

    def plane_copy(src, dst, sems, z, p, q_to, q_src, q_dst):
        return pltpu.make_async_remote_copy(
            src_ref=src.at[z, p, q_src],
            dst_ref=dst.at[z, p, q_dst],
            send_sem=sems[0],
            recv_sem=sems[1].at[z, p],
            device_id=device(my_z, q_to),
            device_id_type=MESH,
        )

    def plane_send(src, dst, sems, z, p):
        def one(o, _):
            q = (my_q + o) % plane
            plane_copy(src, dst, sems, z, p, q, q, my_q).start()
            return 0

        lax.fori_loop(1, plane, one, 0)
        dst[z, p, my_q] = src[z, p, my_q]

    def plane_all(src, dst, sems, z, p):
        others = pl.ds(0, plane - 1)
        return pltpu.make_async_remote_copy(
            src_ref=src.at[z, p, others],
            dst_ref=dst.at[z, p, others],
            send_sem=sems[0],
            recv_sem=sems[1].at[z, p],
            device_id=device(my_z, (my_q + 1) % plane),
            device_id_type=MESH,
        )

    out_way = (outgoing, incoming, (out_send, out_recv))
    back_way = (produced, returned, (back_send, back_recv))

    def dispatch(k, first, last):
        z = by_distance(k)

        def piece(p, _):
            @pl.when(k > 0)
            def _():
                line_copy(z, p, above, up_send).wait_recv()
                spread(z, p)

            block = jnp.dot(table_t[z], line[z, p], preferred_element_type=jnp.float32)
            outgoing[z, p] = block.astype(jnp.bfloat16).reshape(plane, cap, part)
            plane_send(*out_way, z, p)
            return 0

        lax.fori_loop(first, last, piece, 0)

    def expert(k, inline):
        z = by_distance(k)

        def arrive(p, _):
            plane_all(*out_way, z, p).wait_recv()
            return 0

        split = max(PARTS // 2, 1)

        def sides(first, last, at):
            x = jnp.concatenate(
                [incoming[z, p].reshape(rows_in, part) for p in range(first, last)], axis=1
            )
            rows = slice(first * part, last * part)
            a = jnp.dot(x, gate_ref[0, rows, at], preferred_element_type=jnp.float32)
            u = jnp.dot(x, up_ref[0, rows, at], preferred_element_type=jnp.float32)
            return a, u

        def begin_tile(t, _):
            at = pl.ds(pl.multiple_of(t * FF_TILE, FF_TILE), FF_TILE)
            partial[0, :, at], partial[1, :, at] = sides(0, split, at)
            return 0

        def up_tile(t, _):
            at = pl.ds(pl.multiple_of(t * FF_TILE, FF_TILE), FF_TILE)
            a, u = sides(split, PARTS, at)
            a, u = a + partial[0, :, at], u + partial[1, :, at]
            hs[:, at] = (jax.nn.silu(a) * u).astype(jnp.bfloat16)
            return 0

        lax.fori_loop(0, split, arrive, 0)
        lax.fori_loop(0, ff // FF_TILE, begin_tile, 0)
        lax.fori_loop(split, PARTS, arrive, 0)
        lax.fori_loop(0, ff // FF_TILE, up_tile, 0)

        def down_tile(p, _):
            at = pl.ds(pl.multiple_of(p * part, part), part)
            y = jnp.dot(hs[...], down_ref[0, :, at], preferred_element_type=jnp.float32)
            produced[z, p] = y.astype(jnp.bfloat16).reshape(plane, cap, part)

            @pl.when(inline)
            def _():
                plane_send(*back_way, z, p)

            return 0

        lax.fori_loop(0, PARTS, down_tile, 0)

    def send_back(k):
        def piece(p, _):
            plane_send(*back_way, by_distance(k), p)
            return 0

        lax.fori_loop(0, PARTS, piece, 0)

    def partial_copy(z, f):
        to = jnp.where(z < my_z, below, above)
        slot = jnp.where((z > my_z) & (to == z), nz, z)
        return pltpu.make_async_remote_copy(
            src_ref=partial_out.at[z, f],
            dst_ref=partial_in.at[slot, f],
            send_sem=part_send,
            recv_sem=part_recv.at[slot, f],
            device_id=device(to, my_q),
            device_id_type=MESH,
        )

    def partial_arrive(slot, f):
        pltpu.make_async_remote_copy(
            src_ref=partial_out.at[0, f],
            dst_ref=partial_in.at[slot, f],
            send_sem=part_send,
            recv_sem=part_recv.at[slot, f],
            device_id=device(above, my_q),
            device_id_type=MESH,
        ).wait_recv()

    fine = part // SUBS

    def combine(z, p):
        plane_all(*back_way, z, p).wait_recv()
        block = returned[z, p].reshape(rows_in, part)
        mine = jnp.dot(table_hi[z], block, preferred_element_type=jnp.float32) + jnp.dot(
            table_lo[z], block, preferred_element_type=jnp.float32
        )

        @pl.when(z == my_z)
        def _():
            total[p] += mine

        @pl.when((z != my_z) & edge)
        def _():
            for i in range(SUBS):
                f = p * SUBS + i
                partial_out[z, f] = mine[:, i * fine : (i + 1) * fine].astype(jnp.bfloat16)
                partial_copy(z, f).start()

        @pl.when((z != my_z) & ~edge)
        def _():
            total[PARTS] = mine
            for i in range(SUBS):
                f = p * SUBS + i
                partial_arrive(z, f)
                partial_out[z, f] = (
                    total[PARTS, :, i * fine : (i + 1) * fine]
                    + partial_in[z, f].astype(jnp.float32)
                ).astype(jnp.bfloat16)
                partial_copy(z, f).start()

    def combine_all(k):
        def one(p, _):
            combine(by_distance(k), p)
            return 0

        lax.fori_loop(0, PARTS, one, 0)

    dispatch(0, 0, PARTS)
    midway = PARTS // 2

    def tick(k, _):
        last = k == nz - 1
        stop = jnp.where(last, 0, PARTS)
        early = jnp.minimum(jnp.where(k == 0, midway, jnp.where(edge, jnp.where(k == 1, midway // 2, midway), PARTS)), stop)
        dispatch(k + 1, 0, early)

        @pl.when(~edge & (k == nz - 2))
        def _():
            send_back(1)

        expert(k, edge & (k > 0))
        dispatch(k + 1, early, stop)

        @pl.when(edge & (k > 0))
        def _():
            combine_all(k)

        return 0

    lax.fori_loop(0, nz, tick, 0)

    @pl.when(edge)
    def _():
        send_back(0)

    @pl.when(~edge)
    def _():
        for k in range(nz - 1, 1, -1):
            send_back(k)
        send_back(0)
        if nz > 2:
            combine_all(1)

        def one(s, _):
            for behind in range(nz - 2):
                p = s - behind

                @pl.when((p >= 0) & (p < PARTS))
                def _():
                    combine(by_distance(nz - 1 - behind), p)

            return 0

        lax.fori_loop(0, PARTS + max(nz - 3, 0), one, 0)

    combine_all(0)
    for f in range(PARTS * SUBS):
        p, at = f // SUBS, pl.ds(f % SUBS * fine, fine)

        @pl.when(has_above)
        def _():
            partial_arrive(my_z, f)
            total[p, :, at] += partial_in[my_z, f].astype(jnp.float32)

        @pl.when(has_below)
        def _():
            partial_arrive(nz, f)
            total[p, :, at] += partial_in[nz, f].astype(jnp.float32)

        out_ref[0, :, f * fine : (f + 1) * fine] = total[p, :, at].astype(jnp.bfloat16)

    def drain(z, _):
        @pl.when((z <= my_z) & has_above)
        def _():
            all_of(line.at[z], up_send.at[z], meta_recv).wait_send()

        @pl.when((z >= my_z) & has_below)
        def _():
            all_of(line.at[z], down_send.at[z], meta_recv).wait_send()

        return 0

    lax.fori_loop(0, nz, drain, 0)
    if nz > 1:
        all_of(meta.at[pl.ds(0, nz - 1)], meta_send, meta_recv).wait_send()
        all_of(partial_out.at[pl.ds(0, nz - 1)], part_send, meta_recv).wait_send()
    others = pl.ds(0, plane - 1)
    all_of(outgoing.at[:, :, others], out_send, meta_recv).wait_send()
    all_of(produced.at[:, :, others], back_send, meta_recv).wait_send()
    if half > 1:
        qkv_all().wait_send()
        mixed_all().wait_send()
    param_copy(my_half).wait_send()
    state_copy().wait_send()
    for o in range(chips):
        all_of(w_ref, wc_send.at[o], wc_recv.at[o]).wait_send()
    for o in range(1, chips):
        held = w_ref.at[pl.ds(0, direct * piece)]
        all_of(held, wx_send.at[o - 1], wc_recv.at[0]).wait_send()
        for yo in range(1, ny):
            held = w_ref.at[pl.ds(0, sum(onward(j, yo) for j in range(share)) * piece)]
            all_of(held, wy_send.at[o - 1, yo - 1], wc_recv.at[0]).wait_send()


def on_device(
    residual_input,
    queries,
    keys,
    values,
    gate_logits,
    retention_offset,
    log_forget_extra,
    lane_amplifier,
    output_gate_logits,
    output_projection,
    cell_norm_gain,
    expert_norm_gain,
    expert_index,
    group_mixing_weight,
    within_group_weight,
    gate_weight,
    up_weight,
    down_weight,
):
    n, dpn = lax.axis_size("sp"), lax.axis_size("dp")
    tok, width = residual_input.shape[1:]
    dk, dv = queries.shape[2] // n, values.shape[2] // n
    half = n // 2
    length, devices, ff = half * tok, n * dpn, gate_weight.shape[2]
    cap, chips = 4 * tok // devices, dpn // 2
    ny = chips if n % chips == 0 else 1
    nz, plane = n // ny, ny * dpn
    rows_in, part = plane * cap, width // PARTS
    operands = (
        queries, keys, values, jnp.swapaxes(gate_logits, 1, 2), retention_offset, log_forget_extra,
        lane_amplifier.reshape(1, dv), output_gate_logits, output_projection,
        residual_input, cell_norm_gain.reshape(1, width), expert_norm_gain.reshape(1, width),
        jnp.swapaxes(expert_index, 1, 2), jnp.swapaxes(group_mixing_weight, 1, 2),
        jnp.swapaxes(within_group_weight, 1, 2),
        gate_weight, up_weight, down_weight,
    )
    dma = pltpu.SemaphoreType.DMA
    bf16, f32 = jnp.bfloat16, jnp.float32
    hbm = pl.BlockSpec(memory_space=pltpu.HBM)
    return pl.pallas_call(
        partial(layer_kernel, n=n, dpn=dpn, inputs=len(operands)),
        out_shape=pltpu.VMEM((1, tok, width), bf16),
        in_specs=[hbm] * len(operands),
        out_specs=pl.BlockSpec(memory_space=pltpu.VMEM),
        scratch_shapes=[pltpu.VMEM(x.shape, x.dtype) for x in operands]
        + [
            pltpu.VMEM((n, tok + GATE_ROWS, 2 * dk + dv), bf16),
            pltpu.VMEM((2, half, tok + GATE_ROWS, 2 * dk + dv), bf16),
            pltpu.VMEM((128, tok), f32),
            pltpu.VMEM((2, -(-(n + 2) // 8) * 8, max(tok, dv)), f32),
            pltpu.VMEM((2, 8, length), f32),
            pltpu.VMEM((2, length, 128), f32),
            pltpu.VMEM((n, tok, length), f32),
            pltpu.VMEM((n, tok, 128), f32),
            pltpu.VMEM((2, dk + GATE_ROWS, dv), bf16),
            pltpu.VMEM((2, dk + GATE_ROWS, dv), bf16),
            pltpu.VMEM((2, half, tok, dv), bf16),
            pltpu.VMEM((n, tok, dv), bf16),
            pltpu.VMEM((dpn,) + output_projection.shape, bf16),
            pltpu.VMEM((tok, width), f32),
            pltpu.VMEM((nz, 8, tok), f32),
            pltpu.VMEM((nz, rows_in, tok), bf16),
            pltpu.VMEM((nz, tok, rows_in), bf16),
            pltpu.VMEM((nz, tok, rows_in), bf16),
            pltpu.VMEM((nz, PARTS, tok, part), bf16),
            pltpu.VMEM((nz, PARTS, plane, cap, part), bf16),
            pltpu.VMEM((nz, PARTS, plane, cap, part), bf16),
            pltpu.VMEM((rows_in, ff), bf16),
            pltpu.VMEM((nz, PARTS, plane, cap, part), bf16),
            pltpu.VMEM((nz, PARTS, plane, cap, part), bf16),
            pltpu.VMEM((nz, PARTS * SUBS, tok, part // SUBS), bf16),
            pltpu.VMEM((nz + 1, PARTS * SUBS, tok, part // SUBS), bf16),
            pltpu.VMEM((PARTS + 1, tok, part), f32),
            pltpu.VMEM((2, rows_in, ff), f32),
            dma((len(operands),)),
            dma(()), dma(()), dma(()), dma(()), dma(()), dma(()), dma(()), dma(()),
            dma((max(chips - 1, 1),)), dma((max(chips - 1, 1), PIECES)),
            dma((max(chips - 1, 1), max(ny - 1, 1))), dma((chips,)), dma((chips,)),
            dma(()), dma(()), dma(()),
            dma((nz,)), dma((nz,)), dma((nz, PARTS)),
            dma(()), dma((nz, PARTS)), dma(()), dma((nz, PARTS)),
            dma(()), dma((nz + 1, PARTS * SUBS)),
        ],
        compiler_params=pltpu.CompilerParams(
            collective_id=0, has_side_effects=True, vmem_limit_bytes=60 * 1024 * 1024
        ),
    )(*operands)


def solution(mesh):
    in_specs = (
        P("dp", "sp", None),
        P("dp", "sp", None),
        P("dp", "sp", None),
        P("dp", "sp", None),
        P("dp", "sp", None),
        P("sp", None),
        P("dp", "sp", None),
        P("sp"),
        P("dp", "sp", None),
        P(None, "dp"),
        P(),
        P(),
        P("dp", "sp", None),
        P("dp", "sp", None),
        P("dp", "sp", None),
        P(("sp", "dp"), None, None),
        P(("sp", "dp"), None, None),
        P(("sp", "dp"), None, None),
    )
    out_specs = P("dp", "sp", None)
    return jax.shard_map(
        on_device, mesh=mesh, in_specs=in_specs, out_specs=out_specs, check_vma=False
    )
```

```python
from functools import partial

import jax
import jax.numpy as jnp
from jax import lax
from jax.experimental import pallas as pl
from jax.experimental.pallas import tpu as pltpu
from jax.sharding import PartitionSpec as P

EPS = 1e-06
MESH = pl.DeviceIdType.MESH
GATE_ROWS = 16
PARTS = 4
SUBS = 2
FF_TILE = 256
PIECES = 8
EXTRA = 1


def log_sigmoid(x):
    return jnp.minimum(x, 0.0) - jnp.log1p(jnp.exp(-jnp.abs(x)))


def layer_kernel(*refs, n, dpn, inputs):
    hbm, (out_ref,), rest = refs[:inputs], refs[inputs : inputs + 1], refs[inputs + 1 :]
    local, rest = rest[:inputs], rest[inputs:]
    (
        q_ref, k_ref, v_ref, g_ref, offset_ref, extra_ref, amp_ref, logits_ref, w_ref,
        res_ref, cell_gain_ref, expert_gain_ref, index_ref, group_ref, within_ref,
        gate_ref, up_ref, down_ref,
    ) = local
    (
        send, recv, gates_t, params, rows_of_gate, cols, weights, sums, state_out, state_in,
        mixed, mrecv, wfull, proj,
        meta, table_t, table_hi, table_lo, line, outgoing, incoming, hs, produced, returned,
        partial_out, partial_in, total, partial,
        in_sem, send_sem, recv_sem, param_send, param_recv, state_send, state_recv, msend_sem, mrecv_sem, wx_send, wx_recv, wy_send, wc_send,
        wc_recv, wl_sem, meta_send, meta_recv, up_send, down_send, line_recv,
        out_send, out_recv, back_send, back_recv, part_send, part_recv,
    ) = rest
    loads = [pltpu.make_async_copy(hbm[i], local[i], in_sem.at[i]) for i in range(inputs)]
    early = (0, 1, 2, 3, 4, 5, 6, 8)
    for i in early:
        loads[i].start()
    tok = q_ref.shape[1]
    dk = q_ref.shape[2] // n
    dv = v_ref.shape[2] // n
    half = n // 2
    length = half * tok
    wcol = w_ref.shape[1]
    me = lax.axis_index("sp")
    my_half, my_rank = me // half, me % half
    first = my_half * half
    opposite = (me + half) % n
    my_dp = lax.axis_index("dp")
    my_x, my_core = my_dp // 2, my_dp % 2
    chips = dpn // 2

    barrier = pltpu.get_barrier_semaphore()

    devices = n * dpn
    cap = 4 * tok // devices
    ny = chips if n % chips == 0 else 1
    nz = n // ny
    plane = ny * dpn
    my_z, my_y = me // ny, me % ny
    my_q = my_y * dpn + my_dp

    def device(z, q):
        return {"sp": z * ny + q // dpn, "dp": q % dpn}

    def greet_sp(o, _):
        pl.semaphore_signal(
            barrier, inc=1, device_id={"sp": (me + o) % n, "dp": my_dp}, device_id_type=MESH
        )
        return 0

    def greet_plane(o, _):
        pl.semaphore_signal(
            barrier, inc=1, device_id=device(my_z, (my_q + o) % plane), device_id_type=MESH
        )
        return 0

    lax.fori_loop(1, n, greet_sp, 0)
    lax.fori_loop(1, plane, greet_plane, 0)
    for load in loads[:4]:
        load.wait()

    for h in range(n):
        send[h, 0:tok, 0:dk] = k_ref[0, :, h * dk : (h + 1) * dk]
        send[h, 0:tok, dk : 2 * dk] = q_ref[0, :, h * dk : (h + 1) * dk]
        send[h, 0:tok, 2 * dk : 2 * dk + dv] = v_ref[0, :, h * dv : (h + 1) * dv]
    gate_rows = g_ref.shape[1]
    gates_t[0:gate_rows] = g_ref[0].astype(jnp.float32)
    gates_t[gate_rows:] = jnp.zeros((128 - gate_rows, tok), jnp.float32)
    for h in range(n):
        send[h, tok : tok + GATE_ROWS, 0:tok] = gates_t[4 * h : 4 * h + GATE_ROWS, :].astype(
            jnp.bfloat16
        )
        send[h, tok : tok + GATE_ROWS, tok:] = jnp.zeros(
            (GATE_ROWS, send.shape[2] - tok), jnp.bfloat16
        )

    for i in (4, 5, 6):
        loads[i].wait()
    for d in range(n):
        params[my_half, d : d + 1, 0:tok] = extra_ref[0, :, d * tok : (d + 1) * tok]
    params[my_half, n : n + 1, 0:dv] = amp_ref[...]
    lane_p = lax.broadcasted_iota(jnp.int32, (1, params.shape[2]), 1)
    params[my_half, n + 1 : n + 2] = jnp.where(
        lane_p == 0, offset_ref[0:1, 0:1], offset_ref[0:1, 1:2]
    )

    pl.semaphore_wait(barrier, n - 1 + plane - 1)
    for i in range(inputs):
        if i not in early:
            loads[i].start()

    def all_of(ref, send_sem, recv_sem):
        return pltpu.make_async_remote_copy(
            src_ref=ref,
            dst_ref=ref,
            send_sem=send_sem,
            recv_sem=recv_sem,
            device_id={"sp": opposite, "dp": my_dp},
            device_id_type=MESH,
        )

    def qkv_copy(o, j):
        return pltpu.make_async_remote_copy(
            src_ref=send.at[(my_rank + o) % half + j * half],
            dst_ref=recv.at[j, my_rank],
            send_sem=send_sem,
            recv_sem=recv_sem,
            device_id={"sp": first + (my_rank + o) % half, "dp": my_dp},
            device_id_type=MESH,
        )

    def qkv_all():
        return all_of(send.at[pl.ds(0, 2 * (half - 1))], send_sem, recv_sem)

    def param_copy(slot):
        return pltpu.make_async_remote_copy(
            src_ref=params.at[my_half],
            dst_ref=params.at[slot],
            send_sem=param_send,
            recv_sem=param_recv,
            device_id={"sp": opposite, "dp": my_dp},
            device_id_type=MESH,
        )

    def state_copy():
        return pltpu.make_async_remote_copy(
            src_ref=state_out,
            dst_ref=state_in,
            send_sem=state_send,
            recv_sem=state_recv,
            device_id={"sp": opposite, "dp": my_dp},
            device_id_type=MESH,
        )

    piece = w_ref.shape[0] // PIECES

    share = PIECES // ny
    first_piece = my_y * share

    def rows_of(p):
        return pl.ds(pl.multiple_of(p * piece, piece), piece)

    def wx_copy(o, p):
        return pltpu.make_async_remote_copy(
            src_ref=w_ref.at[rows_of(p)],
            dst_ref=wfull.at[my_dp, rows_of(p)],
            send_sem=wx_send.at[o - 1],
            recv_sem=wx_recv.at[o - 1, p],
            device_id={"sp": me, "dp": ((my_x + o) % chips) * 2 + my_core},
            device_id_type=MESH,
        )

    def from_chip(o):
        return ((my_x + chips - o) % chips) * 2 + my_core

    def wy_copy(o, p, yo):
        return pltpu.make_async_remote_copy(
            src_ref=wfull.at[from_chip(o), rows_of(p)],
            dst_ref=wfull.at[from_chip(o), rows_of(p)],
            send_sem=wy_send.at[o - 1, yo - 1],
            recv_sem=wx_recv.at[o - 1, p],
            device_id={"sp": my_z * ny + (my_y + yo) % ny, "dp": my_dp},
            device_id_type=MESH,
        )

    def wc_copy(o, p):
        return pltpu.make_async_remote_copy(
            src_ref=wfull.at[from_chip(o), rows_of(p)],
            dst_ref=wfull.at[from_chip(o), rows_of(p)],
            send_sem=wc_send.at[o],
            recv_sem=wc_recv.at[o],
            device_id={"sp": me, "dp": my_x * 2 + 1 - my_core},
            device_id_type=MESH,
        )

    def own_copy():
        return pltpu.make_async_remote_copy(
            src_ref=w_ref,
            dst_ref=wfull.at[my_dp],
            send_sem=wc_send.at[0],
            recv_sem=wc_recv.at[0],
            device_id={"sp": me, "dp": my_x * 2 + 1 - my_core},
            device_id_type=MESH,
        )

    own_parts = list(range(share))
    extra_parts = list(range(2 * share - EXTRA, 2 * share)) if ny > 1 else []
    other_parts = [i for i in range(share, PIECES) if i not in extra_parts]
    sent_parts = own_parts + extra_parts
    turns = own_parts[:-1] + other_parts[:1] + own_parts[-1:] + other_parts[1:] + extra_parts

    def onward(i, yo):
        return i < share and (i < share - EXTRA or yo < ny - 1)

    def pass_on(turn):
        j = turns[turn]
        p = (first_piece + j) % PIECES
        for o in range(1, chips):
            wx_copy(o, p).wait_recv()
            wc_copy(o, p).start()
            for yo in range(1, ny):
                if onward(j, yo):
                    wy_copy(o, p, yo).start()

    param_copy(my_half).start()
    for o in range(1, half):
        for j in range(2):
            qkv_copy(o, j).start()
    loads[8].wait()
    for j in sent_parts:
        for o in range(1, chips):
            wx_copy(o, (first_piece + j) % PIECES).start()
    own_copy().start()
    own_w = pltpu.make_async_copy(w_ref, wfull.at[my_dp], wl_sem)
    own_w.start()
    for j in range(2):
        recv[j, my_rank] = send[my_rank + j * half]
    for i in (7, 9, 10, 11, 12, 13, 14):
        loads[i].wait()

    rows_in = plane * cap
    ids = index_ref[0].astype(jnp.float32)
    e_0, e_1 = ids[0:1], ids[1:2]
    wide = -(-devices // 128) * 128
    sub_e = lax.broadcasted_iota(jnp.int32, (wide, tok), 0).astype(jnp.float32)
    hit_0 = jnp.where(sub_e == e_0, 1.0, 0.0)
    hit_1 = jnp.where(sub_e == e_1, 1.0, 0.0)
    tri = jnp.where(
        lax.broadcasted_iota(jnp.int32, (tok, tok), 0)
        < lax.broadcasted_iota(jnp.int32, (tok, tok), 1),
        1.0,
        0.0,
    ).astype(jnp.bfloat16)
    rank_0 = jnp.dot(hit_0.astype(jnp.bfloat16), tri, preferred_element_type=jnp.float32)
    rank_1 = jnp.dot(hit_1.astype(jnp.bfloat16), tri, preferred_element_type=jnp.float32)
    rank_1 = rank_1 + jnp.sum(hit_0, axis=1, keepdims=True)
    place_0 = e_0 * cap + jnp.sum(hit_0 * rank_0, axis=0, keepdims=True)
    place_1 = e_1 * cap + jnp.sum(hit_1 * rank_1, axis=0, keepdims=True)
    groups = group_ref.shape[1]
    span = devices // groups
    route_0 = jnp.zeros((1, tok), jnp.float32)
    route_1 = jnp.zeros((1, tok), jnp.float32)
    for c in range(groups):
        weight_c = group_ref[0, c : c + 1, :]
        route_0 += jnp.where((e_0 >= c * span) & (e_0 < (c + 1) * span), weight_c, 0.0)
        route_1 += jnp.where((e_1 >= c * span) & (e_1 < (c + 1) * span), weight_c, 0.0)
    route_0 = route_0 * within_ref[0, 0:1, :]
    route_1 = route_1 * within_ref[0, 1:2, :]
    sub_m = lax.broadcasted_iota(jnp.int32, (8, tok), 0)
    meta[my_z] = jnp.where(
        sub_m == 0,
        place_0,
        jnp.where(sub_m == 1, place_1, jnp.where(sub_m == 2, route_0, route_1)),
    )

    def meta_copy(z, slot):
        return pltpu.make_async_remote_copy(
            src_ref=meta.at[my_z],
            dst_ref=meta.at[slot],
            send_sem=meta_send,
            recv_sem=meta_recv,
            device_id=device(z, my_q),
            device_id_type=MESH,
        )

    for o in range(1, nz):
        meta_copy((my_z + o) % nz, my_z).start()

    stops = [PIECES * i // 8 for i in (2, 2, 4, 6, 8)]

    def pass_until(i):
        for j in range(stops[i - 1] if i else 0, stops[i]):
            pass_on(j)

    pass_until(0)
    if half > 1:
        qkv_all().wait_recv()
    param_copy(1 - my_half).wait_recv()

    upper = my_half == 1
    lane = lax.broadcasted_iota(jnp.int32, (8, length), 1)
    sub = lax.broadcasted_iota(jnp.int32, (8, length), 0)
    gates, f, b = [], [], []
    for j in range(2):
        gates.append(
            jnp.concatenate(
                [recv[j, d, tok : tok + GATE_ROWS, 0:tok].astype(jnp.float32) for d in range(half)],
                axis=1,
            )
        )
        extra = jnp.concatenate(
            [params[j, pl.ds(first + d, 1), 0:tok] for d in range(half)], axis=1
        )
        offset = params[j, n + 1 : n + 2]
        f.append(log_sigmoid(gates[j][1:2] + offset[:, 0:1]) + extra)
        b.append(log_sigmoid(gates[j][3:4] + offset[:, 1:2]) + extra)
    f = jnp.where(sub == 0, f[0], f[1])
    b = jnp.where(sub == 0, b[0], b[1])
    step = 1
    while step < length:
        f = f + jnp.where(lane >= step, pltpu.roll(f, step, 1), 0.0)
        b = b + jnp.where(lane < length - step, pltpu.roll(b, length - step, 1), 0.0)
        step *= 2
    wide_sub = lax.broadcasted_iota(jnp.int32, (128, length), 0)
    for j in range(2):
        row_i = gates[j][0:1]
        row_f = row_i - f[j : j + 1]
        row_b = gates[j][2:3] - b[j : j + 1]
        rows_of_gate[j] = jnp.where(sub == 0, row_f, row_b)
        leaving = jnp.exp(
            jnp.where(upper, row_b + b[j : j + 1, 0:1], row_f + f[j : j + 1, length - 1 : length])
        )
        stacked = jnp.where(wide_sub == 0, f[j : j + 1], jnp.where(wide_sub == 1, b[j : j + 1], row_i))
        cols[j] = jnp.where(wide_sub == 3, leaving, stacked).T

    scale = dk ** (-0.5)

    def state(j, _):
        kq = recv[j, :, 0:tok, 0 : 2 * dk].reshape(length, 2 * dk).astype(jnp.float32)
        kq = kq * cols[j][:, 3:4]
        memory = lax.dot_general(
            kq.astype(jnp.bfloat16),
            recv[j, :, 0:tok, 2 * dk : 2 * dk + dv].reshape(length, dv),
            (((0,), (0,)), ((), ())),
            preferred_element_type=jnp.float32,
        )
        normal = jnp.sum(kq, axis=0, keepdims=True)
        high = normal.astype(jnp.bfloat16).astype(jnp.float32)
        at = lax.broadcasted_iota(jnp.int32, (GATE_ROWS, 2 * dk), 0)
        state_out[j, 0:dk] = memory[0:dk].astype(jnp.bfloat16)
        state_out[j, dk:, 0 : 2 * dk] = jnp.where(
            at == 0, high, jnp.where(at == 1, normal - high, 0.0)
        ).astype(jnp.bfloat16)
        return 0

    lax.fori_loop(0, 2, state, 0)
    state_copy().start()
    pass_until(1)

    def mixed_copy(o, j, rank):
        return pltpu.make_async_remote_copy(
            src_ref=mixed.at[j, (my_rank + o) % half],
            dst_ref=mrecv.at[rank + j * half],
            send_sem=msend_sem,
            recv_sem=mrecv_sem,
            device_id={"sp": first + (my_rank + o) % half, "dp": my_dp},
            device_id_type=MESH,
        )

    def mixed_all():
        return all_of(mrecv.at[pl.ds(0, 2 * (half - 1))], msend_sem, mrecv_sem)

    def scaled(j, d):
        return recv[j, d, 0:tok, dk : 2 * dk].astype(jnp.float32) * scale

    def before_of(d):
        t_pos = d * tok + lax.broadcasted_iota(jnp.int32, (tok, length), 0)
        return lax.broadcasted_iota(jnp.int32, (tok, length), 1) < t_pos

    lane_z = lax.broadcasted_iota(jnp.int32, (tok, 128), 1)

    def weigh_head(d, k, j):
        m = 2 * k + j
        start = pl.multiple_of(d * tok, tok)
        qs = scaled(j, d)
        ks = recv[j, d, 0:tok, 0:dk].astype(jnp.float32)
        diag = jnp.sum(qs * ks, axis=1, keepdims=True)
        qs = jnp.concatenate([qs, jnp.zeros_like(qs)], axis=1).astype(jnp.bfloat16)
        kall = recv[j, :, 0:tok, 0 : 2 * dk].reshape(length, 2 * dk)
        scores = lax.dot_general(
            qs, kall, (((1,), (1,)), ((), ())), preferred_element_type=jnp.float32
        )
        col = cols[j, pl.ds(start, tok), :]
        col_f, col_b, col_i = col[:, 0:1], col[:, 1:2], col[:, 2:3]
        before = before_of(d)
        rows = rows_of_gate[j]
        weight = scores * jnp.exp(jnp.where(before, col_f + rows[0:1], col_b + rows[1:2]))
        weights[m] = weight
        diag = diag * jnp.exp(col_i)
        z_f = jnp.sum(jnp.where(before, weight, 0.0), axis=1, keepdims=True) + diag
        z_b = jnp.sum(jnp.where(before, 0.0, weight), axis=1, keepdims=True)
        sums[m] = jnp.where(lane_z == 0, z_f, jnp.where(lane_z == 1, z_b, diag))
    def weigh(k, _):
        for j in range(2):
            weigh_head((my_rank + 1 + k) % half, k, j)
        return 0

    lax.fori_loop(0, half, weigh, 0)
    pass_until(2)
    state_copy().wait_recv()

    def segment_head(d, k, j):
        m = 2 * k + j
        start = pl.multiple_of(d * tok, tok)
        col = cols[j, pl.ds(start, tok), :]
        carried = jnp.exp(jnp.where(upper, col[:, 0:1], col[:, 1:2]))
        qs = scaled(j, d) * carried
        normal = state_in[j, dk:, 0:dk].astype(jnp.float32)
        z_state = jnp.sum(qs * (normal[0:1] + normal[1:2]), axis=1, keepdims=True)
        z = sums[m]
        z_f, z_b, diag = z[:, 0:1], z[:, 1:2], z[:, 2:3]
        z_f = z_f + jnp.where(upper, z_state, 0.0)
        z_b = z_b + jnp.where(upper, 0.0, z_state)
        inv_f = 1.0 / jnp.maximum(jnp.abs(z_f), 1.0)
        inv_b = 1.0 / jnp.maximum(jnp.abs(z_b), 1.0)
        probs = (weights[m] * jnp.where(before_of(d), inv_f, inv_b)).astype(jnp.bfloat16)
        vall = recv[j, :, 0:tok, 2 * dk : 2 * dk + dv].reshape(length, dv)
        total = jnp.dot(probs, vall, preferred_element_type=jnp.float32)
        total = total + jnp.dot(
            (qs * jnp.where(upper, inv_f, inv_b)).astype(jnp.bfloat16),
            state_in[j, 0:dk],
            preferred_element_type=jnp.float32,
        )
        total = total + (diag * inv_f) * recv[j, d, 0:tok, 2 * dk : 2 * dk + dv].astype(jnp.float32)
        amp = params[j, n : n + 1, 0:dv]
        total = total * lax.rsqrt(jnp.mean(total * total, axis=1, keepdims=True) + EPS) * amp
        mixed[j, d] = total.astype(jnp.bfloat16)

    def segment(k, _):
        d = (my_rank + 1 + k) % half
        for j in range(2):
            segment_head(d, k, j)

        @pl.when(k < half - 1)
        def _():
            for j in range(2):
                mixed_copy(k + 1, j, my_rank).start()

        @pl.when(k == half - 2)
        def _():
            pass_until(3)

        return 0

    lax.fori_loop(0, half, segment, 0)
    pass_until(4)
    for j in range(2):
        mrecv[my_rank + j * half] = mixed[j, my_rank]
    sub_r = lax.broadcasted_iota(jnp.int32, (rows_in, tok), 0).astype(jnp.float32)
    at = sub_r + (my_z * rows_in).astype(jnp.float32)

    def tables(o, _):
        z = (my_z + o) % nz

        rows = meta[z]
        hit_0, hit_1 = at == rows[0:1], at == rows[1:2]
        table_t[z] = (jnp.where(hit_0, 1.0, 0.0) + jnp.where(hit_1, 1.0, 0.0)).astype(jnp.bfloat16)
        weighted = (jnp.where(hit_0, rows[2:3], 0.0) + jnp.where(hit_1, rows[3:4], 0.0)).T
        high = weighted.astype(jnp.bfloat16)
        table_hi[z] = high
        table_lo[z] = (weighted - high.astype(jnp.float32)).astype(jnp.bfloat16)
        return 0

    if nz > 1:
        all_of(meta.at[pl.ds(0, nz - 1)], meta_send, meta_recv).wait_recv()
    lax.fori_loop(0, nz, tables, 0)
    sig = jax.nn.sigmoid(logits_ref[0].astype(jnp.float32))
    if half > 1:
        mixed_all().wait_recv()
    gated = jnp.concatenate([mrecv[h].astype(jnp.float32) for h in range(n)], axis=1) * sig
    gated = gated.astype(jnp.bfloat16)
    own_w.wait()
    for o in range(chips):
        all_of(w_ref, wc_send.at[o], wc_recv.at[o]).wait_recv()
    for j in range(dpn):
        proj[:, j * wcol : (j + 1) * wcol] = jnp.dot(
            gated, wfull[j], preferred_element_type=jnp.float32
        )
    p = proj[...]
    stream = (
        res_ref[0].astype(jnp.float32)
        + cell_gain_ref[...] * p * lax.rsqrt(jnp.mean(p * p, axis=1, keepdims=True) + EPS)
    ).astype(jnp.bfloat16)
    s = stream.astype(jnp.float32)
    width = s.shape[1]
    part = width // PARTS
    moe = (
        expert_gain_ref[...] * s * lax.rsqrt(jnp.mean(s * s, axis=1, keepdims=True) + EPS)
    ).astype(jnp.bfloat16)

    def line_copy(z, p, to, sems):
        return pltpu.make_async_remote_copy(
            src_ref=line.at[z, p],
            dst_ref=line.at[z, p],
            send_sem=sems.at[z],
            recv_sem=line_recv.at[z, p],
            device_id=device(to, my_q),
            device_id_type=MESH,
        )

    above, below = (my_z + 1) % nz, (my_z + nz - 1) % nz
    has_above, has_below = my_z + 1 < nz, my_z > 0
    edge = (my_z == 0) | (my_z == nz - 1)

    inner_above = ~edge & (2 * my_z < nz - 1)
    inner_below = ~edge & (2 * my_z >= nz - 1)

    def spread(z, p, held=False):
        @pl.when((z <= my_z) & has_above & ~(inner_above & held))
        def _():
            line_copy(z, p, above, up_send).start()

        @pl.when((z >= my_z) & has_below & ~(inner_below & held))
        def _():
            line_copy(z, p, below, down_send).start()

    def release(p):
        @pl.when(inner_above)
        def _():
            line_copy(my_z, p, above, up_send).start()

        @pl.when(inner_below)
        def _():
            line_copy(my_z, p, below, down_send).start()

    for p in range(PARTS):
        line[my_z, p] = moe[:, p * part : (p + 1) * part]
        spread(my_z, p, nz == 4 and p >= PARTS // 2)
    for p in range(PARTS):
        total[p] = s[:, p * part : (p + 1) * part]
    for i in (15, 16, 17):
        loads[i].wait()
    ff = hs.shape[1]

    crossed = nz == 4

    def order_of(z):
        if crossed:
            return ((0, 1, 3, 2), (1, 0, 3, 2), (2, 3, 0, 1), (3, 2, 0, 1))[z]
        inner = 1 if 2 * z < nz - 1 else -1
        return sorted(range(nz), key=lambda s: (abs(s - z), -(s - z) * inner))

    def by_distance(k):
        found = my_z
        for z in range(nz):
            near = order_of(z)
            for place in range(nz):
                found = jnp.where((my_z == z) & (k == place), near[place], found)
        return found

    def plane_copy(src, dst, sems, z, p, q_to, q_src, q_dst):
        return pltpu.make_async_remote_copy(
            src_ref=src.at[z, p, q_src],
            dst_ref=dst.at[z, p, q_dst],
            send_sem=sems[0],
            recv_sem=sems[1].at[z, p],
            device_id=device(my_z, q_to),
            device_id_type=MESH,
        )

    def plane_send(src, dst, sems, z, p):
        def one(o, _):
            q = (my_q + o) % plane
            plane_copy(src, dst, sems, z, p, q, q, my_q).start()
            return 0

        lax.fori_loop(1, plane, one, 0)
        dst[z, p, my_q] = src[z, p, my_q]

    def plane_all(src, dst, sems, z, p):
        others = pl.ds(0, plane - 1)
        return pltpu.make_async_remote_copy(
            src_ref=src.at[z, p, others],
            dst_ref=dst.at[z, p, others],
            send_sem=sems[0],
            recv_sem=sems[1].at[z, p],
            device_id=device(my_z, (my_q + 1) % plane),
            device_id_type=MESH,
        )

    out_way = (outgoing, incoming, (out_send, out_recv))
    back_way = (produced, returned, (back_send, back_recv))

    def dispatch(k, first, last):
        z = by_distance(k)

        def piece(p, _):
            @pl.when(k > 0)
            def _():
                line_copy(z, p, above, up_send).wait_recv()
                spread(z, p)

            block = jnp.dot(table_t[z], line[z, p], preferred_element_type=jnp.float32)
            outgoing[z, p] = block.astype(jnp.bfloat16).reshape(plane, cap, part)
            plane_send(*out_way, z, p)
            return 0

        lax.fori_loop(first, last, piece, 0)

    def expert(k, inline):
        z = by_distance(k)

        def arrive(p, _):
            plane_all(*out_way, z, p).wait_recv()
            return 0

        split = max(PARTS // 2, 1)

        def sides(first, last, at):
            x = jnp.concatenate(
                [incoming[z, p].reshape(rows_in, part) for p in range(first, last)], axis=1
            )
            rows = slice(first * part, last * part)
            a = jnp.dot(x, gate_ref[0, rows, at], preferred_element_type=jnp.float32)
            u = jnp.dot(x, up_ref[0, rows, at], preferred_element_type=jnp.float32)
            return a, u

        def begin_tile(t, _):
            at = pl.ds(pl.multiple_of(t * FF_TILE, FF_TILE), FF_TILE)
            partial[0, :, at], partial[1, :, at] = sides(0, split, at)
            return 0

        def up_tile(t, _):
            at = pl.ds(pl.multiple_of(t * FF_TILE, FF_TILE), FF_TILE)
            a, u = sides(split, PARTS, at)
            a, u = a + partial[0, :, at], u + partial[1, :, at]
            hs[:, at] = (jax.nn.silu(a) * u).astype(jnp.bfloat16)
            return 0

        lax.fori_loop(0, split, arrive, 0)
        lax.fori_loop(0, ff // FF_TILE, begin_tile, 0)
        lax.fori_loop(split, PARTS, arrive, 0)
        lax.fori_loop(0, ff // FF_TILE, up_tile, 0)

        def down_tile(p, _):
            at = pl.ds(pl.multiple_of(p * part, part), part)
            y = jnp.dot(hs[...], down_ref[0, :, at], preferred_element_type=jnp.float32)
            produced[z, p] = y.astype(jnp.bfloat16).reshape(plane, cap, part)

            @pl.when(inline)
            def _():
                plane_send(*back_way, z, p)

            return 0

        lax.fori_loop(0, PARTS, down_tile, 0)

    def send_back(k):
        def piece(p, _):
            plane_send(*back_way, by_distance(k), p)
            return 0

        lax.fori_loop(0, PARTS, piece, 0)

    def partial_copy(z, f):
        to = jnp.where(z < my_z, below, above)
        slot = jnp.where((z > my_z) & (to == z), nz, z)
        return pltpu.make_async_remote_copy(
            src_ref=partial_out.at[z, f],
            dst_ref=partial_in.at[slot, f],
            send_sem=part_send,
            recv_sem=part_recv.at[slot, f],
            device_id=device(to, my_q),
            device_id_type=MESH,
        )

    def partial_arrive(slot, f):
        pltpu.make_async_remote_copy(
            src_ref=partial_out.at[0, f],
            dst_ref=partial_in.at[slot, f],
            send_sem=part_send,
            recv_sem=part_recv.at[slot, f],
            device_id=device(above, my_q),
            device_id_type=MESH,
        ).wait_recv()

    fine = part // SUBS

    def combine(z, p):
        plane_all(*back_way, z, p).wait_recv()
        block = returned[z, p].reshape(rows_in, part)
        mine = jnp.dot(table_hi[z], block, preferred_element_type=jnp.float32) + jnp.dot(
            table_lo[z], block, preferred_element_type=jnp.float32
        )

        @pl.when(z == my_z)
        def _():
            total[p] += mine

        @pl.when((z != my_z) & edge)
        def _():
            for i in range(SUBS):
                f = p * SUBS + i
                partial_out[z, f] = mine[:, i * fine : (i + 1) * fine].astype(jnp.bfloat16)
                partial_copy(z, f).start()

        @pl.when((z != my_z) & ~edge)
        def _():
            total[PARTS] = mine
            for i in range(SUBS):
                f = p * SUBS + i
                partial_arrive(z, f)
                partial_out[z, f] = (
                    total[PARTS, :, i * fine : (i + 1) * fine]
                    + partial_in[z, f].astype(jnp.float32)
                ).astype(jnp.bfloat16)
                partial_copy(z, f).start()

    def combine_all(k):
        def one(p, _):
            combine(by_distance(k), p)
            return 0

        lax.fori_loop(0, PARTS, one, 0)

    dispatch(0, 0, PARTS)
    midway = PARTS // 2

    def tick(k, _):
        last = k == nz - 1
        stop = jnp.where(last, 0, PARTS)
        early = jnp.minimum(jnp.where(k == 0, midway, jnp.where(edge, jnp.where(k == 1, midway // 2, midway), PARTS)), stop)
        dispatch(k + 1, 0, early)

        @pl.when(~edge & (k == nz - 2))
        def _():
            send_back(1)

        if crossed:
            @pl.when(~edge & last)
            def _():
                send_back(2)

        expert(k, edge & (k > 0))
        dispatch(k + 1, early, stop)
        if crossed:
            @pl.when(k == 0)
            def _():
                for p in range(midway, PARTS):
                    release(p)

        @pl.when(edge & (k > 0))
        def _():
            combine_all(k)

        return 0

    lax.fori_loop(0, nz, tick, 0)

    @pl.when(edge)
    def _():
        send_back(0)

    @pl.when(~edge)
    def _():
        for k in range(nz - 1, 2 if crossed else 1, -1):
            send_back(k)
        send_back(0)
        if nz > 2 and not crossed:
            combine_all(1)
        chained = (2, 1) if crossed else tuple(range(nz - 1, 1, -1))

        def one(s, _):
            for behind, k in enumerate(chained):
                p = s - behind

                @pl.when((p >= 0) & (p < PARTS))
                def _():
                    combine(by_distance(k), p)

            return 0

        lax.fori_loop(0, PARTS + max(len(chained) - 1, 0), one, 0)
        if crossed:
            combine_all(3)

    combine_all(0)
    for f in range(PARTS * SUBS):
        p, at = f // SUBS, pl.ds(f % SUBS * fine, fine)

        @pl.when(has_above)
        def _():
            partial_arrive(my_z, f)
            total[p, :, at] += partial_in[my_z, f].astype(jnp.float32)

        @pl.when(has_below)
        def _():
            partial_arrive(nz, f)
            total[p, :, at] += partial_in[nz, f].astype(jnp.float32)

        out_ref[0, :, f * fine : (f + 1) * fine] = total[p, :, at].astype(jnp.bfloat16)

    def drain(z, _):
        @pl.when((z <= my_z) & has_above)
        def _():
            all_of(line.at[z], up_send.at[z], meta_recv).wait_send()

        @pl.when((z >= my_z) & has_below)
        def _():
            all_of(line.at[z], down_send.at[z], meta_recv).wait_send()

        return 0

    lax.fori_loop(0, nz, drain, 0)
    if nz > 1:
        all_of(meta.at[pl.ds(0, nz - 1)], meta_send, meta_recv).wait_send()
        all_of(partial_out.at[pl.ds(0, nz - 1)], part_send, meta_recv).wait_send()
    others = pl.ds(0, plane - 1)
    all_of(outgoing.at[:, :, others], out_send, meta_recv).wait_send()
    all_of(produced.at[:, :, others], back_send, meta_recv).wait_send()
    if half > 1:
        qkv_all().wait_send()
        mixed_all().wait_send()
    param_copy(my_half).wait_send()
    state_copy().wait_send()
    for o in range(chips):
        all_of(w_ref, wc_send.at[o], wc_recv.at[o]).wait_send()
    for o in range(1, chips):
        held = w_ref.at[pl.ds(0, len(sent_parts) * piece)]
        all_of(held, wx_send.at[o - 1], wc_recv.at[0]).wait_send()
        for yo in range(1, ny):
            held = w_ref.at[pl.ds(0, sum(onward(j, yo) for j in range(share)) * piece)]
            all_of(held, wy_send.at[o - 1, yo - 1], wc_recv.at[0]).wait_send()


def on_device(
    residual_input,
    queries,
    keys,
    values,
    gate_logits,
    retention_offset,
    log_forget_extra,
    lane_amplifier,
    output_gate_logits,
    output_projection,
    cell_norm_gain,
    expert_norm_gain,
    expert_index,
    group_mixing_weight,
    within_group_weight,
    gate_weight,
    up_weight,
    down_weight,
):
    n, dpn = lax.axis_size("sp"), lax.axis_size("dp")
    tok, width = residual_input.shape[1:]
    dk, dv = queries.shape[2] // n, values.shape[2] // n
    half = n // 2
    length, devices, ff = half * tok, n * dpn, gate_weight.shape[2]
    cap, chips = 4 * tok // devices, dpn // 2
    ny = chips if n % chips == 0 else 1
    nz, plane = n // ny, ny * dpn
    rows_in, part = plane * cap, width // PARTS
    operands = (
        queries, keys, values, jnp.swapaxes(gate_logits, 1, 2), retention_offset, log_forget_extra,
        lane_amplifier.reshape(1, dv), output_gate_logits, output_projection,
        residual_input, cell_norm_gain.reshape(1, width), expert_norm_gain.reshape(1, width),
        jnp.swapaxes(expert_index, 1, 2), jnp.swapaxes(group_mixing_weight, 1, 2),
        jnp.swapaxes(within_group_weight, 1, 2),
        gate_weight, up_weight, down_weight,
    )
    dma = pltpu.SemaphoreType.DMA
    bf16, f32 = jnp.bfloat16, jnp.float32
    hbm = pl.BlockSpec(memory_space=pltpu.HBM)
    return pl.pallas_call(
        partial(layer_kernel, n=n, dpn=dpn, inputs=len(operands)),
        out_shape=pltpu.VMEM((1, tok, width), bf16),
        in_specs=[hbm] * len(operands),
        out_specs=pl.BlockSpec(memory_space=pltpu.VMEM),
        scratch_shapes=[pltpu.VMEM(x.shape, x.dtype) for x in operands]
        + [
            pltpu.VMEM((n, tok + GATE_ROWS, 2 * dk + dv), bf16),
            pltpu.VMEM((2, half, tok + GATE_ROWS, 2 * dk + dv), bf16),
            pltpu.VMEM((128, tok), f32),
            pltpu.VMEM((2, -(-(n + 2) // 8) * 8, max(tok, dv)), f32),
            pltpu.VMEM((2, 8, length), f32),
            pltpu.VMEM((2, length, 128), f32),
            pltpu.VMEM((n, tok, length), f32),
            pltpu.VMEM((n, tok, 128), f32),
            pltpu.VMEM((2, dk + GATE_ROWS, dv), bf16),
            pltpu.VMEM((2, dk + GATE_ROWS, dv), bf16),
            pltpu.VMEM((2, half, tok, dv), bf16),
            pltpu.VMEM((n, tok, dv), bf16),
            pltpu.VMEM((dpn,) + output_projection.shape, bf16),
            pltpu.VMEM((tok, width), f32),
            pltpu.VMEM((nz, 8, tok), f32),
            pltpu.VMEM((nz, rows_in, tok), bf16),
            pltpu.VMEM((nz, tok, rows_in), bf16),
            pltpu.VMEM((nz, tok, rows_in), bf16),
            pltpu.VMEM((nz, PARTS, tok, part), bf16),
            pltpu.VMEM((nz, PARTS, plane, cap, part), bf16),
            pltpu.VMEM((nz, PARTS, plane, cap, part), bf16),
            pltpu.VMEM((rows_in, ff), bf16),
            pltpu.VMEM((nz, PARTS, plane, cap, part), bf16),
            pltpu.VMEM((nz, PARTS, plane, cap, part), bf16),
            pltpu.VMEM((nz, PARTS * SUBS, tok, part // SUBS), bf16),
            pltpu.VMEM((nz + 1, PARTS * SUBS, tok, part // SUBS), bf16),
            pltpu.VMEM((PARTS + 1, tok, part), f32),
            pltpu.VMEM((2, rows_in, ff), f32),
            dma((len(operands),)),
            dma(()), dma(()), dma(()), dma(()), dma(()), dma(()), dma(()), dma(()),
            dma((max(chips - 1, 1),)), dma((max(chips - 1, 1), PIECES)),
            dma((max(chips - 1, 1), max(ny - 1, 1))), dma((chips,)), dma((chips,)),
            dma(()), dma(()), dma(()),
            dma((nz,)), dma((nz,)), dma((nz, PARTS)),
            dma(()), dma((nz, PARTS)), dma(()), dma((nz, PARTS)),
            dma(()), dma((nz + 1, PARTS * SUBS)),
        ],
        compiler_params=pltpu.CompilerParams(
            collective_id=0, has_side_effects=True, vmem_limit_bytes=60 * 1024 * 1024
        ),
    )(*operands)


def solution(mesh):
    in_specs = (
        P("dp", "sp", None),
        P("dp", "sp", None),
        P("dp", "sp", None),
        P("dp", "sp", None),
        P("dp", "sp", None),
        P("sp", None),
        P("dp", "sp", None),
        P("sp"),
        P("dp", "sp", None),
        P(None, "dp"),
        P(),
        P(),
        P("dp", "sp", None),
        P("dp", "sp", None),
        P("dp", "sp", None),
        P(("sp", "dp"), None, None),
        P(("sp", "dp"), None, None),
        P(("sp", "dp"), None, None),
    )
    out_specs = P("dp", "sp", None)
    return jax.shard_map(
        on_device, mesh=mesh, in_specs=in_specs, out_specs=out_specs, check_vma=False
    )
```

```python
from functools import partial

import jax
import jax.numpy as jnp
from jax import lax
from jax.experimental import pallas as pl
from jax.experimental.pallas import tpu as pltpu
from jax.sharding import PartitionSpec as P

EPS = 1e-06
MESH = pl.DeviceIdType.MESH
GATE_ROWS = 16
PARTS = 4
SUBS = 2
FF_TILE = 1024
PIECES = 8
EXTRA = 2


def log_sigmoid(x):
    return jnp.minimum(x, 0.0) - jnp.log1p(jnp.exp(-jnp.abs(x)))


def layer_kernel(*refs, n, dpn, inputs):
    hbm, (out_ref,), rest = refs[:inputs], refs[inputs : inputs + 1], refs[inputs + 1 :]
    local, rest = rest[:inputs], rest[inputs:]
    (
        q_ref, k_ref, v_ref, g_ref, offset_ref, extra_ref, amp_ref, logits_ref, w_ref,
        res_ref, cell_gain_ref, expert_gain_ref, index_ref, group_ref, within_ref,
        gate_ref, up_ref, down_ref,
    ) = local
    (
        send, recv, gates_t, params, rows_of_gate, cols, weights, sums, state_out, state_in,
        mixed, mrecv, wfull, proj,
        meta, table_t, table_hi, table_lo, line, outgoing, incoming, hs, produced, returned,
        partial_out, partial_in, total, partial,
        in_sem, send_sem, recv_sem, param_send, param_recv, state_send, state_recv, msend_sem, mrecv_sem, wx_send, wx_recv, wy_send, wc_send,
        wc_recv, wl_sem, meta_send, meta_recv, up_send, down_send, line_recv,
        out_send, out_recv, back_send, back_recv, part_send, part_recv,
    ) = rest
    loads = [pltpu.make_async_copy(hbm[i], local[i], in_sem.at[i]) for i in range(inputs)]
    early = (0, 1, 2, 3, 4, 5, 6, 8)
    for i in early:
        loads[i].start()
    tok = q_ref.shape[1]
    dk = q_ref.shape[2] // n
    dv = v_ref.shape[2] // n
    half = n // 2
    length = half * tok
    wcol = w_ref.shape[1]
    me = lax.axis_index("sp")
    my_half, my_rank = me // half, me % half
    first = my_half * half
    opposite = (me + half) % n
    my_dp = lax.axis_index("dp")
    my_x, my_core = my_dp // 2, my_dp % 2
    chips = dpn // 2

    barrier = pltpu.get_barrier_semaphore()

    devices = n * dpn
    cap = 4 * tok // devices
    ny = chips if n % chips == 0 else 1
    nz = n // ny
    plane = ny * dpn
    my_z, my_y = me // ny, me % ny
    my_q = my_y * dpn + my_dp

    def device(z, q):
        return {"sp": z * ny + q // dpn, "dp": q % dpn}

    def greet_sp(o, _):
        pl.semaphore_signal(
            barrier, inc=1, device_id={"sp": (me + o) % n, "dp": my_dp}, device_id_type=MESH
        )
        return 0

    def greet_plane(o, _):
        pl.semaphore_signal(
            barrier, inc=1, device_id=device(my_z, (my_q + o) % plane), device_id_type=MESH
        )
        return 0

    lax.fori_loop(1, n, greet_sp, 0)
    lax.fori_loop(1, plane, greet_plane, 0)
    for load in loads[:4]:
        load.wait()

    for h in range(n):
        send[h, 0:tok, 0:dk] = k_ref[0, :, h * dk : (h + 1) * dk]
        send[h, 0:tok, dk : 2 * dk] = q_ref[0, :, h * dk : (h + 1) * dk]
        send[h, 0:tok, 2 * dk : 2 * dk + dv] = v_ref[0, :, h * dv : (h + 1) * dv]
    gate_rows = g_ref.shape[1]
    gates_t[0:gate_rows] = g_ref[0].astype(jnp.float32)
    gates_t[gate_rows:] = jnp.zeros((128 - gate_rows, tok), jnp.float32)
    for h in range(n):
        send[h, tok : tok + GATE_ROWS, 0:tok] = gates_t[4 * h : 4 * h + GATE_ROWS, :].astype(
            jnp.bfloat16
        )
        send[h, tok : tok + GATE_ROWS, tok:] = jnp.zeros(
            (GATE_ROWS, send.shape[2] - tok), jnp.bfloat16
        )

    for i in (4, 5, 6):
        loads[i].wait()
    for d in range(n):
        params[my_half, d : d + 1, 0:tok] = extra_ref[0, :, d * tok : (d + 1) * tok]
    params[my_half, n : n + 1, 0:dv] = amp_ref[...]
    lane_p = lax.broadcasted_iota(jnp.int32, (1, params.shape[2]), 1)
    params[my_half, n + 1 : n + 2] = jnp.where(
        lane_p == 0, offset_ref[0:1, 0:1], offset_ref[0:1, 1:2]
    )

    pl.semaphore_wait(barrier, n - 1 + plane - 1)
    for i in range(inputs):
        if i not in early:
            loads[i].start()

    def all_of(ref, send_sem, recv_sem):
        return pltpu.make_async_remote_copy(
            src_ref=ref,
            dst_ref=ref,
            send_sem=send_sem,
            recv_sem=recv_sem,
            device_id={"sp": opposite, "dp": my_dp},
            device_id_type=MESH,
        )

    def qkv_copy(o, j):
        return pltpu.make_async_remote_copy(
            src_ref=send.at[(my_rank + o) % half + j * half],
            dst_ref=recv.at[j, my_rank],
            send_sem=send_sem,
            recv_sem=recv_sem,
            device_id={"sp": first + (my_rank + o) % half, "dp": my_dp},
            device_id_type=MESH,
        )

    def qkv_all():
        return all_of(send.at[pl.ds(0, 2 * (half - 1))], send_sem, recv_sem)

    def param_copy(slot):
        return pltpu.make_async_remote_copy(
            src_ref=params.at[my_half],
            dst_ref=params.at[slot],
            send_sem=param_send,
            recv_sem=param_recv,
            device_id={"sp": opposite, "dp": my_dp},
            device_id_type=MESH,
        )

    def state_copy():
        return pltpu.make_async_remote_copy(
            src_ref=state_out,
            dst_ref=state_in,
            send_sem=state_send,
            recv_sem=state_recv,
            device_id={"sp": opposite, "dp": my_dp},
            device_id_type=MESH,
        )

    piece = w_ref.shape[0] // PIECES

    share = PIECES // ny
    first_piece = my_y * share

    def rows_of(p):
        return pl.ds(pl.multiple_of(p * piece, piece), piece)

    def wx_copy(o, p):
        return pltpu.make_async_remote_copy(
            src_ref=w_ref.at[rows_of(p)],
            dst_ref=wfull.at[my_dp, rows_of(p)],
            send_sem=wx_send.at[o - 1],
            recv_sem=wx_recv.at[o - 1, p],
            device_id={"sp": me, "dp": ((my_x + o) % chips) * 2 + my_core},
            device_id_type=MESH,
        )

    def from_chip(o):
        return ((my_x + chips - o) % chips) * 2 + my_core

    def wy_copy(o, p, yo):
        return pltpu.make_async_remote_copy(
            src_ref=wfull.at[from_chip(o), rows_of(p)],
            dst_ref=wfull.at[from_chip(o), rows_of(p)],
            send_sem=wy_send.at[o - 1, yo - 1],
            recv_sem=wx_recv.at[o - 1, p],
            device_id={"sp": my_z * ny + (my_y + yo) % ny, "dp": my_dp},
            device_id_type=MESH,
        )

    def wc_copy(o, p):
        return pltpu.make_async_remote_copy(
            src_ref=wfull.at[from_chip(o), rows_of(p)],
            dst_ref=wfull.at[from_chip(o), rows_of(p)],
            send_sem=wc_send.at[o],
            recv_sem=wc_recv.at[o],
            device_id={"sp": me, "dp": my_x * 2 + 1 - my_core},
            device_id_type=MESH,
        )

    def own_copy():
        return pltpu.make_async_remote_copy(
            src_ref=w_ref,
            dst_ref=wfull.at[my_dp],
            send_sem=wc_send.at[0],
            recv_sem=wc_recv.at[0],
            device_id={"sp": me, "dp": my_x * 2 + 1 - my_core},
            device_id_type=MESH,
        )

    own_parts = list(range(share))
    extra_parts = list(range(2 * share - EXTRA, 2 * share)) if ny > 1 else []
    other_parts = [i for i in range(share, PIECES) if i not in extra_parts]
    sent_parts = own_parts + extra_parts
    turns = own_parts[:-1] + other_parts[:1] + own_parts[-1:] + other_parts[1:] + extra_parts

    def onward(i, yo):
        return i < share and (i < share - EXTRA or yo < ny - 1)

    def pass_on(turn):
        j = turns[turn]
        p = (first_piece + j) % PIECES
        for o in range(1, chips):
            wx_copy(o, p).wait_recv()
            wc_copy(o, p).start()
            for yo in range(1, ny):
                if onward(j, yo):
                    wy_copy(o, p, yo).start()

    param_copy(my_half).start()
    for o in range(1, half):
        for j in range(2):
            qkv_copy(o, j).start()
    loads[8].wait()
    for j in sent_parts:
        for o in range(1, chips):
            wx_copy(o, (first_piece + j) % PIECES).start()
    own_copy().start()
    own_w = pltpu.make_async_copy(w_ref, wfull.at[my_dp], wl_sem)
    own_w.start()
    for j in range(2):
        recv[j, my_rank] = send[my_rank + j * half]
    for i in (7, 9, 10, 11, 12, 13, 14):
        loads[i].wait()

    rows_in = plane * cap
    ids = index_ref[0].astype(jnp.float32)
    e_0, e_1 = ids[0:1], ids[1:2]
    wide = -(-devices // 128) * 128
    sub_e = lax.broadcasted_iota(jnp.int32, (wide, tok), 0).astype(jnp.float32)
    hit_0 = jnp.where(sub_e == e_0, 1.0, 0.0)
    hit_1 = jnp.where(sub_e == e_1, 1.0, 0.0)
    tri = jnp.where(
        lax.broadcasted_iota(jnp.int32, (tok, tok), 0)
        < lax.broadcasted_iota(jnp.int32, (tok, tok), 1),
        1.0,
        0.0,
    ).astype(jnp.bfloat16)
    rank_0 = jnp.dot(hit_0.astype(jnp.bfloat16), tri, preferred_element_type=jnp.float32)
    rank_1 = jnp.dot(hit_1.astype(jnp.bfloat16), tri, preferred_element_type=jnp.float32)
    rank_1 = rank_1 + jnp.sum(hit_0, axis=1, keepdims=True)
    place_0 = e_0 * cap + jnp.sum(hit_0 * rank_0, axis=0, keepdims=True)
    place_1 = e_1 * cap + jnp.sum(hit_1 * rank_1, axis=0, keepdims=True)
    groups = group_ref.shape[1]
    span = devices // groups
    route_0 = jnp.zeros((1, tok), jnp.float32)
    route_1 = jnp.zeros((1, tok), jnp.float32)
    for c in range(groups):
        weight_c = group_ref[0, c : c + 1, :]
        route_0 += jnp.where((e_0 >= c * span) & (e_0 < (c + 1) * span), weight_c, 0.0)
        route_1 += jnp.where((e_1 >= c * span) & (e_1 < (c + 1) * span), weight_c, 0.0)
    route_0 = route_0 * within_ref[0, 0:1, :]
    route_1 = route_1 * within_ref[0, 1:2, :]
    sub_m = lax.broadcasted_iota(jnp.int32, (8, tok), 0)
    meta[my_z] = jnp.where(
        sub_m == 0,
        place_0,
        jnp.where(sub_m == 1, place_1, jnp.where(sub_m == 2, route_0, route_1)),
    )

    def meta_copy(z, slot):
        return pltpu.make_async_remote_copy(
            src_ref=meta.at[my_z],
            dst_ref=meta.at[slot],
            send_sem=meta_send,
            recv_sem=meta_recv,
            device_id=device(z, my_q),
            device_id_type=MESH,
        )

    for o in range(1, nz):
        meta_copy((my_z + o) % nz, my_z).start()

    stops = [PIECES * i // 8 for i in (2, 2, 4, 6, 8)]

    def pass_until(i):
        for j in range(stops[i - 1] if i else 0, stops[i]):
            pass_on(j)

    pass_until(0)
    if half > 1:
        qkv_all().wait_recv()
    param_copy(1 - my_half).wait_recv()

    upper = my_half == 1
    lane = lax.broadcasted_iota(jnp.int32, (8, length), 1)
    sub = lax.broadcasted_iota(jnp.int32, (8, length), 0)
    gates, f, b = [], [], []
    for j in range(2):
        gates.append(
            jnp.concatenate(
                [recv[j, d, tok : tok + GATE_ROWS, 0:tok].astype(jnp.float32) for d in range(half)],
                axis=1,
            )
        )
        extra = jnp.concatenate(
            [params[j, pl.ds(first + d, 1), 0:tok] for d in range(half)], axis=1
        )
        offset = params[j, n + 1 : n + 2]
        f.append(log_sigmoid(gates[j][1:2] + offset[:, 0:1]) + extra)
        b.append(log_sigmoid(gates[j][3:4] + offset[:, 1:2]) + extra)
    f = jnp.where(sub == 0, f[0], f[1])
    b = jnp.where(sub == 0, b[0], b[1])
    step = 1
    while step < length:
        f = f + jnp.where(lane >= step, pltpu.roll(f, step, 1), 0.0)
        b = b + jnp.where(lane < length - step, pltpu.roll(b, length - step, 1), 0.0)
        step *= 2
    wide_sub = lax.broadcasted_iota(jnp.int32, (128, length), 0)
    for j in range(2):
        row_i = gates[j][0:1]
        row_f = row_i - f[j : j + 1]
        row_b = gates[j][2:3] - b[j : j + 1]
        rows_of_gate[j] = jnp.where(sub == 0, row_f, row_b)
        leaving = jnp.exp(
            jnp.where(upper, row_b + b[j : j + 1, 0:1], row_f + f[j : j + 1, length - 1 : length])
        )
        stacked = jnp.where(wide_sub == 0, f[j : j + 1], jnp.where(wide_sub == 1, b[j : j + 1], row_i))
        cols[j] = jnp.where(wide_sub == 3, leaving, stacked).T

    scale = dk ** (-0.5)

    def state(j, _):
        kq = recv[j, :, 0:tok, 0 : 2 * dk].reshape(length, 2 * dk).astype(jnp.float32)
        kq = kq * cols[j][:, 3:4]
        memory = lax.dot_general(
            kq.astype(jnp.bfloat16),
            recv[j, :, 0:tok, 2 * dk : 2 * dk + dv].reshape(length, dv),
            (((0,), (0,)), ((), ())),
            preferred_element_type=jnp.float32,
        )
        normal = jnp.sum(kq, axis=0, keepdims=True)
        high = normal.astype(jnp.bfloat16).astype(jnp.float32)
        at = lax.broadcasted_iota(jnp.int32, (GATE_ROWS, 2 * dk), 0)
        state_out[j, 0:dk] = memory[0:dk].astype(jnp.bfloat16)
        state_out[j, dk:, 0 : 2 * dk] = jnp.where(
            at == 0, high, jnp.where(at == 1, normal - high, 0.0)
        ).astype(jnp.bfloat16)
        return 0

    lax.fori_loop(0, 2, state, 0)
    state_copy().start()
    pass_until(1)

    def mixed_copy(o, j, rank):
        return pltpu.make_async_remote_copy(
            src_ref=mixed.at[j, (my_rank + o) % half],
            dst_ref=mrecv.at[rank + j * half],
            send_sem=msend_sem,
            recv_sem=mrecv_sem,
            device_id={"sp": first + (my_rank + o) % half, "dp": my_dp},
            device_id_type=MESH,
        )

    def mixed_all():
        return all_of(mrecv.at[pl.ds(0, 2 * (half - 1))], msend_sem, mrecv_sem)

    def scaled(j, d):
        return recv[j, d, 0:tok, dk : 2 * dk].astype(jnp.float32) * scale

    def before_of(d):
        t_pos = d * tok + lax.broadcasted_iota(jnp.int32, (tok, length), 0)
        return lax.broadcasted_iota(jnp.int32, (tok, length), 1) < t_pos

    lane_z = lax.broadcasted_iota(jnp.int32, (tok, 128), 1)

    def weigh_head(d, k, j):
        m = 2 * k + j
        start = pl.multiple_of(d * tok, tok)
        qs = scaled(j, d)
        ks = recv[j, d, 0:tok, 0:dk].astype(jnp.float32)
        diag = jnp.sum(qs * ks, axis=1, keepdims=True)
        qs = jnp.concatenate([qs, jnp.zeros_like(qs)], axis=1).astype(jnp.bfloat16)
        kall = recv[j, :, 0:tok, 0 : 2 * dk].reshape(length, 2 * dk)
        scores = lax.dot_general(
            qs, kall, (((1,), (1,)), ((), ())), preferred_element_type=jnp.float32
        )
        col = cols[j, pl.ds(start, tok), :]
        col_f, col_b, col_i = col[:, 0:1], col[:, 1:2], col[:, 2:3]
        before = before_of(d)
        rows = rows_of_gate[j]
        weight = scores * jnp.exp(jnp.where(before, col_f + rows[0:1], col_b + rows[1:2]))
        weights[m] = weight
        diag = diag * jnp.exp(col_i)
        z_f = jnp.sum(jnp.where(before, weight, 0.0), axis=1, keepdims=True) + diag
        z_b = jnp.sum(jnp.where(before, 0.0, weight), axis=1, keepdims=True)
        sums[m] = jnp.where(lane_z == 0, z_f, jnp.where(lane_z == 1, z_b, diag))
    def weigh(k, _):
        for j in range(2):
            weigh_head((my_rank + 1 + k) % half, k, j)
        return 0

    lax.fori_loop(0, half, weigh, 0)
    pass_until(2)
    state_copy().wait_recv()

    def segment_head(d, k, j):
        m = 2 * k + j
        start = pl.multiple_of(d * tok, tok)
        col = cols[j, pl.ds(start, tok), :]
        carried = jnp.exp(jnp.where(upper, col[:, 0:1], col[:, 1:2]))
        qs = scaled(j, d) * carried
        normal = state_in[j, dk:, 0:dk].astype(jnp.float32)
        z_state = jnp.sum(qs * (normal[0:1] + normal[1:2]), axis=1, keepdims=True)
        z = sums[m]
        z_f, z_b, diag = z[:, 0:1], z[:, 1:2], z[:, 2:3]
        z_f = z_f + jnp.where(upper, z_state, 0.0)
        z_b = z_b + jnp.where(upper, 0.0, z_state)
        inv_f = 1.0 / jnp.maximum(jnp.abs(z_f), 1.0)
        inv_b = 1.0 / jnp.maximum(jnp.abs(z_b), 1.0)
        probs = (weights[m] * jnp.where(before_of(d), inv_f, inv_b)).astype(jnp.bfloat16)
        vall = recv[j, :, 0:tok, 2 * dk : 2 * dk + dv].reshape(length, dv)
        total = jnp.dot(probs, vall, preferred_element_type=jnp.float32)
        total = total + jnp.dot(
            (qs * jnp.where(upper, inv_f, inv_b)).astype(jnp.bfloat16),
            state_in[j, 0:dk],
            preferred_element_type=jnp.float32,
        )
        total = total + (diag * inv_f) * recv[j, d, 0:tok, 2 * dk : 2 * dk + dv].astype(jnp.float32)
        amp = params[j, n : n + 1, 0:dv]
        total = total * lax.rsqrt(jnp.mean(total * total, axis=1, keepdims=True) + EPS) * amp
        mixed[j, d] = total.astype(jnp.bfloat16)

    def segment(k, _):
        d = (my_rank + 1 + k) % half
        for j in range(2):
            segment_head(d, k, j)

        @pl.when(k < half - 1)
        def _():
            for j in range(2):
                mixed_copy(k + 1, j, my_rank).start()

        @pl.when(k == half - 2)
        def _():
            pass_until(3)

        return 0

    lax.fori_loop(0, half, segment, 0)
    pass_until(4)
    for j in range(2):
        mrecv[my_rank + j * half] = mixed[j, my_rank]
    sub_r = lax.broadcasted_iota(jnp.int32, (rows_in, tok), 0).astype(jnp.float32)
    at = sub_r + (my_z * rows_in).astype(jnp.float32)

    def tables(o, _):
        z = (my_z + o) % nz

        rows = meta[z]
        hit_0, hit_1 = at == rows[0:1], at == rows[1:2]
        table_t[z] = (jnp.where(hit_0, 1.0, 0.0) + jnp.where(hit_1, 1.0, 0.0)).astype(jnp.bfloat16)
        weighted = (jnp.where(hit_0, rows[2:3], 0.0) + jnp.where(hit_1, rows[3:4], 0.0)).T
        high = weighted.astype(jnp.bfloat16)
        table_hi[z] = high
        table_lo[z] = (weighted - high.astype(jnp.float32)).astype(jnp.bfloat16)
        return 0

    if nz > 1:
        all_of(meta.at[pl.ds(0, nz - 1)], meta_send, meta_recv).wait_recv()
    lax.fori_loop(0, nz, tables, 0)
    sig = jax.nn.sigmoid(logits_ref[0].astype(jnp.float32))
    if half > 1:
        mixed_all().wait_recv()
    gated = jnp.concatenate([mrecv[h].astype(jnp.float32) for h in range(n)], axis=1) * sig
    gated = gated.astype(jnp.bfloat16)
    own_w.wait()
    for o in range(chips):
        all_of(w_ref, wc_send.at[o], wc_recv.at[o]).wait_recv()
    for j in range(dpn):
        proj[:, j * wcol : (j + 1) * wcol] = jnp.dot(
            gated, wfull[j], preferred_element_type=jnp.float32
        )
    p = proj[...]
    stream = (
        res_ref[0].astype(jnp.float32)
        + cell_gain_ref[...] * p * lax.rsqrt(jnp.mean(p * p, axis=1, keepdims=True) + EPS)
    ).astype(jnp.bfloat16)
    s = stream.astype(jnp.float32)
    width = s.shape[1]
    part = width // PARTS
    moe = (
        expert_gain_ref[...] * s * lax.rsqrt(jnp.mean(s * s, axis=1, keepdims=True) + EPS)
    ).astype(jnp.bfloat16)

    def line_copy(z, p, to, sems):
        return pltpu.make_async_remote_copy(
            src_ref=line.at[z, p],
            dst_ref=line.at[z, p],
            send_sem=sems.at[z],
            recv_sem=line_recv.at[z, p],
            device_id=device(to, my_q),
            device_id_type=MESH,
        )

    above, below = (my_z + 1) % nz, (my_z + nz - 1) % nz
    has_above, has_below = my_z + 1 < nz, my_z > 0
    edge = (my_z == 0) | (my_z == nz - 1)

    inner_above = ~edge & (2 * my_z < nz - 1)
    inner_below = ~edge & (2 * my_z >= nz - 1)

    def spread(z, p, held=False):
        @pl.when((z <= my_z) & has_above & ~(inner_above & held))
        def _():
            line_copy(z, p, above, up_send).start()

        @pl.when((z >= my_z) & has_below & ~(inner_below & held))
        def _():
            line_copy(z, p, below, down_send).start()

    def release(p):
        @pl.when(inner_above)
        def _():
            line_copy(my_z, p, above, up_send).start()

        @pl.when(inner_below)
        def _():
            line_copy(my_z, p, below, down_send).start()

    for p in range(PARTS):
        line[my_z, p] = moe[:, p * part : (p + 1) * part]
        spread(my_z, p, nz == 4 and p >= PARTS // 2)
    for p in range(PARTS):
        total[p] = s[:, p * part : (p + 1) * part]
    for i in (15, 16, 17):
        loads[i].wait()
    ff = hs.shape[1]

    crossed = nz == 4

    def order_of(z):
        if crossed:
            return ((0, 1, 3, 2), (1, 0, 3, 2), (2, 3, 0, 1), (3, 2, 0, 1))[z]
        inner = 1 if 2 * z < nz - 1 else -1
        return sorted(range(nz), key=lambda s: (abs(s - z), -(s - z) * inner))

    def by_distance(k):
        found = my_z
        for z in range(nz):
            near = order_of(z)
            for place in range(nz):
                found = jnp.where((my_z == z) & (k == place), near[place], found)
        return found

    def plane_copy(src, dst, sems, z, p, q_to, q_src, q_dst):
        return pltpu.make_async_remote_copy(
            src_ref=src.at[z, p, q_src],
            dst_ref=dst.at[z, p, q_dst],
            send_sem=sems[0],
            recv_sem=sems[1].at[z, p],
            device_id=device(my_z, q_to),
            device_id_type=MESH,
        )

    def plane_send(src, dst, sems, z, p):
        def one(o, _):
            q = (my_q + o) % plane
            plane_copy(src, dst, sems, z, p, q, q, my_q).start()
            return 0

        lax.fori_loop(1, plane, one, 0)
        dst[z, p, my_q] = src[z, p, my_q]

    def plane_all(src, dst, sems, z, p):
        others = pl.ds(0, plane - 1)
        return pltpu.make_async_remote_copy(
            src_ref=src.at[z, p, others],
            dst_ref=dst.at[z, p, others],
            send_sem=sems[0],
            recv_sem=sems[1].at[z, p],
            device_id=device(my_z, (my_q + 1) % plane),
            device_id_type=MESH,
        )

    out_way = (outgoing, incoming, (out_send, out_recv))
    back_way = (produced, returned, (back_send, back_recv))

    def dispatch(k, first, last):
        z = by_distance(k)

        def piece(p, _):
            @pl.when(k > 0)
            def _():
                line_copy(z, p, above, up_send).wait_recv()
                spread(z, p)

            block = jnp.dot(table_t[z], line[z, p], preferred_element_type=jnp.float32)
            outgoing[z, p] = block.astype(jnp.bfloat16).reshape(plane, cap, part)
            plane_send(*out_way, z, p)
            return 0

        lax.fori_loop(first, last, piece, 0)

    def expert(k, inline):
        z = by_distance(k)

        def arrive(p, _):
            plane_all(*out_way, z, p).wait_recv()
            return 0

        split = max(PARTS // 2, 1)

        def sides(first, last, at):
            x = jnp.concatenate(
                [incoming[z, p].reshape(rows_in, part) for p in range(first, last)], axis=1
            )
            rows = slice(first * part, last * part)
            a = jnp.dot(x, gate_ref[0, rows, at], preferred_element_type=jnp.float32)
            u = jnp.dot(x, up_ref[0, rows, at], preferred_element_type=jnp.float32)
            return a, u

        def begin_tile(t, _):
            at = pl.ds(pl.multiple_of(t * FF_TILE, FF_TILE), FF_TILE)
            partial[0, :, at], partial[1, :, at] = sides(0, split, at)
            return 0

        def up_tile(t, _):
            at = pl.ds(pl.multiple_of(t * FF_TILE, FF_TILE), FF_TILE)
            a, u = sides(split, PARTS, at)
            a, u = a + partial[0, :, at], u + partial[1, :, at]
            hs[:, at] = (jax.nn.silu(a) * u).astype(jnp.bfloat16)
            return 0

        lax.fori_loop(0, split, arrive, 0)
        lax.fori_loop(0, ff // FF_TILE, begin_tile, 0)
        lax.fori_loop(split, PARTS, arrive, 0)
        lax.fori_loop(0, ff // FF_TILE, up_tile, 0)

        def down_tile(p, _):
            at = pl.ds(pl.multiple_of(p * part, part), part)
            y = jnp.dot(hs[...], down_ref[0, :, at], preferred_element_type=jnp.float32)
            produced[z, p] = y.astype(jnp.bfloat16).reshape(plane, cap, part)

            @pl.when(inline)
            def _():
                plane_send(*back_way, z, p)

            return 0

        lax.fori_loop(0, PARTS, down_tile, 0)

    def send_back(k):
        def piece(p, _):
            plane_send(*back_way, by_distance(k), p)
            return 0

        lax.fori_loop(0, PARTS, piece, 0)

    def partial_copy(z, f):
        to = jnp.where(z < my_z, below, above)
        slot = jnp.where((z > my_z) & (to == z), nz, z)
        return pltpu.make_async_remote_copy(
            src_ref=partial_out.at[z, f],
            dst_ref=partial_in.at[slot, f],
            send_sem=part_send,
            recv_sem=part_recv.at[slot, f],
            device_id=device(to, my_q),
            device_id_type=MESH,
        )

    def partial_arrive(slot, f):
        pltpu.make_async_remote_copy(
            src_ref=partial_out.at[0, f],
            dst_ref=partial_in.at[slot, f],
            send_sem=part_send,
            recv_sem=part_recv.at[slot, f],
            device_id=device(above, my_q),
            device_id_type=MESH,
        ).wait_recv()

    fine = part // SUBS

    def combine(z, p):
        plane_all(*back_way, z, p).wait_recv()
        block = returned[z, p].reshape(rows_in, part)
        mine = jnp.dot(table_hi[z], block, preferred_element_type=jnp.float32) + jnp.dot(
            table_lo[z], block, preferred_element_type=jnp.float32
        )

        @pl.when(z == my_z)
        def _():
            total[p] += mine

        @pl.when((z != my_z) & edge)
        def _():
            for i in range(SUBS):
                f = p * SUBS + i
                partial_out[z, f] = mine[:, i * fine : (i + 1) * fine].astype(jnp.bfloat16)
                partial_copy(z, f).start()

        @pl.when((z != my_z) & ~edge)
        def _():
            total[PARTS] = mine
            for i in range(SUBS):
                f = p * SUBS + i
                partial_arrive(z, f)
                partial_out[z, f] = (
                    total[PARTS, :, i * fine : (i + 1) * fine]
                    + partial_in[z, f].astype(jnp.float32)
                ).astype(jnp.bfloat16)
                partial_copy(z, f).start()

    def combine_all(k):
        def one(p, _):
            combine(by_distance(k), p)
            return 0

        lax.fori_loop(0, PARTS, one, 0)

    dispatch(0, 0, PARTS)
    midway = PARTS // 2

    def tick(k, _):
        last = k == nz - 1
        stop = jnp.where(last, 0, PARTS)
        early = jnp.minimum(jnp.where(k == 0, midway, jnp.where(edge, jnp.where(k == 1, 0, 1), PARTS)), stop)
        dispatch(k + 1, 0, early)

        @pl.when(~edge & (k == nz - 2))
        def _():
            send_back(1)

        if crossed:
            @pl.when(~edge & last)
            def _():
                send_back(2)

        expert(k, edge & (k > 0))
        dispatch(k + 1, early, stop)
        if crossed:
            @pl.when(k == 0)
            def _():
                for p in range(midway, PARTS):
                    release(p)

        @pl.when(edge & (k > 0))
        def _():
            combine_all(k)

        return 0

    lax.fori_loop(0, nz, tick, 0)

    @pl.when(edge)
    def _():
        send_back(0)

    @pl.when(~edge)
    def _():
        for k in range(nz - 1, 2 if crossed else 1, -1):
            send_back(k)
        send_back(0)
        if nz > 2 and not crossed:
            combine_all(1)
        chained = (2, 1) if crossed else tuple(range(nz - 1, 1, -1))

        def one(s, _):
            for behind, k in enumerate(chained):
                p = s - behind

                @pl.when((p >= 0) & (p < PARTS))
                def _():
                    combine(by_distance(k), p)

            return 0

        lax.fori_loop(0, PARTS + max(len(chained) - 1, 0), one, 0)
        if crossed:
            combine_all(3)

    combine_all(0)
    for f in range(PARTS * SUBS):
        p, at = f // SUBS, pl.ds(f % SUBS * fine, fine)

        @pl.when(has_above)
        def _():
            partial_arrive(my_z, f)
            total[p, :, at] += partial_in[my_z, f].astype(jnp.float32)

        @pl.when(has_below)
        def _():
            partial_arrive(nz, f)
            total[p, :, at] += partial_in[nz, f].astype(jnp.float32)

        out_ref[0, :, f * fine : (f + 1) * fine] = total[p, :, at].astype(jnp.bfloat16)

    def drain(z, _):
        @pl.when((z <= my_z) & has_above)
        def _():
            all_of(line.at[z], up_send.at[z], meta_recv).wait_send()

        @pl.when((z >= my_z) & has_below)
        def _():
            all_of(line.at[z], down_send.at[z], meta_recv).wait_send()

        return 0

    lax.fori_loop(0, nz, drain, 0)
    if nz > 1:
        all_of(meta.at[pl.ds(0, nz - 1)], meta_send, meta_recv).wait_send()
        all_of(partial_out.at[pl.ds(0, nz - 1)], part_send, meta_recv).wait_send()
    others = pl.ds(0, plane - 1)
    all_of(outgoing.at[:, :, others], out_send, meta_recv).wait_send()
    all_of(produced.at[:, :, others], back_send, meta_recv).wait_send()
    if half > 1:
        qkv_all().wait_send()
        mixed_all().wait_send()
    param_copy(my_half).wait_send()
    state_copy().wait_send()
    for o in range(chips):
        all_of(w_ref, wc_send.at[o], wc_recv.at[o]).wait_send()
    for o in range(1, chips):
        held = w_ref.at[pl.ds(0, len(sent_parts) * piece)]
        all_of(held, wx_send.at[o - 1], wc_recv.at[0]).wait_send()
        for yo in range(1, ny):
            held = w_ref.at[pl.ds(0, sum(onward(j, yo) for j in range(share)) * piece)]
            all_of(held, wy_send.at[o - 1, yo - 1], wc_recv.at[0]).wait_send()


def on_device(
    residual_input,
    queries,
    keys,
    values,
    gate_logits,
    retention_offset,
    log_forget_extra,
    lane_amplifier,
    output_gate_logits,
    output_projection,
    cell_norm_gain,
    expert_norm_gain,
    expert_index,
    group_mixing_weight,
    within_group_weight,
    gate_weight,
    up_weight,
    down_weight,
):
    n, dpn = lax.axis_size("sp"), lax.axis_size("dp")
    tok, width = residual_input.shape[1:]
    dk, dv = queries.shape[2] // n, values.shape[2] // n
    half = n // 2
    length, devices, ff = half * tok, n * dpn, gate_weight.shape[2]
    cap, chips = 4 * tok // devices, dpn // 2
    ny = chips if n % chips == 0 else 1
    nz, plane = n // ny, ny * dpn
    rows_in, part = plane * cap, width // PARTS
    operands = (
        queries, keys, values, jnp.swapaxes(gate_logits, 1, 2), retention_offset, log_forget_extra,
        lane_amplifier.reshape(1, dv), output_gate_logits, output_projection,
        residual_input, cell_norm_gain.reshape(1, width), expert_norm_gain.reshape(1, width),
        jnp.swapaxes(expert_index, 1, 2), jnp.swapaxes(group_mixing_weight, 1, 2),
        jnp.swapaxes(within_group_weight, 1, 2),
        gate_weight, up_weight, down_weight,
    )
    dma = pltpu.SemaphoreType.DMA
    bf16, f32 = jnp.bfloat16, jnp.float32
    hbm = pl.BlockSpec(memory_space=pltpu.HBM)
    return pl.pallas_call(
        partial(layer_kernel, n=n, dpn=dpn, inputs=len(operands)),
        out_shape=pltpu.VMEM((1, tok, width), bf16),
        in_specs=[hbm] * len(operands),
        out_specs=pl.BlockSpec(memory_space=pltpu.VMEM),
        scratch_shapes=[pltpu.VMEM(x.shape, x.dtype) for x in operands]
        + [
            pltpu.VMEM((n, tok + GATE_ROWS, 2 * dk + dv), bf16),
            pltpu.VMEM((2, half, tok + GATE_ROWS, 2 * dk + dv), bf16),
            pltpu.VMEM((128, tok), f32),
            pltpu.VMEM((2, -(-(n + 2) // 8) * 8, max(tok, dv)), f32),
            pltpu.VMEM((2, 8, length), f32),
            pltpu.VMEM((2, length, 128), f32),
            pltpu.VMEM((n, tok, length), f32),
            pltpu.VMEM((n, tok, 128), f32),
            pltpu.VMEM((2, dk + GATE_ROWS, dv), bf16),
            pltpu.VMEM((2, dk + GATE_ROWS, dv), bf16),
            pltpu.VMEM((2, half, tok, dv), bf16),
            pltpu.VMEM((n, tok, dv), bf16),
            pltpu.VMEM((dpn,) + output_projection.shape, bf16),
            pltpu.VMEM((tok, width), f32),
            pltpu.VMEM((nz, 8, tok), f32),
            pltpu.VMEM((nz, rows_in, tok), bf16),
            pltpu.VMEM((nz, tok, rows_in), bf16),
            pltpu.VMEM((nz, tok, rows_in), bf16),
            pltpu.VMEM((nz, PARTS, tok, part), bf16),
            pltpu.VMEM((nz, PARTS, plane, cap, part), bf16),
            pltpu.VMEM((nz, PARTS, plane, cap, part), bf16),
            pltpu.VMEM((rows_in, ff), bf16),
            pltpu.VMEM((nz, PARTS, plane, cap, part), bf16),
            pltpu.VMEM((nz, PARTS, plane, cap, part), bf16),
            pltpu.VMEM((nz, PARTS * SUBS, tok, part // SUBS), bf16),
            pltpu.VMEM((nz + 1, PARTS * SUBS, tok, part // SUBS), bf16),
            pltpu.VMEM((PARTS + 1, tok, part), f32),
            pltpu.VMEM((2, rows_in, ff), f32),
            dma((len(operands),)),
            dma(()), dma(()), dma(()), dma(()), dma(()), dma(()), dma(()), dma(()),
            dma((max(chips - 1, 1),)), dma((max(chips - 1, 1), PIECES)),
            dma((max(chips - 1, 1), max(ny - 1, 1))), dma((chips,)), dma((chips,)),
            dma(()), dma(()), dma(()),
            dma((nz,)), dma((nz,)), dma((nz, PARTS)),
            dma(()), dma((nz, PARTS)), dma(()), dma((nz, PARTS)),
            dma(()), dma((nz + 1, PARTS * SUBS)),
        ],
        compiler_params=pltpu.CompilerParams(
            collective_id=0, has_side_effects=True, vmem_limit_bytes=60 * 1024 * 1024
        ),
    )(*operands)


def solution(mesh):
    in_specs = (
        P("dp", "sp", None),
        P("dp", "sp", None),
        P("dp", "sp", None),
        P("dp", "sp", None),
        P("dp", "sp", None),
        P("sp", None),
        P("dp", "sp", None),
        P("sp"),
        P("dp", "sp", None),
        P(None, "dp"),
        P(),
        P(),
        P("dp", "sp", None),
        P("dp", "sp", None),
        P("dp", "sp", None),
        P(("sp", "dp"), None, None),
        P(("sp", "dp"), None, None),
        P(("sp", "dp"), None, None),
    )
    out_specs = P("dp", "sp", None)
    return jax.shard_map(
        on_device, mesh=mesh, in_specs=in_specs, out_specs=out_specs, check_vma=False
    )
```
